32 devices in a mesh: sp: 8 (over z, core), tp: 4 (over y, x).
Axes of the slice: x: 2, y: 2, z: 4, core: 2. Of those that a mesh axis runs over, the one named last changes fastest.
Arguments:
- queries: bfloat16 [2048, 2048], P('sp', 'tp'), may hold values from -6 to 6
- keys: bfloat16 [2048, 256], P('sp'), may hold values from -6 to 6
- values: bfloat16 [2048, 256], P('sp'), may hold values from -6 to 6
- query_gain: float32 [128], replicated, may hold values from 0.1 to 5.5
- key_gain: float32 [128], replicated, may hold values from 0.1 to 5.5
- out_proj: bfloat16 [2048, 2048], P(None, 'tp'), may hold values from -0.125 to 0.125
- expert_norm_scale: float32 [2048], replicated, may hold values from 0.1 to 1.9
- residual: bfloat16 [2048, 2048], P(('sp', 'tp')), may hold values from -6 to 6
- routes: int32 [2048, 2], P(('sp', 'tp')), may hold values from 0 to 7, all different within a row; in each aligned block of 64 rows (0 to 63, 64 to 127, ...) at most 32 rows name the same one
- route_weights: float32 [2048, 2], P(('sp', 'tp')), may hold values from 0.1 to 0.9
- w_gate: bfloat16 [8, 2048, 4096], P('sp', None, 'tp'), may hold values from -0.125 to 0.125
- w_up: bfloat16 [8, 2048, 4096], P('sp', None, 'tp'), may hold values from -0.125 to 0.125
- w_down: bfloat16 [8, 4096, 2048], P('sp', 'tp'), may hold values from -0.09375 to 0.09375
Outputs:
- layer_out: bfloat16 [2048, 2048], P(('sp', 'tp'))
The draws below stay inside these ranges and needn't reach their ends.
Inputs may be any that keep to these rules, and one draw needn't show every extreme that they name: `routes`: in the rows of one device no expert is named by more than 32 rows, a bound that some block reaches; a row names 2 different experts.
All inputs are finite; a program needn't handle non-finite values.
Results may differ from the reference program's by a relative error of at most 0.0095.
The reference program's roundings to bfloat16 on the way count: a program that leaves them out, or rounds other values in their place, can miss the bound.
Values may be sent and summed in bfloat16 or wider, within the bound.
A program may use at most 64 MiB of HBM per device.

```python
import math
import jax
import jax.numpy as jnp
import numpy as np
from jax import lax

D = 2048
HD = 128
HEADS = 16
KV = 2
FF = 4096
TOP = 2
GRID_W = 64
TOKENS = 2048
TOK_DEV = 64
EXPERTS = 8
CAP = 32
N_TP = 4


def shared_keys(key):
    base = jax.random.normal(jax.random.fold_in(key, 101), (TOKENS, KV * HD), jnp.float32)
    return jnp.clip(base, -6.0, 6.0)


def draw_keys(key, part):
    return shared_keys(key).astype(jnp.bfloat16)


def draw_queries(key, part):
    base = jax.random.normal(jax.random.fold_in(key, 202), (TOKENS, HEADS * HD), jnp.float32)
    base = jnp.clip(base, -6.0, 6.0)
    return base.astype(jnp.bfloat16)


def draw_query_gain(key, part):
    uniform_draw = jax.random.uniform(jax.random.fold_in(key, 303), (HD,), jnp.float32)
    return 0.1 + 1.8 * uniform_draw


def draw_key_gain(key, part):
    uniform_draw = jax.random.uniform(jax.random.fold_in(key, 404), (HD,), jnp.float32)
    return 0.1 + 1.8 * uniform_draw


def shard_levels(stream_key, dims, pieces, smallest, largest):
    def one(dim, blocks):
        heights = jax.random.uniform(jax.random.fold_in(jax.random.fold_in(stream_key, 6), dim), (blocks,), jnp.float32, smallest / len(pieces), largest / len(pieces))
        return jnp.repeat(jnp.exp(heights), dims[dim] // blocks).reshape((-1,) + (1,) * (len(dims) - dim - 1))

    level = one(*pieces[0])
    for cut in pieces[1:]:
        level = level * one(*cut)
    return level


def assign_block(own_key, own, number, rows, count, top, bound, skew):
    ranking = jax.random.permutation(own_key, count)
    packed, common = load_shares(count, rows * top, bound, skew, True), load_shares(count, rows * top, bound, skew, False)
    places = jnp.arange(count)

    def named(lengths, offset_by):
        used = int((lengths > 0).sum())
        fixed = max(1, used // 4)
        shifted = fixed + (places - fixed + offset_by * (used - fixed)) % max(1, count - fixed)
        return jnp.zeros((count,), jnp.int32).at[ranking[jnp.where(places < fixed, places, shifted)]].set(jnp.asarray(lengths, jnp.int32))

    lengths = jnp.where(number % 4 == 0, named(packed, number // 4), named(common, number - number // 4 - 1))
    mixed = jax.random.permutation(jax.random.fold_in(own, 3), count)
    source_of, taker = mixed[0:count // 2 * 2:2], mixed[1:count // 2 * 2:2]
    slack = jnp.minimum(lengths[source_of] - 1, bound - lengths[taker]) // 2
    slack = jnp.where((source_of == ranking[0]) | (taker == ranking[0]) | (lengths[taker] == 0), 0, jnp.maximum(slack, 0))
    shifted = jax.random.randint(jax.random.fold_in(own, 4), (count // 2,), 0, 1 << 20) % (slack + 1)
    lengths = lengths.at[source_of].add(-shifted).at[taker].add(shifted)
    labels = jnp.searchsorted(jnp.cumsum(lengths), jnp.arange(rows * top), side="right").astype(jnp.int32)
    grid = labels.reshape(top, rows).T
    grid = grid[jax.random.permutation(jax.random.fold_in(own, 1), rows)]
    offset_by = jax.random.randint(jax.random.fold_in(own, 2), (rows, 1), 0, top)
    return jnp.take_along_axis(grid, (jnp.arange(top)[None, :] + offset_by) % top, axis=1)


def load_shares(number_of, total, most, skew, full):
    weights = [(1 << 20) // math.isqrt(rank ** skew) + 1 for rank in range(1, number_of + 1)]
    largest = most if full else min(most, max(-(-total // number_of), total * weights[0] // sum(weights)))
    least = 1 if total - largest >= number_of - 1 else 0
    holding, rest = [largest] + [least] * (number_of - 1), total - largest - least * (number_of - 1)
    while rest > 0:
        candidates = [i for i in range(1, number_of) if holding[i] < largest] or [i for i in range(1, number_of) if holding[i] < most]
        mass, remaining = sum([weights[i] for i in candidates]), rest
        for i in candidates:
            extra = min(most - holding[i], max(1, remaining * weights[i] // mass), rest)
            holding[i] = holding[i] + extra
            rest = rest - extra
    return np.array(holding)


def centred(key, extent, scale, reach, split=(), held_as=jnp.bfloat16):
    result = scale * jax.random.normal(key, extent, jnp.float32)
    if split:
        result = result * shard_levels(key, extent, split, -0.22, 0.18)
    return jnp.clip(result, -reach, reach).astype(held_as)


def setup_inputs(seed: int = 0) -> dict:
    streams_of = jax.random.split(jax.random.key(seed), 14)
    queries = draw_queries(jax.random.fold_in(streams_of[13], 71), 0)
    keys = draw_keys(jax.random.fold_in(streams_of[13], 71), 0)
    values = centred(streams_of[2], (TOKENS, KV * HD), 1.0, 6.0, ((0, 8),))
    query_gain = draw_query_gain(jax.random.fold_in(streams_of[13], 71), 0)
    key_gain = draw_key_gain(jax.random.fold_in(streams_of[13], 71), 0)
    out_proj = centred(streams_of[5], (HEADS * HD, D), (HEADS * HD) ** -0.5, 0.125, ((1, 4),))
    expert_norm_scale = jnp.clip(1.0 + 0.18 * jax.random.normal(streams_of[6], (D,), jnp.float32), 0.1, 1.9)
    residual = centred(streams_of[7], (TOKENS, D), 1.0, 6.0, ((0, 32),))
    routes_keys = jax.random.split(jax.random.fold_in(streams_of[8], 1), TOKENS // TOK_DEV)
    routes_turns = jax.random.permutation(jax.random.fold_in(streams_of[8], 3), TOKENS // TOK_DEV)
    routes = jax.vmap(lambda own, number: assign_block(jax.random.fold_in(streams_of[8], 2), own, number, TOK_DEV, EXPERTS, TOP, CAP, 1))(routes_keys, routes_turns).reshape((TOKENS, TOP))
    route_weights = jnp.clip(0.1 + 0.79999997 * jax.random.uniform(streams_of[9], (TOKENS, TOP), jnp.float32) ** shard_levels(streams_of[9], (TOKENS, TOP), ((0, 32),), -0.2, 0.2), 0.1, 0.9)
    w_gate = centred(streams_of[10], (EXPERTS, D, FF), D ** -0.5, 0.125, ((0, 8), (2, 4)))
    w_up = centred(streams_of[11], (EXPERTS, D, FF), D ** -0.5, 0.125, ((0, 8), (2, 4)))
    w_down = centred(streams_of[12], (EXPERTS, FF, D), FF ** -0.5, 0.09375, ((0, 8), (1, 4)))
    return dict(queries=queries, keys=keys, values=values, query_gain=query_gain, key_gain=key_gain, out_proj=out_proj, expert_norm_scale=expert_norm_scale, residual=residual, routes=routes, route_weights=route_weights, w_gate=w_gate, w_up=w_up, w_down=w_down)


EPS = 1e-06
ROPE_BASE = 10000.0

def rotate(field, position):
    half = field.shape[-1] // 2
    quarter = half // 2
    freqs = ROPE_BASE ** (-jnp.arange(quarter, dtype=jnp.float32) / quarter)
    grid_row = (position // GRID_W).astype(jnp.float32)
    grid_col = (position % GRID_W).astype(jnp.float32)

    def turn_half(part, coord):
        angle = coord[:, None] * freqs[None, :]
        cosine = jnp.cos(angle)[:, None, :]
        sine = jnp.sin(angle)[:, None, :]
        first, second = (part[..., :quarter], part[..., quarter:])
        return jnp.concatenate([first * cosine - second * sine, second * cosine + first * sine], axis=-1)
    return jnp.concatenate([turn_half(field[..., :half], grid_row), turn_half(field[..., half:], grid_col)], axis=-1)

def prepare(field, gain, position):
    count = field.shape[0]
    width = gain.shape[0]
    heads_here = field.shape[1] // width
    values_f = field.reshape(count, heads_here, width).astype(jnp.float32)
    scaled = values_f * lax.rsqrt(lax.optimization_barrier(jnp.mean(values_f * values_f, axis=-1, keepdims=True)) + EPS) * gain
    return rotate(scaled, position).reshape(count, heads_here * width).astype(jnp.bfloat16)

def reference(queries, keys, values, query_gain, key_gain, out_proj, expert_norm_scale, residual, routes, route_weights, w_gate, w_up, w_down):
    position = jnp.arange(TOKENS, dtype=jnp.int32)
    q_rot = prepare(queries, query_gain, position)
    k_rot = prepare(keys, key_gain, position)
    group = HEADS // KV
    block = math.gcd(TOKENS, 1024)

    def one_head(head):
        shared_value_head = head // group
        query_cols = lax.dynamic_slice_in_dim(q_rot, (head * HD).astype(jnp.int32), HD, 1)
        key_cols = lax.dynamic_slice_in_dim(k_rot, (shared_value_head * HD).astype(jnp.int32), HD, 1)
        value_cols = lax.dynamic_slice_in_dim(values, (shared_value_head * HD).astype(jnp.int32), HD, 1)

        def attend(query_block):
            scores = jnp.dot(query_block, key_cols.T, preferred_element_type=jnp.float32) * HD ** (-0.5)
            row_max = lax.optimization_barrier(jnp.max(scores, axis=-1, keepdims=True))
            weight_tensors = jnp.exp(scores - row_max).astype(jnp.bfloat16)
            total = lax.optimization_barrier(jnp.sum(lax.optimization_barrier(weight_tensors).astype(jnp.float32), axis=-1, keepdims=True))
            summed = jnp.dot(weight_tensors, value_cols, preferred_element_type=jnp.float32)
            return (summed / total).astype(jnp.bfloat16)
        blocks = query_cols.reshape(TOKENS // block, block, HD)
        return lax.map(attend, blocks).reshape(TOKENS, HD)
    per_head = lax.map(one_head, jnp.arange(HEADS, dtype=jnp.int32))
    attn = per_head.transpose(1, 0, 2).reshape(TOKENS, HEADS * HD)
    projected = jnp.dot(attn, out_proj, preferred_element_type=jnp.float32).astype(jnp.bfloat16)
    mixed = (residual.astype(jnp.float32) + projected.astype(jnp.float32)).astype(jnp.bfloat16)
    mixed_float_output = mixed.astype(jnp.float32)
    normed = (mixed_float_output * lax.rsqrt(lax.optimization_barrier(jnp.mean(mixed_float_output * mixed_float_output, axis=-1, keepdims=True)) + EPS) * expert_norm_scale).astype(jnp.bfloat16)
    flat_routes = routes.reshape(-1)
    flat_weights = route_weights.reshape(-1)
    flat_token = jnp.arange(TOKENS * TOP, dtype=jnp.int32) // TOP
    most_rows = TOKENS // TOK_DEV * CAP
    block_ff = FF // N_TP

    def expert_step(totals, expert):
        order = jnp.argsort((flat_routes != expert).astype(jnp.int32), stable=True)[:most_rows].astype(jnp.int32)
        valid = flat_routes[order] == expert
        rows = normed[flat_token[order]]
        gate = jnp.dot(rows, w_gate[expert], preferred_element_type=jnp.float32)
        upper = jnp.dot(rows, w_up[expert], preferred_element_type=jnp.float32)
        hidden = (jax.nn.silu(gate) * upper).astype(jnp.bfloat16)
        hidden_blocks = hidden.reshape(most_rows, N_TP, block_ff).astype(jnp.float32)
        down_blocks = w_down[expert].reshape(N_TP, block_ff, D).astype(jnp.float32)
        partial_value = jnp.einsum('mjf,jfd->jmd', hidden_blocks, down_blocks).astype(jnp.bfloat16)
        summed = lax.optimization_barrier(jnp.sum(lax.optimization_barrier(partial_value).astype(jnp.float32), axis=0))
        expert_out = summed.astype(jnp.bfloat16)
        weighted = lax.optimization_barrier(expert_out).astype(jnp.float32) * flat_weights[order][:, None]
        weighted = jnp.where(valid[:, None], weighted, jnp.float32(0.0))
        return (totals.at[order].add(weighted), None)
    start = jnp.zeros((TOKENS * TOP, D), jnp.float32)
    totals, unused = lax.scan(expert_step, start, jnp.arange(EXPERTS, dtype=jnp.int32))
    moe_sum = lax.optimization_barrier(jnp.sum(totals.reshape(TOKENS, TOP, D), axis=1))
    return (mixed_float_output + moe_sum).astype(jnp.bfloat16)
```

```python
import functools

import jax
import jax.numpy as jnp
from jax import lax
from jax.experimental import pallas as pl
from jax.experimental.pallas import tpu as pltpu
from jax.sharding import PartitionSpec as P

GRID_W = 64


EPS = 1e-06
ROPE_BASE = 10000.0
NEG_START = -1e30


def rotate(field, position):
    half = field.shape[-1] // 2
    quarter = half // 2
    freqs = ROPE_BASE ** (-jnp.arange(quarter, dtype=jnp.float32) / quarter)
    grid_row = (position // GRID_W).astype(jnp.float32)
    grid_col = (position % GRID_W).astype(jnp.float32)

    def turn_half(part, coord):
        angle = coord[:, None] * freqs[None, :]
        cosine = jnp.cos(angle)[:, None, :]
        sine = jnp.sin(angle)[:, None, :]
        first, second = (part[..., :quarter], part[..., quarter:])
        return jnp.concatenate(
            [first * cosine - second * sine, second * cosine + first * sine], axis=-1
        )

    return jnp.concatenate(
        [turn_half(field[..., :half], grid_row), turn_half(field[..., half:], grid_col)], axis=-1
    )


def prepare(field, gain, position):
    count = field.shape[0]
    width = gain.shape[0]
    heads_here = field.shape[1] // width
    values_f = field.reshape(count, heads_here, width).astype(jnp.float32)
    scaled = (
        values_f * lax.rsqrt(jnp.mean(values_f * values_f, axis=-1, keepdims=True) + EPS) * gain
    )
    return rotate(scaled, position).reshape(count, heads_here * width).astype(jnp.bfloat16)


def absorb(carry, query_matrix, key_rows, value_rows, scale):
    count = key_rows.shape[0]
    width = 2048 if count > 2048 and count % 2048 == 0 else count
    key_blocks = key_rows.reshape(count // width, width, key_rows.shape[1], key_rows.shape[2])
    value_blocks = value_rows.reshape(
        count // width, width, value_rows.shape[1], value_rows.shape[2]
    )

    def step(state, block):
        run_max, run_sum, run_acc = state
        key_tile_rows, value_tile_rows = block
        scores = (
            jnp.einsum(
                "hxt,ght->hxg", query_matrix, key_tile_rows, preferred_element_type=jnp.float32
            )
            * scale
        )
        new_max = jnp.maximum(run_max, jnp.max(scores, axis=-1))
        weight_tensors = jnp.exp(scores - new_max[..., None]).astype(jnp.bfloat16)
        factor = jnp.exp(run_max - new_max)
        run_sum = run_sum * factor + jnp.sum(weight_tensors.astype(jnp.float32), axis=-1)
        run_acc = run_acc * factor[..., None] + jnp.einsum(
            "zij,jzu->ziu", weight_tensors, value_tile_rows, preferred_element_type=jnp.float32
        )
        return ((new_max, run_sum, run_acc), None)

    result, unused = lax.scan(step, carry, (key_blocks, value_blocks))
    return result


MESH = pl.DeviceIdType.MESH
VMEM_LIMIT = 60 * 1024 * 1024


def greet(partners, count):
    barrier = pltpu.get_barrier_semaphore()
    for where in partners:
        pl.semaphore_signal(barrier, inc=1, device_id=where, device_id_type=MESH)
    pl.semaphore_wait(barrier, count)


def remote(src, dst, send, recv, where):
    return pltpu.make_async_remote_copy(
        src_ref=src, dst_ref=dst, send_sem=send, recv_sem=recv, device_id=where, device_id_type=MESH
    )


def square():
    mine = lax.axis_index("tp")
    return mine, mine + 1 - 2 * lax.rem(mine, 2), lax.rem(mine + 2, 4), 3 - mine


def gather_kernel(n, k_ref, v_ref, n_ref, ko_ref, vo_ref, no_ref, send, recv):
    me = lax.axis_index("sp")
    chips = n // 2
    chip, core = me // 2, lax.rem(me, 2)
    partner = 2 * chip + 1 - core
    has_right, has_left = chip < chips - 1, chip > 0
    right, left = me + 2, me - 2
    barrier = pltpu.get_barrier_semaphore()
    pl.semaphore_signal(barrier, inc=1, device_id={"sp": partner}, device_id_type=MESH)

    @pl.when(has_right)
    def _():
        pl.semaphore_signal(barrier, inc=1, device_id={"sp": right}, device_id_type=MESH)

    @pl.when(has_left)
    def _():
        pl.semaphore_signal(barrier, inc=1, device_id={"sp": left}, device_id_type=MESH)

    pl.semaphore_wait(barrier, 1 + has_right.astype(jnp.int32) + has_left.astype(jnp.int32))

    pairs = ((k_ref, ko_ref), (v_ref, vo_ref), (n_ref, no_ref))

    def block(out, origin):
        rows = out.shape[0] // n
        return out.at[pl.ds(pl.multiple_of(origin * rows, rows), rows)]

    def copies(origin, way, where, own=False):
        return [
            remote(
                ref if own else block(out, origin),
                block(out, origin),
                send.at[origin, way, i],
                recv.at[origin, i],
                {"sp": where},
            )
            for i, (ref, out) in enumerate(pairs)
        ]

    def start(*args, **kw):
        for c in copies(*args, **kw):
            c.start()

    def sent(*args, **kw):
        for c in copies(*args, **kw):
            c.wait_send()

    def arrived(origin):
        for c in copies(origin, 0, partner):
            c.wait_recv()

    @pl.when(has_right)
    def _():
        start(me, 0, right, own=True)

    @pl.when(has_left)
    def _():
        start(me, 2, left, own=True)

    start(me, 1, partner, own=True)
    for ref, out in pairs:
        block(out, me)[...] = ref[...]
    for j in range(1, chips):

        @pl.when(chip - j >= 0)
        def _(origin=me - 2 * j):
            arrived(origin)

            @pl.when(has_right)
            def _():
                start(origin, 0, right)

            start(origin, 1, partner)

        @pl.when(chip + j < chips)
        def _(origin=me + 2 * j):
            arrived(origin)

            @pl.when(has_left)
            def _():
                start(origin, 2, left)

            start(origin, 1, partner)

    for z in range(chips):
        arrived(2 * z + 1 - core)
    sent(me, 1, partner, own=True)

    @pl.when(has_right)
    def _():
        sent(me, 0, right, own=True)

    @pl.when(has_left)
    def _():
        sent(me, 2, left, own=True)

    for j in range(1, chips):

        @pl.when(chip - j >= 0)
        def _(origin=me - 2 * j):
            @pl.when(has_right)
            def _():
                sent(origin, 0, right)

            sent(origin, 1, partner)

        @pl.when(chip + j < chips)
        def _(origin=me + 2 * j):
            @pl.when(has_left)
            def _():
                sent(origin, 2, left)

            sent(origin, 1, partner)


def in_vmem(count):
    return [pl.BlockSpec(memory_space=pltpu.VMEM)] * count


def params(number):
    return pltpu.CompilerParams(
        collective_id=number, has_side_effects=True, vmem_limit_bytes=VMEM_LIMIT
    )


def gather_rows(n, own_keys, own_values, notes):
    arrays = (own_keys, own_values, notes)
    return pl.pallas_call(
        functools.partial(gather_kernel, n),
        out_shape=tuple(
            jax.ShapeDtypeStruct((n * a.shape[0], a.shape[1]), a.dtype) for a in arrays
        ),
        in_specs=in_vmem(3),
        out_specs=tuple(in_vmem(3)),
        scratch_shapes=[pltpu.SemaphoreType.DMA((n, 3, 3)), pltpu.SemaphoreType.DMA((n, 3))],
        compiler_params=params(0),
        name="gather_rows",
    )(*arrays)


def project_kernel(
    attn_ref, w_ref, n_ref, out_ref, no_ref, held, stage, send, recv, give, take, tell, told
):
    mine, across, along, corner = square()
    rows, width = attn_ref.shape
    half = rows // 2
    share = out_ref.shape[0]
    greet([{"tp": across}, {"tp": along}, {"tp": corner}], 3)
    first = [
        remote(attn_ref, held.at[mine], send.at[0], recv.at[0], {"tp": across}),
        remote(attn_ref, held.at[mine], send.at[1], recv.at[1], {"tp": along}),
    ]
    for c in first:
        c.start()
    notes = [
        remote(n_ref, no_ref.at[mine], tell.at[i], told.at[i], {"tp": p})
        for i, p in enumerate((corner, across, along))
    ]
    for c in notes:
        c.start()
    no_ref[mine] = n_ref[...]
    top, low = pl.ds(0, half), pl.ds(half, half)
    second = [
        remote(held.at[across, top], held.at[across, top], send.at[2], recv.at[2], {"tp": along}),
        remote(held.at[along, low], held.at[along, low], send.at[3], recv.at[3], {"tp": across}),
    ]

    def term(rows_here, owner):
        part = w_ref[pl.ds(pl.multiple_of(owner * width, width), width), :]
        return jnp.dot(rows_here, part, preferred_element_type=jnp.float32)

    total = term(attn_ref[...], mine)
    first[0].wait_recv()
    second[0].start()
    first[1].wait_recv()
    second[1].start()
    total += term(held[across], across)
    total += term(held[along], along)
    for c in second:
        c.wait_recv()
    total += term(held[corner], corner)
    stage[...] = total.astype(stage.dtype)
    columns = pl.ds(pl.multiple_of(mine * width, width), width)

    def piece(owner):
        return pl.ds(pl.multiple_of(owner * share, share), share)

    back = [
        remote(stage.at[piece(p)], out_ref.at[:, columns], give.at[i], take.at[i], {"tp": p})
        for i, p in enumerate((corner, across, along))
    ]
    for c in back:
        c.start()
    out_ref[:, columns] = stage[piece(mine), :]
    for c in back + notes:
        c.wait()
    for c in first + second:
        c.wait_send()


def project(attn, out_proj, notes, share):
    rows, width = attn.shape
    parts = out_proj.shape[0] // width
    return pl.pallas_call(
        project_kernel,
        out_shape=(
            jax.ShapeDtypeStruct((share, out_proj.shape[1] * parts), jnp.bfloat16),
            jax.ShapeDtypeStruct((parts,) + notes.shape, notes.dtype),
        ),
        in_specs=in_vmem(3),
        out_specs=tuple(in_vmem(2)),
        scratch_shapes=[
            pltpu.VMEM((parts, rows, width), jnp.bfloat16),
            pltpu.VMEM((rows, out_proj.shape[1]), jnp.bfloat16),
            pltpu.SemaphoreType.DMA((4,)),
            pltpu.SemaphoreType.DMA((4,)),
            pltpu.SemaphoreType.DMA((3,)),
            pltpu.SemaphoreType.DMA((3,)),
            pltpu.SemaphoreType.DMA((3,)),
            pltpu.SemaphoreType.DMA((3,)),
        ],
        compiler_params=params(1),
        name="project",
    )(attn, out_proj, notes)


def visit(chip, chips, step):
    near = jnp.minimum(chip, chips - 1 - chip)
    swing = chip + ((step + 1) // 2) * (1 - 2 * lax.rem(step, 2))
    up = chip < chips - 1 - chip
    tail = jnp.where(up, chip + (step - near), chip - (step - near))
    return jnp.where(step <= 2 * near, swing, tail)


def wide(value):
    return value.astype(jnp.float32)


def moe_kernel(
    n, cuts, x_ref, mixed_ref, slot_ref, part_ref, wg_ref, wu_ref, wd_ref, out_ref,
    tok, wg, wu, wd, picked, hid, wsel, held, own, give, take,
    low, high, from_x, from_y, to_y, to_x, last_y, last_x, acc, zsend, zrecv,
    load, zs, zr, sq_s, sq_r, pd_s, pd_r, tk_s, tk_r, hop_s, hop_r, hz_s, hz_r,
):
    me = lax.axis_index("sp")
    chips = n // 2
    chip, core = me // 2, lax.rem(me, 2)
    other = 1 - core
    partner = {"sp": 2 * chip + other}
    mine, across, along, corner = square()
    x, y = lax.rem(mine, 2), mine // 2
    share, depth = x_ref.shape
    units = wg.shape[1]
    group = 4 * share
    slots = wsel.shape[2] // 2
    width = depth // cuts
    half = width // 2
    steps = chips * cuts

    def column(k):
        return pl.ds(pl.multiple_of(k * width, width), width)

    loads = [
        pltpu.make_async_copy(wg_ref.at[0], wg, load.at[0]),
        pltpu.make_async_copy(wu_ref.at[0], wu, load.at[1]),
    ] + [
        pltpu.make_async_copy(wd_ref.at[0, :, pl.ds(q * width, width)], wd.at[q], load.at[2 + q])
        for q in range(cuts)
    ]
    for c in loads:
        c.start()

    barrier = pltpu.get_barrier_semaphore()

    def greet_one(where):
        pl.semaphore_signal(barrier, inc=1, device_id=where, device_id_type=MESH)

    greet_one(partner)
    greet_one({"tp": across})
    greet_one({"tp": along})
    for d in range(1, chips):
        greet_one({"sp": 2 * lax.rem(chip + d, chips) + core})
    pl.semaphore_wait(barrier, chips + 2)

    def to_plane(p):
        return remote(x_ref, tok.at[chip, core, mine], zs.at[p], zr.at[chip], {"sp": 2 * p + core})

    def from_plane(p):
        return remote(x_ref, tok.at[p, core, mine], zs.at[p], zr.at[p], {"sp": 2 * p + core})

    upper, lower = pl.ds(0, share // 2), pl.ds(share // 2, share // 2)

    def pass_on(p, way, first=False):
        block = tok.at[p, core]
        src, dst, where = (
            (x_ref if first else block.at[mine], block.at[mine], across),
            (x_ref if first else block.at[mine], block.at[mine], along),
            (block.at[across, upper], block.at[across, upper], along),
            (block.at[along, lower], block.at[along, lower], across),
        )[way]
        return remote(src, dst, sq_s.at[p, way], sq_r.at[p, way], {"tp": where})

    def arrive(p, way):
        block = tok.at[p, core]
        dst = (
            block.at[across],
            block.at[along],
            block.at[corner, upper],
            block.at[corner, lower],
        )[way]
        remote(dst, dst, sq_s.at[p, way], sq_r.at[p, way], {"tp": across}).wait_recv()

    def hand(p, t, first=False):
        block = tok.at[p, core, t]
        return remote(x_ref if first else block, block, pd_s.at[p, t], pd_r.at[p, t], partner)

    def handed(p, t):
        block = tok.at[p, other, t]
        remote(block, block, pd_s.at[p, t], pd_r.at[p, t], partner).wait_recv()

    pass_on(chip, 0, True).start()
    pass_on(chip, 1, True).start()
    for j in range(1, chips):

        @pl.when(chip + j < chips)
        def _():
            to_plane(chip + j).start()

        @pl.when(chip - j >= 0)
        def _():
            to_plane(chip - j).start()

    hand(chip, mine, True).start()
    tok[chip, core, mine] = x_ref[...]

    def expert(p):
        arrive(p, 2)
        arrive(p, 3)
        hand(p, corner).start()
        for t in range(4):
            handed(p, t)
        for side in range(2):
            spot = slot_ref[2 * p + side]
            hit = lax.broadcasted_iota(jnp.int32, (slots, group), 0) == spot
            pick = jnp.where(hit, 1.0, 0.0).astype(tok.dtype)
            parts = part_ref[2 * p + side]
            wsel[p, side, :slots] = jnp.where(hit, parts[0:1], 0.0).astype(wsel.dtype)
            wsel[p, side, slots:] = jnp.where(hit, parts[1:2], 0.0).astype(wsel.dtype)

            @pl.loop(0, cuts)
            def _(q):
                block = tok[p, side, :, :, column(q)].reshape(group, width)
                rows = jnp.dot(pick, block, preferred_element_type=jnp.float32)
                picked[side * slots : (side + 1) * slots, column(q)] = rows.astype(picked.dtype)

        @pl.loop(0, units // 256)
        def _(u):
            cols = pl.ds(pl.multiple_of(u * 256, 256), 256)
            gate = jnp.dot(picked[...], wg[:, cols], preferred_element_type=jnp.float32)
            upper_part = jnp.dot(picked[...], wu[:, cols], preferred_element_type=jnp.float32)
            hid[p, :, cols] = (jax.nn.silu(gate) * upper_part).astype(hid.dtype)

    @pl.loop(0, chips)
    def _(s):
        @pl.when(s + 1 < chips)
        def _():
            p = visit(chip, chips, s + 1)
            from_plane(p).wait_recv()
            pass_on(p, 0).start()
            pass_on(p, 1).start()
            hand(p, mine).start()

        p = visit(chip, chips, s)
        arrive(p, 0)
        pass_on(p, 2).start()
        hand(p, across).start()
        arrive(p, 1)
        pass_on(p, 3).start()
        hand(p, along).start()

        @pl.when(s == 0)
        def _():
            for c in loads:
                c.wait()

        @pl.when(s >= 1)
        def _():
            expert(visit(chip, chips, s - 1))

    def plane_of(k):
        return visit(chip, chips, lax.rem(k // cuts + 1, chips))

    def swap(k):
        return remote(give.at[k], take.at[k], tk_s.at[k], tk_r.at[k], partner)

    def hop(k, way):
        src, dst, where = (
            (low.at[k, 1 - x], from_x.at[k], across),
            (high.at[k, 1 - y], from_y.at[k], along),
            (to_y.at[k], last_y.at[k], along),
            (to_x.at[k], last_x.at[k], across),
        )[way]
        return remote(src, dst, hop_s.at[k, way], hop_r.at[k, way], {"tp": where})

    def home(k):
        p, q = plane_of(k), lax.rem(k, cuts)
        return remote(
            zsend.at[k], zrecv.at[chip, q], hz_s.at[k], hz_r.at[chip, q], {"sp": 2 * p + core}
        )

    def homed(p, q):
        return remote(zsend.at[0], zrecv.at[p, q], hz_s.at[0], hz_r.at[p, q], partner)

    @pl.loop(0, steps + 5)
    def _(step):
        @pl.when((step >= 1) & (step <= steps))
        def _(k=step - 1):
            swap(k).wait_recv()
            total = own[lax.rem(k, 2)] + wide(take[k])
            cast = total.astype(low.dtype).reshape(4, share, width)
            for t in range(4):
                low[k, t % 2, t // 2] = cast[t, :, :half]
                high[k, t // 2, t % 2] = cast[t, :, half:]
            hop(k, 0).start()
            hop(k, 1).start()

        @pl.when(step < steps)
        def _(k=step):
            @pl.when(k == cuts)
            def _():
                expert(visit(chip, chips, chips - 1))

            p, q = plane_of(k), lax.rem(k, cuts)
            out = jnp.dot(hid[p], wd[q], preferred_element_type=jnp.float32).astype(held.dtype)
            for side in range(2):
                block = out[side * slots : (side + 1) * slots]
                held[side, :slots] = block
                held[side, slots:] = block

            def spread(side):
                return lax.dot_general(
                    wsel[p, side], held[side], (((0,), (0,)), ((), ())),
                    preferred_element_type=jnp.float32,
                )

            give[k] = spread(other).astype(give.dtype)
            swap(k).start()
            own[lax.rem(k, 2)] = spread(core)

        @pl.when((step >= 3) & (step < steps + 3))
        def _(k=step - 3):
            hop(k, 0).wait_recv()
            to_y[k] = (wide(low[k, x, 1 - y]) + wide(from_x[k, 1 - y])).astype(to_y.dtype)
            hop(k, 2).start()
            hop(k, 1).wait_recv()
            to_x[k] = (wide(high[k, y, 1 - x]) + wide(from_y[k, 1 - x])).astype(to_x.dtype)
            hop(k, 3).start()

        @pl.when(step >= 5)
        def _(k=step - 5):
            hop(k, 2).wait_recv()
            left = wide(low[k, x, y]) + wide(from_x[k, y]) + wide(last_y[k])
            hop(k, 3).wait_recv()
            right = wide(high[k, y, x]) + wide(from_y[k, x]) + wide(last_x[k])

            @pl.when(k < steps - cuts)
            def _():
                zsend[k, :, :half] = left.astype(zsend.dtype)
                zsend[k, :, half:] = right.astype(zsend.dtype)
                home(k).start()

            @pl.when(k >= steps - cuts)
            def _():
                acc[lax.rem(k, cuts), :, :half] = left
                acc[lax.rem(k, cuts), :, half:] = right

    @pl.loop(0, cuts)
    def _(q):
        total = acc[q] + wide(mixed_ref[:, column(q)])
        for d in range(1, chips):
            p = lax.rem(chip + d, chips)
            homed(p, q).wait_recv()
            total += wide(zrecv[p, q])
        out_ref[:, column(q)] = total.astype(out_ref.dtype)

    for d in range(1, chips):
        to_plane(lax.rem(chip + d, chips)).wait_send()

    @pl.loop(0, chips)
    def _(p):
        for way in range(4):
            pass_on(p, way).wait_send()
            hand(p, way).wait_send()

    @pl.loop(0, steps)
    def _(k):
        swap(k).wait_send()
        for way in range(4):
            hop(k, way).wait_send()

        @pl.when(k < steps - cuts)
        def _():
            home(k).wait_send()


def moe(n, normed, mixed, slot_rows, weight_rows, capacity, w_gate, w_up, w_down, cuts=4):
    share, depth = normed.shape
    units = w_gate.shape[2]
    chips = n // 2
    kind = normed.dtype
    width = depth // cuts
    half = width // 2
    steps = chips * cuts
    group, slots = 4 * share, 4 * capacity
    dma = pltpu.SemaphoreType.DMA

    def room(*extent):
        return pltpu.VMEM(extent, kind)

    def exact(*extent):
        return pltpu.VMEM(extent, jnp.float32)

    return pl.pallas_call(
        functools.partial(moe_kernel, n, cuts),
        out_shape=jax.ShapeDtypeStruct((share, depth), kind),
        in_specs=in_vmem(4) + [pl.BlockSpec(memory_space=pl.ANY)] * 3,
        out_specs=in_vmem(1)[0],
        scratch_shapes=[
            room(chips, 2, 4, share, depth),
            room(depth, units),
            room(depth, units),
            room(cuts, units, width),
            room(2 * slots, depth),
            room(chips, 2 * slots, units),
            room(chips, 2, 2 * slots, group),
            room(2, 2 * slots, width),
            exact(2, group, width),
            room(steps, group, width),
            room(steps, group, width),
            room(steps, 2, 2, share, half),
            room(steps, 2, 2, share, half),
            room(steps, 2, share, half),
            room(steps, 2, share, half),
            room(steps, share, half),
            room(steps, share, half),
            room(steps, share, half),
            room(steps, share, half),
            exact(cuts, share, width),
            room(steps - cuts, share, width),
            room(chips, cuts, share, width),
            dma((2 + cuts,)),
            dma((chips,)),
            dma((chips,)),
            dma((chips, 4)),
            dma((chips, 4)),
            dma((chips, 4)),
            dma((chips, 4)),
            dma((steps,)),
            dma((steps,)),
            dma((steps, 4)),
            dma((steps, 4)),
            dma((steps,)),
            dma((chips, cuts)),
        ],
        compiler_params=params(2),
        name="moe",
    )(normed, mixed, slot_rows, weight_rows, w_gate, w_up, w_down)


def start_state(batch, rows, width):
    return (
        jnp.full((batch, rows), NEG_START, jnp.float32),
        jnp.zeros((batch, rows), jnp.float32),
        jnp.zeros((batch, rows, width), jnp.float32),
    )


def local(
    queries,
    keys,
    values,
    query_gain,
    key_gain,
    out_proj,
    expert_norm_scale,
    residual,
    routes,
    route_weights,
    w_gate,
    w_up,
    w_down,
):
    head_size = query_gain.shape[0]
    tok_sp = queries.shape[0]
    tp_count = lax.axis_size("tp")
    sp_count = lax.axis_size("sp")
    heads_dev = queries.shape[1] // head_size
    all_heads = heads_dev * tp_count
    kv_heads = keys.shape[1] // head_size
    group = all_heads // kv_heads
    scale = head_size ** (-0.5)
    tp_index = lax.axis_index("tp")
    sp_index = lax.axis_index("sp")
    position = sp_index * tok_sp + jnp.arange(tok_sp, dtype=jnp.int32)
    q_rot = prepare(queries, query_gain, position)
    shared_value_head = tp_index * heads_dev // group
    own_keys = prepare(
        lax.dynamic_slice_in_dim(keys, shared_value_head * head_size, head_size, 1),
        key_gain,
        position,
    )
    own_values = lax.dynamic_slice_in_dim(values, shared_value_head * head_size, head_size, 1)
    query_matrix = (
        q_rot.reshape(tok_sp, heads_dev, head_size)
        .transpose(1, 0, 2)
        .reshape(1, heads_dev * tok_sp, head_size)
    )
    tok_dev = residual.shape[0]
    top = routes.shape[1]
    capacity = max(2, 2 * tok_dev * top // sp_count)
    direct = (
        tp_count == 4 and sp_count % 2 == 0 and capacity % 16 == 0 and 2 * tok_dev % 128 == 0
    )
    named = routes[:, :, None] == jnp.arange(sp_count, dtype=jnp.int32)[None, None, :]
    if direct:
        taken = jnp.any(named, axis=1).astype(jnp.int32)
        place = jnp.where(taken > 0, jnp.cumsum(taken, axis=0) - 1, -1).astype(jnp.float32)
        load = jnp.sum(jnp.where(named, route_weights[:, :, None], 0.0), axis=1)
        notes = jnp.concatenate([place, load], axis=0).T
        key_piece, value_piece, notes = gather_rows(sp_count, own_keys, own_values, notes)
    else:
        key_piece = lax.all_gather(own_keys, "sp", axis=0, tiled=True)
        value_piece = lax.all_gather(own_values, "sp", axis=0, tiled=True)
    run_max, run_sum, run_acc = absorb(
        start_state(1, heads_dev * tok_sp, head_size),
        query_matrix,
        key_piece[:, None, :],
        value_piece[:, None, :],
        scale,
    )
    attn = (run_acc / run_sum[..., None]).astype(jnp.bfloat16)
    attn = (
        attn.reshape(heads_dev, tok_sp, head_size)
        .transpose(1, 0, 2)
        .reshape(tok_sp, heads_dev * head_size)
    )
    if direct:
        projected, notes = project(attn, out_proj, notes, tok_dev)
    else:
        columns = jnp.dot(
            lax.all_gather(attn, "tp", axis=1, tiled=True),
            out_proj,
            preferred_element_type=jnp.float32,
        )
        projected = lax.all_to_all(
            columns.astype(jnp.bfloat16), "tp", split_axis=0, concat_axis=1, tiled=True
        )
    mixed_float_output = residual.astype(jnp.float32) + projected.astype(jnp.float32)
    mixed = mixed_float_output.astype(jnp.bfloat16)
    mixed_float_output = mixed.astype(jnp.float32)
    normed = (
        mixed_float_output
        * lax.rsqrt(jnp.mean(mixed_float_output * mixed_float_output, axis=-1, keepdims=True) + EPS)
        * expert_norm_scale
    ).astype(jnp.bfloat16)
    if direct:
        notes = notes.reshape(tp_count, sp_count, sp_count, 2, tok_dev)
        notes = lax.dynamic_index_in_dim(notes, sp_index, 2, keepdims=False)
        notes = notes.transpose(1, 2, 0, 3)
        base = capacity * jnp.arange(tp_count, dtype=jnp.float32)[:, None]
        spots = jnp.where(notes[:, 0] >= 0, notes[:, 0] + base, -1.0).astype(jnp.int32)
        coarse = lax.reduce_precision(notes[:, 1], 8, 7)
        pair = jnp.stack([coarse, notes[:, 1] - coarse], axis=1)
        return moe(
            sp_count,
            normed,
            mixed,
            spots.reshape(sp_count, 1, tp_count * tok_dev),
            pair.reshape(sp_count, 2, tp_count * tok_dev),
            capacity,
            w_gate,
            w_up,
            w_down,
        )
    flat_routes = routes.reshape(-1)
    one_hot = (flat_routes[:, None] == jnp.arange(sp_count, dtype=jnp.int32)[None, :]).astype(
        jnp.int32
    )
    earlier = jnp.cumsum(one_hot, axis=0) - one_hot
    slot_index = jnp.sum(earlier * one_hot, axis=1)
    target = flat_routes * capacity + slot_index
    selector = (
        jnp.arange(sp_count * capacity, dtype=jnp.int32)[:, None] == target[None, :]
    ).astype(jnp.bfloat16)
    selector = jnp.sum(selector.reshape(sp_count * capacity, tok_dev, top), axis=2)
    send_rows = jnp.dot(selector, normed, preferred_element_type=jnp.float32).astype(jnp.bfloat16)
    arrived = lax.all_to_all(send_rows, "sp", split_axis=0, concat_axis=0, tiled=True)
    piece = lax.all_gather(arrived, "tp", axis=0, tiled=True)
    gate = jnp.dot(piece, w_gate[0], preferred_element_type=jnp.float32)
    upper = jnp.dot(piece, w_up[0], preferred_element_type=jnp.float32)
    hidden = (jax.nn.silu(gate) * upper).astype(jnp.bfloat16)
    partial = jnp.dot(hidden, w_down[0], preferred_element_type=jnp.float32).astype(jnp.bfloat16)
    expert_out = lax.psum_scatter(partial, "tp", scatter_dimension=0, tiled=True)
    returned = lax.all_to_all(expert_out, "sp", split_axis=0, concat_axis=0, tiled=True)
    picked = (
        jnp.take(returned, target, axis=0)
        .astype(jnp.float32)
        .reshape(tok_dev, top, returned.shape[1])
    )
    moe_sum = jnp.sum(picked * route_weights[:, :, None], axis=1)
    return (mixed_float_output + moe_sum).astype(jnp.bfloat16)


def solution(mesh):
    placed = (
        P("sp", "tp"),
        P("sp", None),
        P("sp", None),
        P(),
        P(),
        P(None, "tp"),
        P(),
        P(("sp", "tp"), None),
        P(("sp", "tp"), None),
        P(("sp", "tp"), None),
        P("sp", None, "tp"),
        P("sp", None, "tp"),
        P("sp", "tp", None),
    )
    return jax.shard_map(
        local, mesh=mesh, in_specs=placed, out_specs=P(("sp", "tp"), None), check_vma=False
    )
```

```python
import functools

import jax
import jax.numpy as jnp
from jax import lax
from jax.experimental import pallas as pl
from jax.experimental.pallas import tpu as pltpu
from jax.sharding import PartitionSpec as P

GRID_W = 64


EPS = 1e-06
ROPE_BASE = 10000.0
NEG_START = -1e30


def rotate(field, position):
    half = field.shape[-1] // 2
    quarter = half // 2
    freqs = ROPE_BASE ** (-jnp.arange(quarter, dtype=jnp.float32) / quarter)
    grid_row = (position // GRID_W).astype(jnp.float32)
    grid_col = (position % GRID_W).astype(jnp.float32)

    def turn_half(part, coord):
        angle = coord[:, None] * freqs[None, :]
        cosine = jnp.cos(angle)[:, None, :]
        sine = jnp.sin(angle)[:, None, :]
        first, second = (part[..., :quarter], part[..., quarter:])
        return jnp.concatenate(
            [first * cosine - second * sine, second * cosine + first * sine], axis=-1
        )

    return jnp.concatenate(
        [turn_half(field[..., :half], grid_row), turn_half(field[..., half:], grid_col)], axis=-1
    )


def prepare(field, gain, position):
    count = field.shape[0]
    width = gain.shape[0]
    heads_here = field.shape[1] // width
    values_f = field.reshape(count, heads_here, width).astype(jnp.float32)
    scaled = (
        values_f * lax.rsqrt(jnp.mean(values_f * values_f, axis=-1, keepdims=True) + EPS) * gain
    )
    return rotate(scaled, position).reshape(count, heads_here * width).astype(jnp.bfloat16)


def absorb(carry, query_matrix, key_rows, value_rows, scale):
    count = key_rows.shape[0]
    width = 2048 if count > 2048 and count % 2048 == 0 else count
    key_blocks = key_rows.reshape(count // width, width, key_rows.shape[1], key_rows.shape[2])
    value_blocks = value_rows.reshape(
        count // width, width, value_rows.shape[1], value_rows.shape[2]
    )

    def step(state, block):
        run_max, run_sum, run_acc = state
        key_tile_rows, value_tile_rows = block
        scores = (
            jnp.einsum(
                "hxt,ght->hxg", query_matrix, key_tile_rows, preferred_element_type=jnp.float32
            )
            * scale
        )
        new_max = jnp.maximum(run_max, jnp.max(scores, axis=-1))
        weight_tensors = jnp.exp(scores - new_max[..., None]).astype(jnp.bfloat16)
        factor = jnp.exp(run_max - new_max)
        run_sum = run_sum * factor + jnp.sum(weight_tensors.astype(jnp.float32), axis=-1)
        run_acc = run_acc * factor[..., None] + jnp.einsum(
            "zij,jzu->ziu", weight_tensors, value_tile_rows, preferred_element_type=jnp.float32
        )
        return ((new_max, run_sum, run_acc), None)

    result, unused = lax.scan(step, carry, (key_blocks, value_blocks))
    return result


MESH = pl.DeviceIdType.MESH
VMEM_LIMIT = 60 * 1024 * 1024


def greet(partners, count):
    barrier = pltpu.get_barrier_semaphore()
    for where in partners:
        pl.semaphore_signal(barrier, inc=1, device_id=where, device_id_type=MESH)
    pl.semaphore_wait(barrier, count)


def remote(src, dst, send, recv, where):
    return pltpu.make_async_remote_copy(
        src_ref=src, dst_ref=dst, send_sem=send, recv_sem=recv, device_id=where, device_id_type=MESH
    )


def square():
    mine = lax.axis_index("tp")
    return mine, mine + 1 - 2 * lax.rem(mine, 2), lax.rem(mine + 2, 4), 3 - mine


def gather_kernel(n, k_ref, v_ref, n_ref, ko_ref, vo_ref, no_ref, send, recv):
    me = lax.axis_index("sp")
    chips = n // 2
    chip, core = me // 2, lax.rem(me, 2)
    partner = 2 * chip + 1 - core
    has_right, has_left = chip < chips - 1, chip > 0
    right, left = me + 2, me - 2
    barrier = pltpu.get_barrier_semaphore()
    pl.semaphore_signal(barrier, inc=1, device_id={"sp": partner}, device_id_type=MESH)

    @pl.when(has_right)
    def _():
        pl.semaphore_signal(barrier, inc=1, device_id={"sp": right}, device_id_type=MESH)

    @pl.when(has_left)
    def _():
        pl.semaphore_signal(barrier, inc=1, device_id={"sp": left}, device_id_type=MESH)

    pl.semaphore_wait(barrier, 1 + has_right.astype(jnp.int32) + has_left.astype(jnp.int32))

    pairs = ((k_ref, ko_ref), (v_ref, vo_ref), (n_ref, no_ref))

    def block(out, origin):
        rows = out.shape[0] // n
        return out.at[pl.ds(pl.multiple_of(origin * rows, rows), rows)]

    def copies(origin, way, where, own=False):
        return [
            remote(
                ref if own else block(out, origin),
                block(out, origin),
                send.at[origin, way, i],
                recv.at[origin, i],
                {"sp": where},
            )
            for i, (ref, out) in enumerate(pairs)
        ]

    def start(*args, **kw):
        for c in copies(*args, **kw):
            c.start()

    def sent(*args, **kw):
        for c in copies(*args, **kw):
            c.wait_send()

    def arrived(origin):
        for c in copies(origin, 0, partner):
            c.wait_recv()

    @pl.when(has_right)
    def _():
        start(me, 0, right, own=True)

    @pl.when(has_left)
    def _():
        start(me, 2, left, own=True)

    start(me, 1, partner, own=True)
    for ref, out in pairs:
        block(out, me)[...] = ref[...]
    for j in range(1, chips):

        @pl.when(chip - j >= 0)
        def _(origin=me - 2 * j):
            arrived(origin)

            @pl.when(has_right)
            def _():
                start(origin, 0, right)

            start(origin, 1, partner)

        @pl.when(chip + j < chips)
        def _(origin=me + 2 * j):
            arrived(origin)

            @pl.when(has_left)
            def _():
                start(origin, 2, left)

            start(origin, 1, partner)

    for z in range(chips):
        arrived(2 * z + 1 - core)
    sent(me, 1, partner, own=True)

    @pl.when(has_right)
    def _():
        sent(me, 0, right, own=True)

    @pl.when(has_left)
    def _():
        sent(me, 2, left, own=True)

    for j in range(1, chips):

        @pl.when(chip - j >= 0)
        def _(origin=me - 2 * j):
            @pl.when(has_right)
            def _():
                sent(origin, 0, right)

            sent(origin, 1, partner)

        @pl.when(chip + j < chips)
        def _(origin=me + 2 * j):
            @pl.when(has_left)
            def _():
                sent(origin, 2, left)

            sent(origin, 1, partner)


def in_vmem(count):
    return [pl.BlockSpec(memory_space=pltpu.VMEM)] * count


def params(number):
    return pltpu.CompilerParams(
        collective_id=number, has_side_effects=True, vmem_limit_bytes=VMEM_LIMIT
    )


def gather_rows(n, own_keys, own_values, notes):
    arrays = (own_keys, own_values, notes)
    return pl.pallas_call(
        functools.partial(gather_kernel, n),
        out_shape=tuple(
            jax.ShapeDtypeStruct((n * a.shape[0], a.shape[1]), a.dtype) for a in arrays
        ),
        in_specs=in_vmem(3),
        out_specs=tuple(in_vmem(3)),
        scratch_shapes=[pltpu.SemaphoreType.DMA((n, 3, 3)), pltpu.SemaphoreType.DMA((n, 3))],
        compiler_params=params(0),
        name="gather_rows",
    )(*arrays)


def project_kernel(
    attn_ref, w_ref, n_ref, out_ref, no_ref, held, stage, send, recv, give, take, tell, told
):
    mine, across, along, corner = square()
    rows, width = attn_ref.shape
    half = rows // 2
    share = out_ref.shape[0]
    greet([{"tp": across}, {"tp": along}, {"tp": corner}], 3)
    first = [
        remote(attn_ref, held.at[mine], send.at[0], recv.at[0], {"tp": across}),
        remote(attn_ref, held.at[mine], send.at[1], recv.at[1], {"tp": along}),
    ]
    for c in first:
        c.start()
    notes = [
        remote(n_ref, no_ref.at[mine], tell.at[i], told.at[i], {"tp": p})
        for i, p in enumerate((corner, across, along))
    ]
    for c in notes:
        c.start()
    no_ref[mine] = n_ref[...]
    top, low = pl.ds(0, half), pl.ds(half, half)
    second = [
        remote(held.at[across, top], held.at[across, top], send.at[2], recv.at[2], {"tp": along}),
        remote(held.at[along, low], held.at[along, low], send.at[3], recv.at[3], {"tp": across}),
    ]

    def term(rows_here, owner):
        part = w_ref[pl.ds(pl.multiple_of(owner * width, width), width), :]
        return jnp.dot(rows_here, part, preferred_element_type=jnp.float32)

    total = term(attn_ref[...], mine)
    first[0].wait_recv()
    second[0].start()
    first[1].wait_recv()
    second[1].start()
    total += term(held[across], across)
    total += term(held[along], along)
    for c in second:
        c.wait_recv()
    total += term(held[corner], corner)
    stage[...] = total.astype(stage.dtype)
    columns = pl.ds(pl.multiple_of(mine * width, width), width)

    def piece(owner):
        return pl.ds(pl.multiple_of(owner * share, share), share)

    back = [
        remote(stage.at[piece(p)], out_ref.at[:, columns], give.at[i], take.at[i], {"tp": p})
        for i, p in enumerate((corner, across, along))
    ]
    for c in back:
        c.start()
    out_ref[:, columns] = stage[piece(mine), :]
    for c in back + notes:
        c.wait()
    for c in first + second:
        c.wait_send()


def project(attn, out_proj, notes, share):
    rows, width = attn.shape
    parts = out_proj.shape[0] // width
    return pl.pallas_call(
        project_kernel,
        out_shape=(
            jax.ShapeDtypeStruct((share, out_proj.shape[1] * parts), jnp.bfloat16),
            jax.ShapeDtypeStruct((parts,) + notes.shape, notes.dtype),
        ),
        in_specs=in_vmem(3),
        out_specs=tuple(in_vmem(2)),
        scratch_shapes=[
            pltpu.VMEM((parts, rows, width), jnp.bfloat16),
            pltpu.VMEM((rows, out_proj.shape[1]), jnp.bfloat16),
            pltpu.SemaphoreType.DMA((4,)),
            pltpu.SemaphoreType.DMA((4,)),
            pltpu.SemaphoreType.DMA((3,)),
            pltpu.SemaphoreType.DMA((3,)),
            pltpu.SemaphoreType.DMA((3,)),
            pltpu.SemaphoreType.DMA((3,)),
        ],
        compiler_params=params(1),
        name="project",
    )(attn, out_proj, notes)


def visit(chip, chips, step):
    near = jnp.minimum(chip, chips - 1 - chip)
    swing = chip + ((step + 1) // 2) * (1 - 2 * lax.rem(step, 2))
    up = chip < chips - 1 - chip
    tail = jnp.where(up, chip + (step - near), chip - (step - near))
    return jnp.where(step <= 2 * near, swing, tail)


def wide(value):
    return value.astype(jnp.float32)


def moe_kernel(
    n, cuts, x_ref, slot_ref, part_ref, wg_ref, wu_ref, wd_ref, out_ref,
    tok, wg, wu, wd, picked, hid, wsel, held, own, give, take,
    low, high, from_x, from_y, to_y, to_x, last_y, last_x, acc, zsend, zrecv,
    load, zs, zr, sq_s, sq_r, pd_s, pd_r, tk_s, tk_r, hop_s, hop_r, hz_s, hz_r,
):
    me = lax.axis_index("sp")
    chips = n // 2
    chip, core = me // 2, lax.rem(me, 2)
    other = 1 - core
    partner = {"sp": 2 * chip + other}
    mine, across, along, corner = square()
    x, y = lax.rem(mine, 2), mine // 2
    share, depth = x_ref.shape
    units = wg.shape[1]
    group = 4 * share
    slots = wsel.shape[3] // 2
    width = depth // cuts
    half = width // 2
    steps = chips * cuts

    def column(k):
        return pl.ds(pl.multiple_of(k * width, width), width)

    loads = [
        pltpu.make_async_copy(wg_ref.at[0], wg, load.at[0]),
        pltpu.make_async_copy(wu_ref.at[0], wu, load.at[1]),
    ] + [
        pltpu.make_async_copy(wd_ref.at[0, :, pl.ds(q * width, width)], wd.at[q], load.at[2 + q])
        for q in range(cuts)
    ]
    for c in loads:
        c.start()

    barrier = pltpu.get_barrier_semaphore()

    def greet_one(where):
        pl.semaphore_signal(barrier, inc=1, device_id=where, device_id_type=MESH)

    greet_one(partner)
    greet_one({"tp": across})
    greet_one({"tp": along})
    for d in range(1, chips):
        greet_one({"sp": 2 * lax.rem(chip + d, chips) + core})
    pl.semaphore_wait(barrier, chips + 2)

    has_right, has_left = chip < chips - 1, chip > 0

    def cols(h):
        return pl.ds(pl.multiple_of(h * (depth // 2), depth // 2), depth // 2)

    def own_half(h):
        return x_ref.at[:, cols(h)]

    def along_z(p, h, way, first=False):
        block = tok.at[p, core, h, mine]
        to = 2 * (chip + 1 - 2 * way) + core
        return remote(
            own_half(h) if first else block, block, zs.at[p, h, way], zr.at[p, h], {"sp": to}
        )

    upper, lower = pl.ds(0, share // 2), pl.ds(share // 2, share // 2)

    def pass_on(p, h, way, first=False):
        block = tok.at[p, core, h]
        start = own_half(h) if first else block.at[mine]
        src, dst, where = (
            (start, block.at[mine], across),
            (start, block.at[mine], along),
            (block.at[across, upper], block.at[across, upper], along),
            (block.at[along, lower], block.at[along, lower], across),
        )[way]
        return remote(src, dst, sq_s.at[p, h, way], sq_r.at[p, h, way], {"tp": where})

    def arrive(p, h, way):
        block = tok.at[p, core, h]
        dst = (
            block.at[across],
            block.at[along],
            block.at[corner, upper],
            block.at[corner, lower],
        )[way]
        remote(dst, dst, sq_s.at[p, h, way], sq_r.at[p, h, way], {"tp": across}).wait_recv()

    def hand(p, h, t, first=False):
        block = tok.at[p, core, h, t]
        src = own_half(h) if first else block
        return remote(src, block, pd_s.at[p, h, t], pd_r.at[p, h, t], partner)

    def handed(p, h, t):
        block = tok.at[p, other, h, t]
        remote(block, block, pd_s.at[p, h, t], pd_r.at[p, h, t], partner).wait_recv()

    for h in range(2):
        pass_on(chip, h, 0, True).start()
        pass_on(chip, h, 1, True).start()

        @pl.when(has_right)
        def _():
            along_z(chip, h, 0, True).start()

        @pl.when(has_left)
        def _():
            along_z(chip, h, 1, True).start()

        hand(chip, h, mine, True).start()
        tok[chip, core, h, mine] = x_ref[:, cols(h)]

    def part(u):
        return visit(chip, chips, u // 2), lax.rem(u, 2)

    def finish(u):
        p, h = part(u)
        arrive(p, h, 2)
        arrive(p, h, 3)
        hand(p, h, corner).start()

    def expert(p):
        for h in range(2):
            for t in range(4):
                handed(p, h, t)
        for side in range(2):
            spot = slot_ref[2 * p + side]
            hit = lax.broadcasted_iota(jnp.int32, (slots, group), 0) == spot
            pick = jnp.where(hit, 1.0, 0.0).astype(tok.dtype)
            parts = part_ref[2 * p + side]
            for i in range(2):
                turned = jnp.transpose(jnp.where(hit, parts[i : i + 1], 0.0))
                wsel[p, side, :, i * slots : (i + 1) * slots] = turned.astype(wsel.dtype)
            for h in range(2):
                block = tok[p, side, h].reshape(group, depth // 2)
                rows = jnp.dot(pick, block, preferred_element_type=jnp.float32)
                picked[side * slots : (side + 1) * slots, cols(h)] = rows.astype(picked.dtype)

        @pl.loop(0, units // 512)
        def _(u):
            some = pl.ds(pl.multiple_of(u * 512, 512), 512)
            gate = jnp.dot(picked[...], wg[:, some], preferred_element_type=jnp.float32)
            rise = jnp.dot(picked[...], wu[:, some], preferred_element_type=jnp.float32)
            hid[p, :, some] = (jax.nn.silu(gate) * rise).astype(hid.dtype)

    def forward(u):
        p, h = part(u)
        arrive(p, h, 0)
        pass_on(p, h, 2).start()
        hand(p, h, across).start()
        arrive(p, h, 1)
        pass_on(p, h, 3).start()
        hand(p, h, along).start()

    last = 2 * chips - 1

    def passes(p):
        return ((p < chip) & has_right) | ((p > chip) & has_left)

    def relay(u):
        p, h = part(u)

        @pl.when(passes(p))
        def _():
            along_z(p, h, 0).wait_recv()

        @pl.when((p < chip) & has_right)
        def _():
            along_z(p, h, 0).start()

        @pl.when((p > chip) & has_left)
        def _():
            along_z(p, h, 1).start()

    def open_up(u):
        p, h = part(u)

        @pl.when(jnp.logical_not(passes(p)))
        def _():
            along_z(p, h, 0).wait_recv()

        pass_on(p, h, 0).start()
        pass_on(p, h, 1).start()
        hand(p, h, mine).start()

    relay(2)
    open_up(2)

    @pl.loop(0, last)
    def _(u):
        forward(u)

        @pl.when(u + 4 <= last)
        def _():
            relay(u + 4)

        @pl.when(u == 0)
        def _():
            relay(3)

        @pl.when(u + 3 <= last)
        def _():
            open_up(u + 3)

        @pl.when(u == 0)
        def _():
            for c in loads:
                c.wait()

        @pl.when((u == 4) | ((u > 4) & (lax.rem(u, 2) == 1)))
        def _():
            j = (u - 3) // 2
            finish(2 * j)
            finish(2 * j + 1)
            expert(visit(chip, chips, j))

    def plane_of(k):
        return visit(chip, chips, lax.rem(k // cuts + 1, chips))

    def swap(k):
        return remote(give.at[k], take.at[k], tk_s.at[k], tk_r.at[k], partner)

    def hop(k, way):
        src, dst, where = (
            (low.at[k, 1 - x], from_x.at[k], across),
            (high.at[k, 1 - y], from_y.at[k], along),
            (to_y.at[k], last_y.at[k], along),
            (to_x.at[k], last_x.at[k], across),
        )[way]
        return remote(src, dst, hop_s.at[k, way], hop_r.at[k, way], {"tp": where})

    def home(k):
        p, q = plane_of(k), lax.rem(k, cuts)
        return remote(
            zsend.at[k], zrecv.at[chip, q], hz_s.at[k], hz_r.at[chip, q], {"sp": 2 * p + core}
        )

    def homed(p, q):
        return remote(zsend.at[0], zrecv.at[p, q], hz_s.at[0], hz_r.at[p, q], partner)

    @pl.loop(0, steps + 5)
    def _(step):
        @pl.when((step >= 1) & (step <= steps))
        def _(k=step - 1):
            swap(k).wait_recv()
            total = own[lax.rem(k, 2)] + wide(take[k])
            cast = total.astype(low.dtype).reshape(4, share, width)
            for t in range(4):
                low[k, t % 2, t // 2] = cast[t, :, :half]
                high[k, t // 2, t % 2] = cast[t, :, half:]
            hop(k, 0).start()
            hop(k, 1).start()

        @pl.when(step < steps)
        def _(k=step):
            @pl.when(k == cuts // 2)
            def _():
                forward(last)

            @pl.when((k == cuts) | (k == 2 * cuts))
            def _():
                late = jnp.where(k == cuts, 0, 1)
                finish(last - 3 + 2 * late)
                finish(last - 2 + 2 * late)
                expert(visit(chip, chips, chips - 2 + late))

            p, q = plane_of(k), lax.rem(k, cuts)
            out = jnp.dot(hid[p], wd[q], preferred_element_type=jnp.float32).astype(held.dtype)
            for side in range(2):
                block = out[side * slots : (side + 1) * slots]
                held[side, :slots] = block
                held[side, slots:] = block

            def spread(side):
                return jnp.dot(wsel[p, side], held[side], preferred_element_type=jnp.float32)

            give[k] = spread(other).astype(give.dtype)
            swap(k).start()
            own[lax.rem(k, 2)] = spread(core)

        @pl.when((step >= 3) & (step < steps + 3))
        def _(k=step - 3):
            hop(k, 0).wait_recv()
            to_y[k] = (wide(low[k, x, 1 - y]) + wide(from_x[k, 1 - y])).astype(to_y.dtype)
            hop(k, 2).start()
            hop(k, 1).wait_recv()
            to_x[k] = (wide(high[k, y, 1 - x]) + wide(from_y[k, 1 - x])).astype(to_x.dtype)
            hop(k, 3).start()

        @pl.when(step >= 5)
        def _(k=step - 5):
            hop(k, 2).wait_recv()
            left = wide(low[k, x, y]) + wide(from_x[k, y]) + wide(last_y[k])
            hop(k, 3).wait_recv()
            right = wide(high[k, y, x]) + wide(from_y[k, x]) + wide(last_x[k])

            @pl.when(k < steps - cuts)
            def _():
                zsend[k, :, :half] = left.astype(zsend.dtype)
                zsend[k, :, half:] = right.astype(zsend.dtype)
                home(k).start()

            @pl.when(k >= steps - cuts)
            def _():
                acc[lax.rem(k, cuts), :, :half] = left
                acc[lax.rem(k, cuts), :, half:] = right

    @pl.loop(0, cuts)
    def _(q):
        total = acc[q]
        for d in range(1, chips):
            p = lax.rem(chip + d, chips)
            homed(p, q).wait_recv()
            total += wide(zrecv[p, q])
        out_ref[:, column(q)] = total

    @pl.loop(0, 2 * chips)
    def _(u):
        p, h = u // 2, lax.rem(u, 2)
        for way in range(4):
            pass_on(p, h, way).wait_send()
            hand(p, h, way).wait_send()

        @pl.when((p <= chip) & has_right)
        def _():
            along_z(p, h, 0).wait_send()

        @pl.when((p >= chip) & has_left)
        def _():
            along_z(p, h, 1).wait_send()

    @pl.loop(0, steps)
    def _(k):
        swap(k).wait_send()
        for way in range(4):
            hop(k, way).wait_send()

        @pl.when(k < steps - cuts)
        def _():
            home(k).wait_send()


def moe(n, normed, slot_rows, weight_rows, capacity, w_gate, w_up, w_down, cuts=4):
    share, depth = normed.shape
    units = w_gate.shape[2]
    chips = n // 2
    kind = normed.dtype
    width = depth // cuts
    half = width // 2
    steps = chips * cuts
    group, slots = 4 * share, 4 * capacity
    dma = pltpu.SemaphoreType.DMA

    def room(*extent):
        return pltpu.VMEM(extent, kind)

    def exact(*extent):
        return pltpu.VMEM(extent, jnp.float32)

    return pl.pallas_call(
        functools.partial(moe_kernel, n, cuts),
        out_shape=jax.ShapeDtypeStruct((share, depth), jnp.float32),
        in_specs=in_vmem(3) + [pl.BlockSpec(memory_space=pl.ANY)] * 3,
        out_specs=in_vmem(1)[0],
        scratch_shapes=[
            room(chips, 2, 2, 4, share, depth // 2),
            room(depth, units),
            room(depth, units),
            room(cuts, units, width),
            room(2 * slots, depth),
            room(chips, 2 * slots, units),
            room(chips, 2, group, 2 * slots),
            room(2, 2 * slots, width),
            exact(2, group, width),
            room(steps, group, width),
            room(steps, group, width),
            room(steps, 2, 2, share, half),
            room(steps, 2, 2, share, half),
            room(steps, 2, share, half),
            room(steps, 2, share, half),
            room(steps, share, half),
            room(steps, share, half),
            room(steps, share, half),
            room(steps, share, half),
            exact(cuts, share, width),
            room(steps - cuts, share, width),
            room(chips, cuts, share, width),
            dma((2 + cuts,)),
            dma((chips, 2, 2)),
            dma((chips, 2)),
            dma((chips, 2, 4)),
            dma((chips, 2, 4)),
            dma((chips, 2, 4)),
            dma((chips, 2, 4)),
            dma((steps,)),
            dma((steps,)),
            dma((steps, 4)),
            dma((steps, 4)),
            dma((steps,)),
            dma((chips, cuts)),
        ],
        compiler_params=params(2),
        name="moe",
    )(normed, slot_rows, weight_rows, w_gate, w_up, w_down)


def start_state(batch, rows, width):
    return (
        jnp.full((batch, rows), NEG_START, jnp.float32),
        jnp.zeros((batch, rows), jnp.float32),
        jnp.zeros((batch, rows, width), jnp.float32),
    )


def local(
    queries,
    keys,
    values,
    query_gain,
    key_gain,
    out_proj,
    expert_norm_scale,
    residual,
    routes,
    route_weights,
    w_gate,
    w_up,
    w_down,
):
    head_size = query_gain.shape[0]
    tok_sp = queries.shape[0]
    tp_count = lax.axis_size("tp")
    sp_count = lax.axis_size("sp")
    heads_dev = queries.shape[1] // head_size
    all_heads = heads_dev * tp_count
    kv_heads = keys.shape[1] // head_size
    group = all_heads // kv_heads
    scale = head_size ** (-0.5)
    tp_index = lax.axis_index("tp")
    sp_index = lax.axis_index("sp")
    position = sp_index * tok_sp + jnp.arange(tok_sp, dtype=jnp.int32)
    q_rot = prepare(queries, query_gain, position)
    shared_value_head = tp_index * heads_dev // group
    own_keys = prepare(
        lax.dynamic_slice_in_dim(keys, shared_value_head * head_size, head_size, 1),
        key_gain,
        position,
    )
    own_values = lax.dynamic_slice_in_dim(values, shared_value_head * head_size, head_size, 1)
    query_matrix = (
        q_rot.reshape(tok_sp, heads_dev, head_size)
        .transpose(1, 0, 2)
        .reshape(1, heads_dev * tok_sp, head_size)
    )
    tok_dev = residual.shape[0]
    top = routes.shape[1]
    capacity = max(2, 2 * tok_dev * top // sp_count)
    direct = (
        tp_count == 4 and sp_count % 2 == 0 and capacity % 16 == 0 and 2 * tok_dev % 128 == 0
    )
    named = routes[:, :, None] == jnp.arange(sp_count, dtype=jnp.int32)[None, None, :]
    if direct:
        taken = jnp.any(named, axis=1).astype(jnp.int32)
        place = jnp.where(taken > 0, jnp.cumsum(taken, axis=0) - 1, -1).astype(jnp.float32)
        load = jnp.sum(jnp.where(named, route_weights[:, :, None], 0.0), axis=1)
        notes = jnp.concatenate([place, load], axis=0).T
        key_piece, value_piece, notes = gather_rows(sp_count, own_keys, own_values, notes)
    else:
        key_piece = lax.all_gather(own_keys, "sp", axis=0, tiled=True)
        value_piece = lax.all_gather(own_values, "sp", axis=0, tiled=True)
    run_max, run_sum, run_acc = absorb(
        start_state(1, heads_dev * tok_sp, head_size),
        query_matrix,
        key_piece[:, None, :],
        value_piece[:, None, :],
        scale,
    )
    attn = (run_acc / run_sum[..., None]).astype(jnp.bfloat16)
    attn = (
        attn.reshape(heads_dev, tok_sp, head_size)
        .transpose(1, 0, 2)
        .reshape(tok_sp, heads_dev * head_size)
    )
    if direct:
        projected, notes = project(attn, out_proj, notes, tok_dev)
    else:
        columns = jnp.dot(
            lax.all_gather(attn, "tp", axis=1, tiled=True),
            out_proj,
            preferred_element_type=jnp.float32,
        )
        projected = lax.all_to_all(
            columns.astype(jnp.bfloat16), "tp", split_axis=0, concat_axis=1, tiled=True
        )
    mixed_float_output = residual.astype(jnp.float32) + projected.astype(jnp.float32)
    mixed = mixed_float_output.astype(jnp.bfloat16)
    mixed_float_output = mixed.astype(jnp.float32)
    normed = (
        mixed_float_output
        * lax.rsqrt(jnp.mean(mixed_float_output * mixed_float_output, axis=-1, keepdims=True) + EPS)
        * expert_norm_scale
    ).astype(jnp.bfloat16)
    if direct:
        notes = notes.reshape(tp_count, sp_count, sp_count, 2, tok_dev)
        notes = lax.dynamic_index_in_dim(notes, sp_index, 2, keepdims=False)
        notes = notes.transpose(1, 2, 0, 3)
        base = capacity * jnp.arange(tp_count, dtype=jnp.float32)[:, None]
        spots = jnp.where(notes[:, 0] >= 0, notes[:, 0] + base, -1.0).astype(jnp.int32)
        coarse = lax.reduce_precision(notes[:, 1], 8, 7)
        pair = jnp.stack([coarse, notes[:, 1] - coarse], axis=1)
        summed = moe(
            sp_count,
            normed,
            spots.reshape(sp_count, 1, tp_count * tok_dev),
            pair.reshape(sp_count, 2, tp_count * tok_dev),
            capacity,
            w_gate,
            w_up,
            w_down,
        )
        return (mixed_float_output + summed).astype(jnp.bfloat16)
    flat_routes = routes.reshape(-1)
    one_hot = (flat_routes[:, None] == jnp.arange(sp_count, dtype=jnp.int32)[None, :]).astype(
        jnp.int32
    )
    earlier = jnp.cumsum(one_hot, axis=0) - one_hot
    slot_index = jnp.sum(earlier * one_hot, axis=1)
    target = flat_routes * capacity + slot_index
    selector = (
        jnp.arange(sp_count * capacity, dtype=jnp.int32)[:, None] == target[None, :]
    ).astype(jnp.bfloat16)
    selector = jnp.sum(selector.reshape(sp_count * capacity, tok_dev, top), axis=2)
    send_rows = jnp.dot(selector, normed, preferred_element_type=jnp.float32).astype(jnp.bfloat16)
    arrived = lax.all_to_all(send_rows, "sp", split_axis=0, concat_axis=0, tiled=True)
    piece = lax.all_gather(arrived, "tp", axis=0, tiled=True)
    gate = jnp.dot(piece, w_gate[0], preferred_element_type=jnp.float32)
    upper = jnp.dot(piece, w_up[0], preferred_element_type=jnp.float32)
    hidden = (jax.nn.silu(gate) * upper).astype(jnp.bfloat16)
    partial = jnp.dot(hidden, w_down[0], preferred_element_type=jnp.float32).astype(jnp.bfloat16)
    expert_out = lax.psum_scatter(partial, "tp", scatter_dimension=0, tiled=True)
    returned = lax.all_to_all(expert_out, "sp", split_axis=0, concat_axis=0, tiled=True)
    picked = (
        jnp.take(returned, target, axis=0)
        .astype(jnp.float32)
        .reshape(tok_dev, top, returned.shape[1])
    )
    moe_sum = jnp.sum(picked * route_weights[:, :, None], axis=1)
    return (mixed_float_output + moe_sum).astype(jnp.bfloat16)


def solution(mesh):
    placed = (
        P("sp", "tp"),
        P("sp", None),
        P("sp", None),
        P(),
        P(),
        P(None, "tp"),
        P(),
        P(("sp", "tp"), None),
        P(("sp", "tp"), None),
        P(("sp", "tp"), None),
        P("sp", None, "tp"),
        P("sp", None, "tp"),
        P("sp", "tp", None),
    )
    return jax.shard_map(
        local, mesh=mesh, in_specs=placed, out_specs=P(("sp", "tp"), None), check_vma=False
    )
```

```python
import functools

import jax
import jax.numpy as jnp
import numpy as np
from jax import lax
from jax.experimental import pallas as pl
from jax.experimental.pallas import tpu as pltpu
from jax.sharding import PartitionSpec as P

GRID_W = 64


EPS = 1e-06
ROPE_BASE = 10000.0
NEG_START = -1e30


def rotate(field, position):
    half = field.shape[-1] // 2
    quarter = half // 2
    freqs = ROPE_BASE ** (-jnp.arange(quarter, dtype=jnp.float32) / quarter)
    grid_row = (position // GRID_W).astype(jnp.float32)
    grid_col = (position % GRID_W).astype(jnp.float32)

    def turn_half(part, coord):
        angle = coord[:, None] * freqs[None, :]
        cosine = jnp.cos(angle)[:, None, :]
        sine = jnp.sin(angle)[:, None, :]
        first, second = (part[..., :quarter], part[..., quarter:])
        return jnp.concatenate(
            [first * cosine - second * sine, second * cosine + first * sine], axis=-1
        )

    return jnp.concatenate(
        [turn_half(field[..., :half], grid_row), turn_half(field[..., half:], grid_col)], axis=-1
    )


def prepare(field, gain, position):
    count = field.shape[0]
    width = gain.shape[0]
    heads_here = field.shape[1] // width
    values_f = field.reshape(count, heads_here, width).astype(jnp.float32)
    scaled = (
        values_f * lax.rsqrt(jnp.mean(values_f * values_f, axis=-1, keepdims=True) + EPS) * gain
    )
    return rotate(scaled, position).reshape(count, heads_here * width).astype(jnp.bfloat16)


def absorb(carry, query_matrix, key_rows, value_rows, scale):
    count = key_rows.shape[0]
    width = 2048 if count > 2048 and count % 2048 == 0 else count
    key_blocks = key_rows.reshape(count // width, width, key_rows.shape[1], key_rows.shape[2])
    value_blocks = value_rows.reshape(
        count // width, width, value_rows.shape[1], value_rows.shape[2]
    )

    def step(state, block):
        run_max, run_sum, run_acc = state
        key_tile_rows, value_tile_rows = block
        scores = (
            jnp.einsum(
                "hxt,ght->hxg", query_matrix, key_tile_rows, preferred_element_type=jnp.float32
            )
            * scale
        )
        new_max = jnp.maximum(run_max, jnp.max(scores, axis=-1))
        weight_tensors = jnp.exp(scores - new_max[..., None]).astype(jnp.bfloat16)
        factor = jnp.exp(run_max - new_max)
        run_sum = run_sum * factor + jnp.sum(weight_tensors.astype(jnp.float32), axis=-1)
        run_acc = run_acc * factor[..., None] + jnp.einsum(
            "zij,jzu->ziu", weight_tensors, value_tile_rows, preferred_element_type=jnp.float32
        )
        return ((new_max, run_sum, run_acc), None)

    result, unused = lax.scan(step, carry, (key_blocks, value_blocks))
    return result


MESH = pl.DeviceIdType.MESH
VMEM_LIMIT = 60 * 1024 * 1024


def greet(partners, count):
    barrier = pltpu.get_barrier_semaphore()
    for where in partners:
        pl.semaphore_signal(barrier, inc=1, device_id=where, device_id_type=MESH)
    pl.semaphore_wait(barrier, count)


def remote(src, dst, send, recv, where):
    return pltpu.make_async_remote_copy(
        src_ref=src, dst_ref=dst, send_sem=send, recv_sem=recv, device_id=where, device_id_type=MESH
    )


def square():
    mine = lax.axis_index("tp")
    return mine, mine + 1 - 2 * lax.rem(mine, 2), lax.rem(mine + 2, 4), 3 - mine


def in_vmem(count):
    return [pl.BlockSpec(memory_space=pltpu.VMEM)] * count


def params(number):
    return pltpu.CompilerParams(
        collective_id=number, has_side_effects=True, vmem_limit_bytes=VMEM_LIMIT
    )


def turn_tables(width, rows):
    quarter = width // 4
    freqs = ROPE_BASE ** (-np.arange(quarter, dtype=np.float32) / np.float32(quarter))
    zero = np.zeros((max(rows, GRID_W), quarter), np.float32)

    def table(count, blocks):
        angle = np.arange(count, dtype=np.float32)[:, None] * freqs.astype(np.float32)[None, :]
        kinds = {"c": np.cos(angle), "s": np.sin(angle), "m": -np.sin(angle), "0": zero[:count]}
        return np.stack([np.concatenate([kinds[k] for k in b], axis=1) for b in blocks])

    by_col = table(GRID_W, ("00cc", "00m0", "000s"))
    by_row = table(rows, ("cc00", "m000", "0s00"))
    return by_col.astype(np.float32), by_row.astype(np.float32)


def attend_kernel(
    n, q_ref, k_ref, v_ref, qg_ref, kg_ref, col_ref, row_ref, res_ref, gain_ref, name_ref, share_ref, w_ref,
    mixed_ref, normed_ref, notes_ref,
    w, kv, qs, top, acc, held, total, stage, proj, sheet,
    load, zs, zr, xs, xr, ds, dr, ns, nr, fs, fr, give, take, tell, told,
):
    me = lax.axis_index("sp")
    chips = n // 2
    chip, core = me // 2, lax.rem(me, 2)
    other = 1 - core
    partner = {"sp": 2 * chip + other}
    mine, across, along, corner = square()
    x = lax.rem(mine, 2)
    rows, width = q_ref.shape
    size = qg_ref.shape[1]
    heads = width // size
    pairs = heads // 2
    share = rows // 4
    keys_half = rows // 2
    fetch = pltpu.make_async_copy(w_ref, w, load.at[0])
    fetch.start()

    barrier = pltpu.get_barrier_semaphore()
    peers = [lax.rem(me + d, n) for d in range(1, n)]
    for p in peers:
        pl.semaphore_signal(barrier, inc=1, device_id={"sp": p}, device_id_type=MESH)
    for p in (across, along, corner):
        pl.semaphore_signal(barrier, inc=1, device_id={"tp": p}, device_id_type=MESH)

    def turned(part, gain_row, g):
        values = part.astype(jnp.float32)
        mean = jnp.mean(values * values, axis=-1, keepdims=True)
        scaled = values * lax.rsqrt(mean + EPS) * gain_row
        grid_row = pl.ds(me * (rows // GRID_W) + g, 1)
        turn = [col_ref[i] + row_ref[i, grid_row] for i in range(3)]
        return (
            scaled * turn[0]
            + pltpu.roll(scaled, size - size // 4, 1) * turn[1]
            + pltpu.roll(scaled, size // 4, 1) * turn[2]
        ).astype(jnp.bfloat16)

    kv_heads = k_ref.shape[1] // size
    kv_head = mine * kv_heads // 4
    at = pl.ds(pl.multiple_of(kv_head * size, size), size)
    for g in range(rows // GRID_W):
        span = pl.ds(g * GRID_W, GRID_W)
        side, low = (g * GRID_W) // keys_half, (g * GRID_W) % keys_half
        place = pl.ds(low, GRID_W)
        kv[chip, core, side, 0, place] = turned(k_ref[span, at], kg_ref[...], g)
        kv[chip, core, side, 1, place] = v_ref[span, at]
    lanes = lax.broadcasted_iota(jnp.int32, (n, 2 * share), 1)
    expert = lax.broadcasted_iota(jnp.int32, (n, 2 * share), 0)
    first_one, second_one = name_ref[0:1] == expert, name_ref[1:2] == expert
    taken = jnp.where((first_one | second_one) & (lanes < share), 1.0, 0.0)
    before = lax.broadcasted_iota(jnp.int32, (2 * share, 2 * share), 0)
    after = lax.broadcasted_iota(jnp.int32, (2 * share, 2 * share), 1)
    ladder = jnp.where(before < after, 1.0, 0.0).astype(jnp.bfloat16)
    slot = jnp.dot(taken.astype(jnp.bfloat16), ladder, preferred_element_type=jnp.float32)
    weight = jnp.where(first_one, share_ref[0:1], 0.0) + jnp.where(second_one, share_ref[1:2], 0.0)
    sheet[me] = jnp.where(lanes < share, jnp.where(taken > 0, slot, -1.0), weight)

    pl.semaphore_wait(barrier, n + 2)

    def to_plane(p):
        block = kv.at[chip, core, x]
        return remote(block, block, zs.at[p], zr.at[chip], {"sp": 2 * p + core})

    def from_plane(p):
        block = kv.at[p, core, x]
        remote(block, block, zs.at[p], zr.at[p], partner).wait_recv()

    def sideways(p):
        block = kv.at[p, core, x]
        return remote(block, block, xs.at[p], xr.at[p], {"tp": across})

    def from_side(p):
        block = kv.at[p, core, 1 - x]
        remote(block, block, xs.at[p], xr.at[p], partner).wait_recv()

    def hand(p, side):
        block = kv.at[p, core, side]
        return remote(block, block, ds.at[p, side], dr.at[p, side], partner)

    def handed(p, side):
        block = kv.at[p, other, side]
        remote(block, block, ds.at[p, side], dr.at[p, side], partner).wait_recv()

    for j in range(1, chips):

        @pl.when(chip + j < chips)
        def _():
            to_plane(chip + j).start()

        @pl.when(chip - j >= 0)
        def _():
            to_plane(chip - j).start()

    for side in range(2):
        hand(chip, side).start()
    inform = [
        remote(sheet.at[me], sheet.at[me], ns.at[d], nr.at[d], {"sp": p})
        for d, p in enumerate(peers)
    ]
    for c in inform:
        c.start()

    @pl.loop(0, heads)
    def _(h):
        @pl.loop(0, rows // GRID_W)
        def _(g):
            span = pl.ds(pl.multiple_of(g * GRID_W, GRID_W), GRID_W)
            block = q_ref[span, pl.ds(pl.multiple_of(h * size, size), size)]
            qs[h, span] = turned(block, qg_ref[...], g)

        top[h] = jnp.full(top.shape[1:], NEG_START, jnp.float32)
        acc[h] = jnp.zeros(acc.shape[1:], jnp.float32)

    grade = size ** (-0.5) * 1.4426950408889634

    def first(j, way):
        block = held.at[mine, j]
        where = (across, along)[way]
        return remote(block, block, fs.at[j, way], fr.at[j, way], {"tp": where})

    upper, lower = pl.ds(0, rows // 2), pl.ds(rows // 2, rows // 2)

    def second(j, way):
        block = (held.at[across, j, upper], held.at[along, j, lower])[way]
        where = (along, across)[way]
        return remote(block, block, fs.at[j, 2 + way], fr.at[j, 2 + way], {"tp": where})

    def arrive(j, way):
        block = (
            held.at[across, j],
            held.at[along, j],
            held.at[corner, j, upper],
            held.at[corner, j, lower],
        )[way]
        remote(block, block, fs.at[j, way], fr.at[j, way], partner).wait_recv()

    @pl.loop(0, chips)
    def _(s):
        @pl.when(s + 1 < chips)
        def _():
            p = visit(chip, chips, s + 1)
            from_plane(p)
            sideways(p).start()
            hand(p, x).start()

        p = visit(chip, chips, s)

        @pl.when(s > 0)
        def _():
            from_side(p)
            hand(p, 1 - x).start()

        for side in range(2):
            handed(p, side)

        @pl.loop(0, pairs)
        def _(j):
            for i in range(2):
                h = 2 * j + i
                keys = kv[p, :, :, 0].reshape(2 * rows, size)
                values = kv[p, :, :, 1].reshape(2 * rows, size)
                scores = lax.dot_general(
                    qs[h], keys, (((1,), (1,)), ((), ())), preferred_element_type=jnp.float32
                )
                old = top[h]
                new = jnp.maximum(old, jnp.max(scores, axis=1, keepdims=True))
                top[h] = new
                weights = jnp.exp2((scores - new[:, :1]) * grade).astype(jnp.bfloat16)
                full = jnp.concatenate([values, jnp.ones_like(values)], axis=1)
                grown = jnp.dot(weights, full, preferred_element_type=jnp.float32)
                factor = jnp.exp2((old - new) * grade)
                acc[h] = acc[h] * jnp.concatenate([factor, factor], axis=1) + grown

            @pl.when(s == chips - 1)
            def _():
                for i in range(2):
                    done = acc[2 * j + i]
                    ratio = done[:, :size] / done[:, size:]
                    held[mine, j, :, i * size : (i + 1) * size] = ratio.astype(held.dtype)
                first(j, 0).start()
                first(j, 1).start()

        @pl.when(s == chips - 2)
        def _():
            for c in inform:
                c.wait_recv()
            notes_ref[mine] = sheet[...]
            for i, p in enumerate((corner, across, along)):
                remote(sheet, notes_ref.at[mine], tell.at[i], told.at[i], {"tp": p}).start()

    fetch.wait()

    def term(owner, j):
        start = pl.multiple_of(owner * width + j * 2 * size, 2 * size)
        part = w[pl.ds(start, 2 * size), :]
        total[...] += jnp.dot(held[owner, j], part, preferred_element_type=jnp.float32)

    total[...] = jnp.zeros_like(total)

    @pl.loop(0, pairs)
    def _(j):
        term(mine, j)

    @pl.loop(0, pairs)
    def _(j):
        arrive(j, 0)
        second(j, 0).start()
        arrive(j, 1)
        second(j, 1).start()
        term(across, j)
        term(along, j)

    @pl.loop(0, pairs)
    def _(j):
        arrive(j, 2)
        arrive(j, 3)
        term(corner, j)

    stage[...] = total[...].astype(stage.dtype)
    columns = pl.ds(pl.multiple_of(mine * width, width), width)

    def piece(owner):
        return pl.ds(pl.multiple_of(owner * share, share), share)

    back = [
        remote(stage.at[piece(p)], proj.at[:, columns], give.at[i], take.at[i], {"tp": p})
        for i, p in enumerate((corner, across, along))
    ]
    for c in back:
        c.start()
    proj[:, columns] = stage[piece(mine), :]
    for c in back:
        c.wait()
    mixed = (res_ref[...].astype(jnp.float32) + proj[...].astype(jnp.float32)).astype(mixed_ref.dtype)
    mixed_ref[...] = mixed
    mixed = mixed.astype(jnp.float32)
    mean = jnp.mean(mixed * mixed, axis=-1, keepdims=True)
    normed_ref[...] = (mixed * lax.rsqrt(mean + EPS) * gain_ref[...]).astype(normed_ref.dtype)

    for i, p in enumerate((corner, across, along)):
        remote(sheet, notes_ref.at[mine], tell.at[i], told.at[i], {"tp": p}).wait()
    for c in inform:
        c.wait_send()
    for d in range(1, chips):
        p = lax.rem(chip + d, chips)
        to_plane(p).wait_send()
        sideways(p).wait_send()
    for p in range(chips):
        for side in range(2):
            hand(p, side).wait_send()
    for j in range(pairs):
        for way in range(2):
            first(j, way).wait_send()
            second(j, way).wait_send()


def attend(n, queries, keys, values, query_gain, key_gain, residual, gain, names, shares, out_proj):
    rows, width = queries.shape
    size = query_gain.shape[0]
    heads = width // size
    share, depth = residual.shape
    chips = n // 2
    kind = queries.dtype
    by_col, by_row = turn_tables(size, n * rows // GRID_W)
    dma = pltpu.SemaphoreType.DMA
    exact = jnp.float32
    return pl.pallas_call(
        functools.partial(attend_kernel, n),
        out_shape=(
            jax.ShapeDtypeStruct((share, depth), kind),
            jax.ShapeDtypeStruct((share, depth), kind),
            jax.ShapeDtypeStruct((4, n, n, 2 * share), exact),
        ),
        in_specs=in_vmem(11) + [pl.BlockSpec(memory_space=pl.ANY)],
        out_specs=tuple(in_vmem(3)),
        scratch_shapes=[
            pltpu.VMEM(out_proj.shape, kind),
            pltpu.VMEM((chips, 2, 2, 2, rows // 2, size), kind),
            pltpu.VMEM((heads, rows, size), kind),
            pltpu.VMEM((heads, rows, size), exact),
            pltpu.VMEM((heads, rows, 2 * size), exact),
            pltpu.VMEM((4, heads // 2, rows, 2 * size), kind),
            pltpu.VMEM((rows, width), exact),
            pltpu.VMEM((rows, width), kind),
            pltpu.VMEM((share, depth), kind),
            pltpu.VMEM((n, n, 2 * share), exact),
            dma((1,)),
            dma((chips,)),
            dma((chips,)),
            dma((chips,)),
            dma((chips,)),
            dma((chips, 2)),
            dma((chips, 2)),
            dma((n - 1,)),
            dma((n - 1,)),
            dma((heads // 2, 4)),
            dma((heads // 2, 4)),
            dma((3,)),
            dma((3,)),
            dma((3,)),
            dma((3,)),
        ],
        compiler_params=params(1),
        name="attend",
    )(
        queries,
        keys,
        values,
        query_gain[None, :],
        key_gain[None, :],
        jnp.asarray(by_col),
        jnp.asarray(by_row),
        residual,
        gain[None, :],
        names,
        shares,
        out_proj,
    )


def visit(chip, chips, step):
    near = jnp.minimum(chip, chips - 1 - chip)
    swing = chip + ((step + 1) // 2) * (1 - 2 * lax.rem(step, 2))
    up = chip < chips - 1 - chip
    tail = jnp.where(up, chip + (step - near), chip - (step - near))
    return jnp.where(step <= 2 * near, swing, tail)


def wide(value):
    return value.astype(jnp.float32)


def moe_kernel(
    n, cuts, x_ref, note_ref, wg_ref, wu_ref, wd_ref, out_ref,
    tok, wg, wu, wd, picked, hid, wsel, held, own, give, take,
    low, high, from_x, from_y, to_y, to_x, last_y, last_x, acc, zsend, zrecv,
    load, zs, zr, sq_s, sq_r, pd_s, pd_r, tk_s, tk_r, hop_s, hop_r, hz_s, hz_r,
):
    me = lax.axis_index("sp")
    chips = n // 2
    chip, core = me // 2, lax.rem(me, 2)
    other = 1 - core
    partner = {"sp": 2 * chip + other}
    mine, across, along, corner = square()
    x, y = lax.rem(mine, 2), mine // 2
    share, depth = x_ref.shape
    units = wg.shape[1]
    group = 4 * share
    slots = wsel.shape[3] // 2
    width = depth // cuts
    half = width // 2
    steps = chips * cuts

    def column(k):
        return pl.ds(pl.multiple_of(k * width, width), width)

    loads = [
        pltpu.make_async_copy(wg_ref.at[0], wg, load.at[0]),
        pltpu.make_async_copy(wu_ref.at[0], wu, load.at[1]),
    ] + [
        pltpu.make_async_copy(wd_ref.at[0, :, pl.ds(q * width, width)], wd.at[q], load.at[2 + q])
        for q in range(cuts)
    ]
    for c in loads:
        c.start()

    barrier = pltpu.get_barrier_semaphore()

    def greet_one(where):
        pl.semaphore_signal(barrier, inc=1, device_id=where, device_id_type=MESH)

    greet_one(partner)
    greet_one({"tp": across})
    greet_one({"tp": along})
    for d in range(1, chips):
        greet_one({"sp": 2 * lax.rem(chip + d, chips) + core})
    pl.semaphore_wait(barrier, chips + 2)

    has_right, has_left = chip < chips - 1, chip > 0

    def cols(h):
        return pl.ds(pl.multiple_of(h * (depth // 2), depth // 2), depth // 2)

    def own_half(h):
        return x_ref.at[:, cols(h)]

    def along_z(p, h, way, first=False):
        block = tok.at[p, core, h, mine]
        to = 2 * (chip + 1 - 2 * way) + core
        return remote(
            own_half(h) if first else block, block, zs.at[p, h, way], zr.at[p, h], {"sp": to}
        )

    upper, lower = pl.ds(0, share // 2), pl.ds(share // 2, share // 2)

    def pass_on(p, h, way, first=False):
        block = tok.at[p, core, h]
        start = own_half(h) if first else block.at[mine]
        src, dst, where = (
            (start, block.at[mine], across),
            (start, block.at[mine], along),
            (block.at[across, upper], block.at[across, upper], along),
            (block.at[along, lower], block.at[along, lower], across),
        )[way]
        return remote(src, dst, sq_s.at[p, h, way], sq_r.at[p, h, way], {"tp": where})

    def arrive(p, h, way):
        block = tok.at[p, core, h]
        dst = (
            block.at[across],
            block.at[along],
            block.at[corner, upper],
            block.at[corner, lower],
        )[way]
        remote(dst, dst, sq_s.at[p, h, way], sq_r.at[p, h, way], {"tp": across}).wait_recv()

    def hand(p, h, t, first=False):
        block = tok.at[p, core, h, t]
        src = own_half(h) if first else block
        return remote(src, block, pd_s.at[p, h, t], pd_r.at[p, h, t], partner)

    def handed(p, h, t):
        block = tok.at[p, other, h, t]
        remote(block, block, pd_s.at[p, h, t], pd_r.at[p, h, t], partner).wait_recv()

    for h in range(2):
        pass_on(chip, h, 0, True).start()
        pass_on(chip, h, 1, True).start()

        @pl.when(has_right)
        def _():
            along_z(chip, h, 0, True).start()

        @pl.when(has_left)
        def _():
            along_z(chip, h, 1, True).start()

        hand(chip, h, mine, True).start()
        tok[chip, core, h, mine] = x_ref[:, cols(h)]

    def part(u):
        return visit(chip, chips, u // 2), lax.rem(u, 2)

    def finish(u):
        p, h = part(u)
        arrive(p, h, 2)
        arrive(p, h, 3)
        hand(p, h, corner).start()

    def expert(p):
        for h in range(2):
            for t in range(4):
                handed(p, h, t)
        for side in range(2):
            tiles = [note_ref[t, 2 * p + side] for t in range(4)]
            lane = lax.broadcasted_iota(jnp.int32, (n, 2 * share), 1)
            chosen = lax.broadcasted_iota(jnp.int32, (n, 2 * share), 0) == me

            def across_two(even, odd, swap_even):
                moved = pltpu.roll(even if swap_even else odd, share, 1)
                return jnp.where(lane < share, moved, odd) if swap_even else jnp.where(
                    lane < share, even, moved
                )

            def row_of(swap_even):
                parts_two = [across_two(tiles[t], tiles[t + 1], swap_even) for t in (0, 2)]
                picks = [
                    jnp.sum(jnp.where(chosen, v, 0.0), axis=0, keepdims=True) for v in parts_two
                ]
                return jnp.concatenate(picks, axis=1)

            spot = row_of(False)
            base = lax.broadcasted_iota(jnp.int32, (1, group), 1) // share * (slots // 4)
            spot = jnp.where(spot >= 0, spot.astype(jnp.int32) + base, -1)
            weight = row_of(True)
            coarse = weight.astype(jnp.bfloat16).astype(jnp.float32)
            parts = (coarse, weight - coarse)
            hit = lax.broadcasted_iota(jnp.int32, (slots, group), 0) == spot
            pick = jnp.where(hit, 1.0, 0.0).astype(tok.dtype)
            for i in range(2):
                turned = jnp.transpose(jnp.where(hit, parts[i], 0.0))
                wsel[p, side, :, i * slots : (i + 1) * slots] = turned.astype(wsel.dtype)
            for h in range(2):
                block = tok[p, side, h].reshape(group, depth // 2)
                rows = jnp.dot(pick, block, preferred_element_type=jnp.float32)
                picked[side * slots : (side + 1) * slots, cols(h)] = rows.astype(picked.dtype)

        @pl.loop(0, units // 512)
        def _(u):
            some = pl.ds(pl.multiple_of(u * 512, 512), 512)
            gate = jnp.dot(picked[...], wg[:, some], preferred_element_type=jnp.float32)
            rise = jnp.dot(picked[...], wu[:, some], preferred_element_type=jnp.float32)
            hid[p, :, some] = (jax.nn.silu(gate) * rise).astype(hid.dtype)

    def forward(u):
        p, h = part(u)
        arrive(p, h, 0)
        pass_on(p, h, 2).start()
        hand(p, h, across).start()
        arrive(p, h, 1)
        pass_on(p, h, 3).start()
        hand(p, h, along).start()

    last = 2 * chips - 1

    def passes(p):
        return ((p < chip) & has_right) | ((p > chip) & has_left)

    def relay(u):
        p, h = part(u)

        @pl.when(passes(p))
        def _():
            along_z(p, h, 0).wait_recv()

        @pl.when((p < chip) & has_right)
        def _():
            along_z(p, h, 0).start()

        @pl.when((p > chip) & has_left)
        def _():
            along_z(p, h, 1).start()

    def open_up(u):
        p, h = part(u)

        @pl.when(jnp.logical_not(passes(p)))
        def _():
            along_z(p, h, 0).wait_recv()

        pass_on(p, h, 0).start()
        pass_on(p, h, 1).start()
        hand(p, h, mine).start()

    relay(2)
    open_up(2)

    @pl.loop(0, last)
    def _(u):
        forward(u)

        @pl.when(u + 4 <= last)
        def _():
            relay(u + 4)

        @pl.when(u == 0)
        def _():
            relay(3)

        @pl.when(u + 3 <= last)
        def _():
            open_up(u + 3)

        @pl.when(u == 0)
        def _():
            for c in loads:
                c.wait()

        @pl.when((u == 4) | ((u > 4) & (lax.rem(u, 2) == 1)))
        def _():
            j = (u - 3) // 2
            finish(2 * j)
            finish(2 * j + 1)
            expert(visit(chip, chips, j))

    def plane_of(k):
        return visit(chip, chips, lax.rem(k // cuts + 1, chips))

    def swap(k):
        return remote(give.at[k], take.at[k], tk_s.at[k], tk_r.at[k], partner)

    def hop(k, way):
        src, dst, where = (
            (low.at[k, 1 - x], from_x.at[k], across),
            (high.at[k, 1 - y], from_y.at[k], along),
            (to_y.at[k], last_y.at[k], along),
            (to_x.at[k], last_x.at[k], across),
        )[way]
        return remote(src, dst, hop_s.at[k, way], hop_r.at[k, way], {"tp": where})

    def home(k):
        p, q = plane_of(k), lax.rem(k, cuts)
        return remote(
            zsend.at[k], zrecv.at[chip, q], hz_s.at[k], hz_r.at[chip, q], {"sp": 2 * p + core}
        )

    def homed(p, q):
        return remote(zsend.at[0], zrecv.at[p, q], hz_s.at[0], hz_r.at[p, q], partner)

    @pl.loop(0, steps + 5)
    def _(step):
        @pl.when((step >= 1) & (step <= steps))
        def _(k=step - 1):
            swap(k).wait_recv()
            total = own[lax.rem(k, 2)] + wide(take[k])
            cast = total.astype(low.dtype).reshape(4, share, width)
            for t in range(4):
                low[k, t % 2, t // 2] = cast[t, :, :half]
                high[k, t // 2, t % 2] = cast[t, :, half:]
            hop(k, 0).start()
            hop(k, 1).start()

        @pl.when(step < steps)
        def _(k=step):
            @pl.when(k == cuts // 2)
            def _():
                forward(last)

            @pl.when((k == cuts) | (k == 2 * cuts))
            def _():
                late = jnp.where(k == cuts, 0, 1)
                finish(last - 3 + 2 * late)
                finish(last - 2 + 2 * late)
                expert(visit(chip, chips, chips - 2 + late))

            p, q = plane_of(k), lax.rem(k, cuts)
            out = jnp.dot(hid[p], wd[q], preferred_element_type=jnp.float32).astype(held.dtype)
            for side in range(2):
                block = out[side * slots : (side + 1) * slots]
                held[side, :slots] = block
                held[side, slots:] = block

            def spread(side):
                return jnp.dot(wsel[p, side], held[side], preferred_element_type=jnp.float32)

            give[k] = spread(other).astype(give.dtype)
            swap(k).start()
            own[lax.rem(k, 2)] = spread(core)

        @pl.when((step >= 3) & (step < steps + 3))
        def _(k=step - 3):
            hop(k, 0).wait_recv()
            to_y[k] = (wide(low[k, x, 1 - y]) + wide(from_x[k, 1 - y])).astype(to_y.dtype)
            hop(k, 2).start()
            hop(k, 1).wait_recv()
            to_x[k] = (wide(high[k, y, 1 - x]) + wide(from_y[k, 1 - x])).astype(to_x.dtype)
            hop(k, 3).start()

        @pl.when(step >= 5)
        def _(k=step - 5):
            hop(k, 2).wait_recv()
            left = wide(low[k, x, y]) + wide(from_x[k, y]) + wide(last_y[k])
            hop(k, 3).wait_recv()
            right = wide(high[k, y, x]) + wide(from_y[k, x]) + wide(last_x[k])

            @pl.when(k < steps - cuts)
            def _():
                zsend[k, :, :half] = left.astype(zsend.dtype)
                zsend[k, :, half:] = right.astype(zsend.dtype)
                home(k).start()

            @pl.when(k >= steps - cuts)
            def _():
                acc[lax.rem(k, cuts), :, :half] = left
                acc[lax.rem(k, cuts), :, half:] = right

    @pl.loop(0, cuts)
    def _(q):
        total = acc[q]
        for d in range(1, chips):
            p = lax.rem(chip + d, chips)
            homed(p, q).wait_recv()
            total += wide(zrecv[p, q])
        out_ref[:, column(q)] = total

    @pl.loop(0, 2 * chips)
    def _(u):
        p, h = u // 2, lax.rem(u, 2)
        for way in range(4):
            pass_on(p, h, way).wait_send()
            hand(p, h, way).wait_send()

        @pl.when((p <= chip) & has_right)
        def _():
            along_z(p, h, 0).wait_send()

        @pl.when((p >= chip) & has_left)
        def _():
            along_z(p, h, 1).wait_send()

    @pl.loop(0, steps)
    def _(k):
        swap(k).wait_send()
        for way in range(4):
            hop(k, way).wait_send()

        @pl.when(k < steps - cuts)
        def _():
            home(k).wait_send()


def moe(n, normed, notes, capacity, w_gate, w_up, w_down, cuts=4):
    share, depth = normed.shape
    units = w_gate.shape[2]
    chips = n // 2
    kind = normed.dtype
    width = depth // cuts
    half = width // 2
    steps = chips * cuts
    group, slots = 4 * share, 4 * capacity
    dma = pltpu.SemaphoreType.DMA

    def room(*extent):
        return pltpu.VMEM(extent, kind)

    def exact(*extent):
        return pltpu.VMEM(extent, jnp.float32)

    return pl.pallas_call(
        functools.partial(moe_kernel, n, cuts),
        out_shape=jax.ShapeDtypeStruct((share, depth), jnp.float32),
        in_specs=in_vmem(2) + [pl.BlockSpec(memory_space=pl.ANY)] * 3,
        out_specs=in_vmem(1)[0],
        scratch_shapes=[
            room(chips, 2, 2, 4, share, depth // 2),
            room(depth, units),
            room(depth, units),
            room(cuts, units, width),
            room(2 * slots, depth),
            room(chips, 2 * slots, units),
            room(chips, 2, group, 2 * slots),
            room(2, 2 * slots, width),
            exact(2, group, width),
            room(steps, group, width),
            room(steps, group, width),
            room(steps, 2, 2, share, half),
            room(steps, 2, 2, share, half),
            room(steps, 2, share, half),
            room(steps, 2, share, half),
            room(steps, share, half),
            room(steps, share, half),
            room(steps, share, half),
            room(steps, share, half),
            exact(cuts, share, width),
            room(steps - cuts, share, width),
            room(chips, cuts, share, width),
            dma((2 + cuts,)),
            dma((chips, 2, 2)),
            dma((chips, 2)),
            dma((chips, 2, 4)),
            dma((chips, 2, 4)),
            dma((chips, 2, 4)),
            dma((chips, 2, 4)),
            dma((steps,)),
            dma((steps,)),
            dma((steps, 4)),
            dma((steps, 4)),
            dma((steps,)),
            dma((chips, cuts)),
        ],
        compiler_params=params(2),
        name="moe",
    )(normed, notes, w_gate, w_up, w_down)


def start_state(batch, rows, width):
    return (
        jnp.full((batch, rows), NEG_START, jnp.float32),
        jnp.zeros((batch, rows), jnp.float32),
        jnp.zeros((batch, rows, width), jnp.float32),
    )


def local(
    queries,
    keys,
    values,
    query_gain,
    key_gain,
    out_proj,
    expert_norm_scale,
    residual,
    routes,
    route_weights,
    w_gate,
    w_up,
    w_down,
):
    head_size = query_gain.shape[0]
    tok_sp = queries.shape[0]
    tp_count = lax.axis_size("tp")
    sp_count = lax.axis_size("sp")
    heads_dev = queries.shape[1] // head_size
    all_heads = heads_dev * tp_count
    kv_heads = keys.shape[1] // head_size
    group = all_heads // kv_heads
    scale = head_size ** (-0.5)
    tp_index = lax.axis_index("tp")
    sp_index = lax.axis_index("sp")
    tok_dev = residual.shape[0]
    top = routes.shape[1]
    capacity = max(2, 2 * tok_dev * top // sp_count)
    direct = (
        tp_count == 4
        and sp_count % 2 == 0
        and capacity % 16 == 0
        and 2 * tok_dev % 128 == 0
        and tok_sp % (2 * GRID_W) == 0
        and heads_dev % 2 == 0
        and 2 * heads_dev <= group
        and tok_sp == tp_count * tok_dev
    )
    if direct:
        mixed, normed, notes = attend(
            sp_count,
            queries,
            keys,
            values,
            query_gain,
            key_gain,
            residual,
            expert_norm_scale,
            jnp.tile(routes.T, (1, 2)),
            jnp.tile(route_weights.T, (1, 2)),
            out_proj,
        )
        summed = moe(sp_count, normed, notes, capacity, w_gate, w_up, w_down)
        return (mixed.astype(jnp.float32) + summed).astype(jnp.bfloat16)
    position = sp_index * tok_sp + jnp.arange(tok_sp, dtype=jnp.int32)
    q_rot = prepare(queries, query_gain, position)
    shared_value_head = tp_index * heads_dev // group
    own_keys = prepare(
        lax.dynamic_slice_in_dim(keys, shared_value_head * head_size, head_size, 1),
        key_gain,
        position,
    )
    own_values = lax.dynamic_slice_in_dim(values, shared_value_head * head_size, head_size, 1)
    query_matrix = (
        q_rot.reshape(tok_sp, heads_dev, head_size)
        .transpose(1, 0, 2)
        .reshape(1, heads_dev * tok_sp, head_size)
    )
    key_piece = lax.all_gather(own_keys, "sp", axis=0, tiled=True)
    value_piece = lax.all_gather(own_values, "sp", axis=0, tiled=True)
    run_max, run_sum, run_acc = absorb(
        start_state(1, heads_dev * tok_sp, head_size),
        query_matrix,
        key_piece[:, None, :],
        value_piece[:, None, :],
        scale,
    )
    attn = (run_acc / run_sum[..., None]).astype(jnp.bfloat16)
    attn = (
        attn.reshape(heads_dev, tok_sp, head_size)
        .transpose(1, 0, 2)
        .reshape(tok_sp, heads_dev * head_size)
    )
    columns = jnp.dot(
        lax.all_gather(attn, "tp", axis=1, tiled=True),
        out_proj,
        preferred_element_type=jnp.float32,
    )
    projected = lax.all_to_all(
        columns.astype(jnp.bfloat16), "tp", split_axis=0, concat_axis=1, tiled=True
    )
    mixed_float_output = residual.astype(jnp.float32) + projected.astype(jnp.float32)
    mixed = mixed_float_output.astype(jnp.bfloat16)
    mixed_float_output = mixed.astype(jnp.float32)
    normed = (
        mixed_float_output
        * lax.rsqrt(jnp.mean(mixed_float_output * mixed_float_output, axis=-1, keepdims=True) + EPS)
        * expert_norm_scale
    ).astype(jnp.bfloat16)
    flat_routes = routes.reshape(-1)
    one_hot = (flat_routes[:, None] == jnp.arange(sp_count, dtype=jnp.int32)[None, :]).astype(
        jnp.int32
    )
    earlier = jnp.cumsum(one_hot, axis=0) - one_hot
    slot_index = jnp.sum(earlier * one_hot, axis=1)
    target = flat_routes * capacity + slot_index
    selector = (
        jnp.arange(sp_count * capacity, dtype=jnp.int32)[:, None] == target[None, :]
    ).astype(jnp.bfloat16)
    selector = jnp.sum(selector.reshape(sp_count * capacity, tok_dev, top), axis=2)
    send_rows = jnp.dot(selector, normed, preferred_element_type=jnp.float32).astype(jnp.bfloat16)
    arrived = lax.all_to_all(send_rows, "sp", split_axis=0, concat_axis=0, tiled=True)
    piece = lax.all_gather(arrived, "tp", axis=0, tiled=True)
    gate = jnp.dot(piece, w_gate[0], preferred_element_type=jnp.float32)
    upper = jnp.dot(piece, w_up[0], preferred_element_type=jnp.float32)
    hidden = (jax.nn.silu(gate) * upper).astype(jnp.bfloat16)
    partial = jnp.dot(hidden, w_down[0], preferred_element_type=jnp.float32).astype(jnp.bfloat16)
    expert_out = lax.psum_scatter(partial, "tp", scatter_dimension=0, tiled=True)
    returned = lax.all_to_all(expert_out, "sp", split_axis=0, concat_axis=0, tiled=True)
    picked = (
        jnp.take(returned, target, axis=0)
        .astype(jnp.float32)
        .reshape(tok_dev, top, returned.shape[1])
    )
    moe_sum = jnp.sum(picked * route_weights[:, :, None], axis=1)
    return (mixed_float_output + moe_sum).astype(jnp.bfloat16)


def solution(mesh):
    placed = (
        P("sp", "tp"),
        P("sp", None),
        P("sp", None),
        P(),
        P(),
        P(None, "tp"),
        P(),
        P(("sp", "tp"), None),
        P(("sp", "tp"), None),
        P(("sp", "tp"), None),
        P("sp", None, "tp"),
        P("sp", None, "tp"),
        P("sp", "tp", None),
    )
    return jax.shard_map(
        local, mesh=mesh, in_specs=placed, out_specs=P(("sp", "tp"), None), check_vma=False
    )
```

```python
import functools

import jax
import jax.numpy as jnp
import numpy as np
from jax import lax
from jax.experimental import pallas as pl
from jax.experimental.pallas import tpu as pltpu
from jax.sharding import PartitionSpec as P

GRID_W = 64


EPS = 1e-06
ROPE_BASE = 10000.0
NEG_START = -1e30


def rotate(field, position):
    half = field.shape[-1] // 2
    quarter = half // 2
    freqs = ROPE_BASE ** (-jnp.arange(quarter, dtype=jnp.float32) / quarter)
    grid_row = (position // GRID_W).astype(jnp.float32)
    grid_col = (position % GRID_W).astype(jnp.float32)

    def turn_half(part, coord):
        angle = coord[:, None] * freqs[None, :]
        cosine = jnp.cos(angle)[:, None, :]
        sine = jnp.sin(angle)[:, None, :]
        first, second = (part[..., :quarter], part[..., quarter:])
        return jnp.concatenate(
            [first * cosine - second * sine, second * cosine + first * sine], axis=-1
        )

    return jnp.concatenate(
        [turn_half(field[..., :half], grid_row), turn_half(field[..., half:], grid_col)], axis=-1
    )


def prepare(field, gain, position):
    count = field.shape[0]
    width = gain.shape[0]
    heads_here = field.shape[1] // width
    values_f = field.reshape(count, heads_here, width).astype(jnp.float32)
    scaled = (
        values_f * lax.rsqrt(jnp.mean(values_f * values_f, axis=-1, keepdims=True) + EPS) * gain
    )
    return rotate(scaled, position).reshape(count, heads_here * width).astype(jnp.bfloat16)


def absorb(carry, query_matrix, key_rows, value_rows, scale):
    count = key_rows.shape[0]
    width = 2048 if count > 2048 and count % 2048 == 0 else count
    key_blocks = key_rows.reshape(count // width, width, key_rows.shape[1], key_rows.shape[2])
    value_blocks = value_rows.reshape(
        count // width, width, value_rows.shape[1], value_rows.shape[2]
    )

    def step(state, block):
        run_max, run_sum, run_acc = state
        key_tile_rows, value_tile_rows = block
        scores = (
            jnp.einsum(
                "hxt,ght->hxg", query_matrix, key_tile_rows, preferred_element_type=jnp.float32
            )
            * scale
        )
        new_max = jnp.maximum(run_max, jnp.max(scores, axis=-1))
        weight_tensors = jnp.exp(scores - new_max[..., None]).astype(jnp.bfloat16)
        factor = jnp.exp(run_max - new_max)
        run_sum = run_sum * factor + jnp.sum(weight_tensors.astype(jnp.float32), axis=-1)
        run_acc = run_acc * factor[..., None] + jnp.einsum(
            "zij,jzu->ziu", weight_tensors, value_tile_rows, preferred_element_type=jnp.float32
        )
        return ((new_max, run_sum, run_acc), None)

    result, unused = lax.scan(step, carry, (key_blocks, value_blocks))
    return result


MESH = pl.DeviceIdType.MESH
VMEM_LIMIT = 60 * 1024 * 1024


def greet(partners, count):
    barrier = pltpu.get_barrier_semaphore()
    for where in partners:
        pl.semaphore_signal(barrier, inc=1, device_id=where, device_id_type=MESH)
    pl.semaphore_wait(barrier, count)


def remote(src, dst, send, recv, where):
    return pltpu.make_async_remote_copy(
        src_ref=src, dst_ref=dst, send_sem=send, recv_sem=recv, device_id=where, device_id_type=MESH
    )


def square():
    mine = lax.axis_index("tp")
    return mine, mine + 1 - 2 * lax.rem(mine, 2), lax.rem(mine + 2, 4), 3 - mine


def in_vmem(count):
    return [pl.BlockSpec(memory_space=pltpu.VMEM)] * count


def params(number):
    return pltpu.CompilerParams(
        collective_id=number, has_side_effects=True, vmem_limit_bytes=VMEM_LIMIT
    )


def turn_tables(width, rows):
    quarter = width // 4
    freqs = ROPE_BASE ** (-np.arange(quarter, dtype=np.float32) / np.float32(quarter))
    zero = np.zeros((max(rows, GRID_W), quarter), np.float32)

    def table(count, blocks):
        angle = np.arange(count, dtype=np.float32)[:, None] * freqs.astype(np.float32)[None, :]
        kinds = {"c": np.cos(angle), "s": np.sin(angle), "m": -np.sin(angle), "0": zero[:count]}
        return np.stack([np.concatenate([kinds[k] for k in b], axis=1) for b in blocks])

    by_col = table(GRID_W, ("00cc", "00m0", "000s"))
    by_row = table(rows, ("cc00", "m000", "0s00"))
    return by_col.astype(np.float32), by_row.astype(np.float32)


def attend_kernel(
    n, q_ref, k_ref, v_ref, qg_ref, kg_ref, col_ref, row_ref, res_ref, gain_ref, name_ref, share_ref, w_ref,
    mixed_ref, normed_ref, notes_ref,
    w, kv, qs, top, acc, held, total, stage, proj, sheet,
    load, zs, zr, xs, xr, ds, dr, ns, nr, fs, fr, give, take, tell, told,
):
    me = lax.axis_index("sp")
    chips = n // 2
    chip, core = me // 2, lax.rem(me, 2)
    other = 1 - core
    partner = {"sp": 2 * chip + other}
    mine, across, along, corner = square()
    x = lax.rem(mine, 2)
    rows, width = q_ref.shape
    size = qg_ref.shape[1]
    heads = width // size
    pairs = heads // 2
    share = rows // 4
    keys_half = rows // 2
    fetch = pltpu.make_async_copy(w_ref, w, load.at[0])
    fetch.start()

    barrier = pltpu.get_barrier_semaphore()
    peers = [lax.rem(me + d, n) for d in range(1, n)]
    for p in peers:
        pl.semaphore_signal(barrier, inc=1, device_id={"sp": p}, device_id_type=MESH)
    for p in (across, along, corner):
        pl.semaphore_signal(barrier, inc=1, device_id={"tp": p}, device_id_type=MESH)

    def turned(part, gain_row, g):
        values = part.astype(jnp.float32)
        mean = jnp.mean(values * values, axis=-1, keepdims=True)
        scaled = values * lax.rsqrt(mean + EPS) * gain_row
        grid_row = pl.ds(me * (rows // GRID_W) + g, 1)
        turn = [col_ref[i] + row_ref[i, grid_row] for i in range(3)]
        return (
            scaled * turn[0]
            + pltpu.roll(scaled, size - size // 4, 1) * turn[1]
            + pltpu.roll(scaled, size // 4, 1) * turn[2]
        ).astype(jnp.bfloat16)

    kv_heads = k_ref.shape[1] // size
    kv_head = mine * kv_heads // 4
    at = pl.ds(pl.multiple_of(kv_head * size, size), size)
    for g in range(rows // GRID_W):
        span = pl.ds(g * GRID_W, GRID_W)
        side, low = (g * GRID_W) // keys_half, (g * GRID_W) % keys_half
        place = pl.ds(low, GRID_W)
        kv[chip, core, side, 0, place] = turned(k_ref[span, at], kg_ref[...], g)
        kv[chip, core, side, 1, place] = v_ref[span, at]
    lanes = lax.broadcasted_iota(jnp.int32, (n, 2 * share), 1)
    expert = lax.broadcasted_iota(jnp.int32, (n, 2 * share), 0)
    def as_row(ref, i):
        column = jnp.broadcast_to(ref[:, i : i + 1].astype(jnp.float32), (share, 2 * share))
        return jnp.transpose(jnp.concatenate([column, column], axis=0))[:n]

    first_one, second_one = [as_row(name_ref, i).astype(jnp.int32) == expert for i in range(2)]
    taken = jnp.where((first_one | second_one) & (lanes < share), 1.0, 0.0)
    before = lax.broadcasted_iota(jnp.int32, (2 * share, 2 * share), 0)
    after = lax.broadcasted_iota(jnp.int32, (2 * share, 2 * share), 1)
    ladder = jnp.where(before < after, 1.0, 0.0).astype(jnp.bfloat16)
    slot = jnp.dot(taken.astype(jnp.bfloat16), ladder, preferred_element_type=jnp.float32)
    weight = jnp.where(first_one, as_row(share_ref, 0), 0.0)
    weight += jnp.where(second_one, as_row(share_ref, 1), 0.0)
    sheet[me] = jnp.where(lanes < share, jnp.where(taken > 0, slot, -1.0), weight)

    pl.semaphore_wait(barrier, n + 2)

    def to_plane(p):
        block = kv.at[chip, core, x]
        return remote(block, block, zs.at[p], zr.at[chip], {"sp": 2 * p + core})

    def from_plane(p):
        block = kv.at[p, core, x]
        remote(block, block, zs.at[p], zr.at[p], partner).wait_recv()

    def sideways(p):
        block = kv.at[p, core, x]
        return remote(block, block, xs.at[p], xr.at[p], {"tp": across})

    def from_side(p):
        block = kv.at[p, core, 1 - x]
        remote(block, block, xs.at[p], xr.at[p], partner).wait_recv()

    def hand(p, side):
        block = kv.at[p, core, side]
        return remote(block, block, ds.at[p, side], dr.at[p, side], partner)

    def handed(p, side):
        block = kv.at[p, other, side]
        remote(block, block, ds.at[p, side], dr.at[p, side], partner).wait_recv()

    for j in range(1, chips):

        @pl.when(chip + j < chips)
        def _():
            to_plane(chip + j).start()

        @pl.when(chip - j >= 0)
        def _():
            to_plane(chip - j).start()

    for side in range(2):
        hand(chip, side).start()
    inform = [
        remote(sheet.at[me], sheet.at[me], ns.at[d], nr.at[d], {"sp": p})
        for d, p in enumerate(peers)
    ]
    for c in inform:
        c.start()

    @pl.loop(0, heads)
    def _(h):
        @pl.loop(0, rows // GRID_W)
        def _(g):
            span = pl.ds(pl.multiple_of(g * GRID_W, GRID_W), GRID_W)
            block = q_ref[span, pl.ds(pl.multiple_of(h * size, size), size)]
            qs[h, span] = turned(block, qg_ref[...], g)

        top[h] = jnp.full(top.shape[1:], NEG_START, jnp.float32)
        acc[h] = jnp.zeros(acc.shape[1:], jnp.float32)

    grade = size ** (-0.5) * 1.4426950408889634

    def first(j, way):
        block = held.at[mine, j]
        where = (across, along)[way]
        return remote(block, block, fs.at[j, way], fr.at[j, way], {"tp": where})

    upper, lower = pl.ds(0, rows // 2), pl.ds(rows // 2, rows // 2)

    def second(j, way):
        block = (held.at[across, j, upper], held.at[along, j, lower])[way]
        where = (along, across)[way]
        return remote(block, block, fs.at[j, 2 + way], fr.at[j, 2 + way], {"tp": where})

    def arrive(j, way):
        block = (
            held.at[across, j],
            held.at[along, j],
            held.at[corner, j, upper],
            held.at[corner, j, lower],
        )[way]
        remote(block, block, fs.at[j, way], fr.at[j, way], partner).wait_recv()

    @pl.loop(0, chips)
    def _(s):
        @pl.when(s + 1 < chips)
        def _():
            p = visit(chip, chips, s + 1)
            from_plane(p)
            sideways(p).start()
            hand(p, x).start()

        p = visit(chip, chips, s)

        @pl.when(s > 0)
        def _():
            from_side(p)
            hand(p, 1 - x).start()

        for side in range(2):
            handed(p, side)

        @pl.loop(0, pairs)
        def _(j):
            for i in range(2):
                h = 2 * j + i
                keys = kv[p, :, :, 0].reshape(2 * rows, size)
                values = kv[p, :, :, 1].reshape(2 * rows, size)
                scores = lax.dot_general(
                    qs[h], keys, (((1,), (1,)), ((), ())), preferred_element_type=jnp.float32
                )
                old = top[h]
                new = jnp.maximum(old, jnp.max(scores, axis=1, keepdims=True))
                top[h] = new
                weights = jnp.exp2((scores - new[:, :1]) * grade).astype(jnp.bfloat16)
                full = jnp.concatenate([values, jnp.ones_like(values)], axis=1)
                grown = jnp.dot(weights, full, preferred_element_type=jnp.float32)
                factor = jnp.exp2((old - new) * grade)
                acc[h] = acc[h] * jnp.concatenate([factor, factor], axis=1) + grown

            @pl.when(s == chips - 1)
            def _():
                for i in range(2):
                    done = acc[2 * j + i]
                    ratio = done[:, :size] / done[:, size:]
                    held[mine, j, :, i * size : (i + 1) * size] = ratio.astype(held.dtype)
                first(j, 0).start()
                first(j, 1).start()

        @pl.when(s == chips - 2)
        def _():
            for c in inform:
                c.wait_recv()
            notes_ref[mine] = sheet[...]
            for i, p in enumerate((corner, across, along)):
                remote(sheet, notes_ref.at[mine], tell.at[i], told.at[i], {"tp": p}).start()

    fetch.wait()

    def term(owner, j):
        start = pl.multiple_of(owner * width + j * 2 * size, 2 * size)
        part = w[pl.ds(start, 2 * size), :]
        total[...] += jnp.dot(held[owner, j], part, preferred_element_type=jnp.float32)

    total[...] = jnp.zeros_like(total)

    @pl.loop(0, pairs)
    def _(j):
        term(mine, j)

    @pl.loop(0, pairs)
    def _(j):
        arrive(j, 0)
        second(j, 0).start()
        arrive(j, 1)
        second(j, 1).start()
        term(across, j)
        term(along, j)

    @pl.loop(0, pairs)
    def _(j):
        arrive(j, 2)
        arrive(j, 3)
        term(corner, j)

    stage[...] = total[...].astype(stage.dtype)
    columns = pl.ds(pl.multiple_of(mine * width, width), width)

    def piece(owner):
        return pl.ds(pl.multiple_of(owner * share, share), share)

    back = [
        remote(stage.at[piece(p)], proj.at[:, columns], give.at[i], take.at[i], {"tp": p})
        for i, p in enumerate((corner, across, along))
    ]
    for c in back:
        c.start()
    proj[:, columns] = stage[piece(mine), :]
    for c in back:
        c.wait()
    mixed = (res_ref[...].astype(jnp.float32) + proj[...].astype(jnp.float32)).astype(mixed_ref.dtype)
    mixed_ref[...] = mixed
    mixed = mixed.astype(jnp.float32)
    mean = jnp.mean(mixed * mixed, axis=-1, keepdims=True)
    normed_ref[...] = (mixed * lax.rsqrt(mean + EPS) * gain_ref[...]).astype(normed_ref.dtype)

    for i, p in enumerate((corner, across, along)):
        remote(sheet, notes_ref.at[mine], tell.at[i], told.at[i], {"tp": p}).wait()
    for c in inform:
        c.wait_send()
    for d in range(1, chips):
        p = lax.rem(chip + d, chips)
        to_plane(p).wait_send()
        sideways(p).wait_send()
    for p in range(chips):
        for side in range(2):
            hand(p, side).wait_send()
    for j in range(pairs):
        for way in range(2):
            first(j, way).wait_send()
            second(j, way).wait_send()


def attend(n, queries, keys, values, query_gain, key_gain, residual, gain, names, shares, out_proj):
    rows, width = queries.shape
    size = query_gain.shape[0]
    heads = width // size
    share, depth = residual.shape
    chips = n // 2
    kind = queries.dtype
    by_col, by_row = turn_tables(size, n * rows // GRID_W)
    dma = pltpu.SemaphoreType.DMA
    exact = jnp.float32
    return pl.pallas_call(
        functools.partial(attend_kernel, n),
        out_shape=(
            jax.ShapeDtypeStruct((share, depth), kind),
            jax.ShapeDtypeStruct((share, depth), kind),
            jax.ShapeDtypeStruct((4, n, n, 2 * share), exact),
        ),
        in_specs=in_vmem(11) + [pl.BlockSpec(memory_space=pl.ANY)],
        out_specs=tuple(in_vmem(3)),
        scratch_shapes=[
            pltpu.VMEM(out_proj.shape, kind),
            pltpu.VMEM((chips, 2, 2, 2, rows // 2, size), kind),
            pltpu.VMEM((heads, rows, size), kind),
            pltpu.VMEM((heads, rows, size), exact),
            pltpu.VMEM((heads, rows, 2 * size), exact),
            pltpu.VMEM((4, heads // 2, rows, 2 * size), kind),
            pltpu.VMEM((rows, width), exact),
            pltpu.VMEM((rows, width), kind),
            pltpu.VMEM((share, depth), kind),
            pltpu.VMEM((n, n, 2 * share), exact),
            dma((1,)),
            dma((chips,)),
            dma((chips,)),
            dma((chips,)),
            dma((chips,)),
            dma((chips, 2)),
            dma((chips, 2)),
            dma((n - 1,)),
            dma((n - 1,)),
            dma((heads // 2, 4)),
            dma((heads // 2, 4)),
            dma((3,)),
            dma((3,)),
            dma((3,)),
            dma((3,)),
        ],
        compiler_params=params(1),
        name="attend",
    )(
        queries,
        keys,
        values,
        query_gain[None, :],
        key_gain[None, :],
        jnp.asarray(by_col),
        jnp.asarray(by_row),
        residual,
        gain[None, :],
        names,
        shares,
        out_proj,
    )


def visit(chip, chips, step):
    near = jnp.minimum(chip, chips - 1 - chip)
    up = chip < chips - 1 - chip
    swing = (step + 1) // 2 * (2 * lax.rem(step, 2) - 1)
    swing = jnp.where(up, chip + swing, chip - swing)
    tail = jnp.where(up, chip + (step - near), chip - (step - near))
    return jnp.where(step <= 2 * near, swing, tail)


def wide(value):
    return value.astype(jnp.float32)


def moe_kernel(
    n, cuts, x_ref, note_ref, wg_ref, wu_ref, wd_ref, out_ref,
    tok, wg, wu, wd, picked, hid, wsel, held, own, give, take,
    low, high, from_x, from_y, to_y, to_x, last_y, last_x, acc, zsend, zrecv, zmid,
    load, zs, zr, sq_s, sq_r, pd_s, pd_r, tk_s, tk_r, hop_s, hop_r, hz_s, hz_r, mid_r,
):
    me = lax.axis_index("sp")
    chips = n // 2
    chip, core = me // 2, lax.rem(me, 2)
    other = 1 - core
    partner = {"sp": 2 * chip + other}
    mine, across, along, corner = square()
    x, y = lax.rem(mine, 2), mine // 2
    share, depth = x_ref.shape
    units = wg.shape[1]
    group = 4 * share
    slots = wsel.shape[3] // 2
    width = depth // cuts
    half = width // 2
    steps = chips * cuts

    def column(k):
        return pl.ds(pl.multiple_of(k * width, width), width)

    loads = [
        pltpu.make_async_copy(wg_ref.at[0], wg, load.at[0]),
        pltpu.make_async_copy(wu_ref.at[0], wu, load.at[1]),
    ] + [
        pltpu.make_async_copy(wd_ref.at[0, :, pl.ds(q * width, width)], wd.at[q], load.at[2 + q])
        for q in range(cuts)
    ]
    for c in loads:
        c.start()

    barrier = pltpu.get_barrier_semaphore()

    def greet_one(where):
        pl.semaphore_signal(barrier, inc=1, device_id=where, device_id_type=MESH)

    greet_one(partner)
    greet_one({"tp": across})
    greet_one({"tp": along})
    for d in range(1, chips):
        greet_one({"sp": 2 * lax.rem(chip + d, chips) + core})
    pl.semaphore_wait(barrier, chips + 2)

    has_right, has_left = chip < chips - 1, chip > 0

    def cols(h):
        return pl.ds(pl.multiple_of(h * (depth // 2), depth // 2), depth // 2)

    def own_half(h):
        return x_ref.at[:, cols(h)]

    def along_z(p, h, way, first=False):
        block = tok.at[p, core, h, mine]
        to = 2 * (chip + 1 - 2 * way) + core
        return remote(
            own_half(h) if first else block, block, zs.at[p, h, way], zr.at[p, h], {"sp": to}
        )

    upper, lower = pl.ds(0, share // 2), pl.ds(share // 2, share // 2)

    def pass_on(p, h, way, first=False):
        block = tok.at[p, core, h]
        start = own_half(h) if first else block.at[mine]
        src, dst, where = (
            (start, block.at[mine], across),
            (start, block.at[mine], along),
            (block.at[across, upper], block.at[across, upper], along),
            (block.at[along, lower], block.at[along, lower], across),
        )[way]
        return remote(src, dst, sq_s.at[way], sq_r.at[p, h, way], {"tp": where})

    def arrive(p, h, way):
        block = tok.at[p, core, h]
        dst = (
            block.at[across],
            block.at[along],
            block.at[corner, upper],
            block.at[corner, lower],
        )[way]
        remote(dst, dst, sq_s.at[way], sq_r.at[p, h, way], {"tp": across}).wait_recv()

    def hand(p, h, t, first=False):
        block = tok.at[p, core, h, t]
        src = own_half(h) if first else block
        return remote(src, block, pd_s.at[0], pd_r.at[p, h, t], partner)

    def handed(p, h, t):
        block = tok.at[p, other, h, t]
        remote(block, block, pd_s.at[0], pd_r.at[p, h, t], partner).wait_recv()

    for h in range(2):
        pass_on(chip, h, 0, True).start()
        pass_on(chip, h, 1, True).start()

        @pl.when(has_right)
        def _():
            along_z(chip, h, 0, True).start()

        @pl.when(has_left)
        def _():
            along_z(chip, h, 1, True).start()

        hand(chip, h, mine, True).start()
        tok[chip, core, h, mine] = x_ref[:, cols(h)]

    def part(u):
        return visit(chip, chips, u // 2), lax.rem(u, 2)

    def finish(u):
        p, h = part(u)
        arrive(p, h, 2)
        arrive(p, h, 3)
        hand(p, h, corner).start()

    def wait_rows(p):
        for h in range(2):
            for t in range(4):
                handed(p, h, t)

    def pick_rows(p, side):
        tiles = [note_ref[t, 2 * p + side] for t in range(4)]
        lane = lax.broadcasted_iota(jnp.int32, (n, 2 * share), 1)
        chosen = lax.broadcasted_iota(jnp.int32, (n, 2 * share), 0) == me

        def across_two(even, odd, swap_even):
            moved = pltpu.roll(even if swap_even else odd, share, 1)
            return jnp.where(lane < share, moved, odd) if swap_even else jnp.where(
                lane < share, even, moved
            )

        def row_of(swap_even):
            parts_two = [across_two(tiles[t], tiles[t + 1], swap_even) for t in (0, 2)]
            picks = [
                jnp.sum(jnp.where(chosen, v, 0.0), axis=0, keepdims=True) for v in parts_two
            ]
            return jnp.concatenate(picks, axis=1)

        spot = row_of(False)
        base = lax.broadcasted_iota(jnp.int32, (1, group), 1) // share * (slots // 4)
        spot = jnp.where(spot >= 0, spot.astype(jnp.int32) + base, -1)
        weight = row_of(True)
        coarse = weight.astype(jnp.bfloat16).astype(jnp.float32)
        parts = (coarse, weight - coarse)
        hit = lax.broadcasted_iota(jnp.int32, (slots, group), 0) == spot
        pick = jnp.where(hit, 1.0, 0.0).astype(tok.dtype)
        for i in range(2):
            turned = jnp.transpose(jnp.where(hit, parts[i], 0.0))
            wsel[p, side, :, i * slots : (i + 1) * slots] = turned.astype(wsel.dtype)
        for h in range(2):
            block = tok[p, side, h].reshape(group, depth // 2)
            rows = jnp.dot(pick, block, preferred_element_type=jnp.float32)
            picked[side * slots : (side + 1) * slots, cols(h)] = rows.astype(picked.dtype)

    def activate(p, u):
        some = pl.ds(pl.multiple_of(u * 512, 512), 512)
        gate = jnp.dot(picked[...], wg[:, some], preferred_element_type=jnp.float32)
        rise = jnp.dot(picked[...], wu[:, some], preferred_element_type=jnp.float32)
        hid[p, :, some] = (jax.nn.silu(gate) * rise).astype(hid.dtype)

    def expert(p):
        wait_rows(p)
        pick_rows(p, 0)
        pick_rows(p, 1)

        @pl.loop(0, units // 512)
        def _(u):
            activate(p, u)

    def forward(u):
        p, h = part(u)
        arrive(p, h, 0)
        pass_on(p, h, 2).start()
        hand(p, h, across).start()
        arrive(p, h, 1)
        pass_on(p, h, 3).start()
        hand(p, h, along).start()

    last = 2 * chips - 1

    def passes(p):
        return ((p < chip) & has_right) | ((p > chip) & has_left)

    def relay(u):
        p, h = part(u)

        @pl.when(passes(p))
        def _():
            along_z(p, h, 0).wait_recv()

        @pl.when((p < chip) & has_right)
        def _():
            along_z(p, h, 0).start()

        @pl.when((p > chip) & has_left)
        def _():
            along_z(p, h, 1).start()

    def open_up(u):
        p, h = part(u)

        @pl.when(jnp.logical_not(passes(p)))
        def _():
            along_z(p, h, 0).wait_recv()

        pass_on(p, h, 0).start()
        pass_on(p, h, 1).start()
        hand(p, h, mine).start()

    relay(2)
    open_up(2)

    @pl.loop(0, last)
    def _(u):
        forward(u)

        @pl.when(u + 4 <= last)
        def _():
            relay(u + 4)

        @pl.when(u == 0)
        def _():
            relay(3)

        @pl.when(u + 3 <= last)
        def _():
            open_up(u + 3)

        @pl.when(u == 0)
        def _():
            for c in loads:
                c.wait()

        @pl.when((u == 4) | ((u > 4) & (lax.rem(u, 2) == 1)))
        def _():
            expert(visit(chip, chips, (u - 3) // 2))

        @pl.when((u >= 2) & (lax.rem(u, 2) == 0))
        def _():
            finish(u - 2)

            @pl.when(u < last - 1)
            def _():
                finish(u - 1)

    def plane_of(k):
        return visit(chip, chips, lax.rem(k // cuts + 1, chips))

    def swap(k):
        return remote(give.at[k], take.at[k], tk_s.at[0], tk_r.at[k], partner)

    def hop(k, way):
        src, dst, where = (
            (low.at[k, 1 - x], from_x.at[k], across),
            (high.at[k, 1 - y], from_y.at[k], along),
            (to_y.at[k], last_y.at[k], along),
            (to_x.at[k], last_x.at[k], across),
        )[way]
        return remote(src, dst, hop_s.at[way], hop_r.at[k, way], {"tp": where})

    def home(k):
        p, q = plane_of(k), lax.rem(k, cuts)
        return remote(
            zsend.at[k], zrecv.at[chip, q], hz_s.at[0], hz_r.at[chip, q], {"sp": 2 * p + core}
        )

    is_end = (chip == 0) | (chip == chips - 1)

    def lend(k):
        to = chip + jnp.where(chip == 0, 1, -1)
        return remote(
            zsend.at[k], zmid.at[lax.rem(k, cuts)], hz_s.at[0], mid_r.at[lax.rem(k, cuts)],
            {"sp": 2 * to + core},
        )

    def homed(p, q):
        return remote(zsend.at[0], zrecv.at[p, q], hz_s.at[0], hz_r.at[p, q], partner)

    def settle(k):
        swap(k).wait_recv()
        total = own[lax.rem(k, 3)] + wide(take[k])
        cast = total.astype(low.dtype).reshape(4, share, width)
        for t in range(4):
            low[k, t % 2, t // 2] = cast[t, :, :half]
            high[k, t // 2, t % 2] = cast[t, :, half:]
        hop(k, 0).start()
        hop(k, 1).start()

    @pl.loop(0, steps + 6)
    def _(step):
        @pl.when((step >= 2) & (step < steps + 2))
        def _():
            settle(step - 2)

        @pl.when((step >= 4) & (step < steps + 4))
        def _(k=step - 4):
            hop(k, 0).wait_recv()
            to_y[k] = (wide(low[k, x, 1 - y]) + wide(from_x[k, 1 - y])).astype(to_y.dtype)
            hop(k, 2).start()
            hop(k, 1).wait_recv()
            to_x[k] = (wide(high[k, y, 1 - x]) + wide(from_y[k, 1 - x])).astype(to_x.dtype)
            hop(k, 3).start()

        @pl.when(step >= 6)
        def _(k=step - 6):
            hop(k, 2).wait_recv()
            left = wide(low[k, x, y]) + wide(from_x[k, y]) + wide(last_y[k])
            hop(k, 3).wait_recv()
            right = wide(high[k, y, x]) + wide(from_y[k, x]) + wide(last_x[k])

            far = (k >= steps - 2 * cuts) & (k < steps - cuts)

            @pl.when((k < steps - cuts) & jnp.logical_not(far & jnp.logical_not(is_end)))
            def _():
                zsend[k, :, :half] = left.astype(zsend.dtype)
                zsend[k, :, half:] = right.astype(zsend.dtype)

                @pl.when(far)
                def _():
                    lend(k).start()

                @pl.when(jnp.logical_not(far))
                def _():
                    home(k).start()

            @pl.when(far & jnp.logical_not(is_end))
            def _():
                lend(k).wait_recv()
                more = wide(zmid[lax.rem(k, cuts)])
                zsend[k, :, :half] = (left + more[:, :half]).astype(zsend.dtype)
                zsend[k, :, half:] = (right + more[:, half:]).astype(zsend.dtype)
                home(k).start()

            @pl.when(k >= steps - cuts)
            def _():
                acc[lax.rem(k, cuts), :, :half] = left
                acc[lax.rem(k, cuts), :, half:] = right

        @pl.when(step < steps)
        def _(k=step):
            third, fourth = visit(chip, chips, chips - 2), visit(chip, chips, chips - 1)

            @pl.when(k == cuts)
            def _():
                @pl.loop(0, units // 512)
                def _(u):
                    activate(third, u)

            p, q = plane_of(k), lax.rem(k, cuts)
            out = jnp.dot(hid[p], wd[q], preferred_element_type=jnp.float32).astype(held.dtype)
            for side in range(2):
                block = out[side * slots : (side + 1) * slots]
                held[side, :slots] = block
                held[side, slots:] = block

            def spread(side):
                return jnp.dot(wsel[p, side], held[side], preferred_element_type=jnp.float32)

            give[k] = spread(other).astype(give.dtype)
            swap(k).start()
            own[lax.rem(k, 3)] = spread(core)

            @pl.when(k == cuts // 2)
            def _():
                forward(last)
                finish(last - 2)

            @pl.when(k == cuts)
            def _():
                finish(last - 1)
                finish(last)

            @pl.when((k == cuts - 1) | (k == cuts + 1))
            def _():
                p = jnp.where(k < cuts, third, fourth)
                wait_rows(p)
                pick_rows(p, 0)
                pick_rows(p, 1)

            each = units // 1024

            @pl.when((k >= cuts + 2) & (k < cuts + 4))
            def _():
                @pl.loop(0, each)
                def _(u):
                    activate(fourth, (k - cuts - 2) * each + u)

    @pl.loop(0, cuts)
    def _(q):
        for d in range(1, chips):
            p = lax.rem(chip + d, chips)

            @pl.when(jnp.logical_not(is_end & (p == chips - 1 - chip)))
            def _():
                homed(p, q).wait_recv()
                acc[q] += wide(zrecv[p, q])

        out_ref[:, column(q)] = acc[q]

    @pl.loop(0, 2 * chips)
    def _(u):
        p, h = u // 2, lax.rem(u, 2)
        @pl.when((p <= chip) & has_right)
        def _():
            along_z(p, h, 0).wait_send()

        @pl.when((p >= chip) & has_left)
        def _():
            along_z(p, h, 1).wait_send()

    def all_left(ref, sem):
        remote(ref, ref, sem, sem, partner).wait_send()

    whole = tok.at[:, 0, :, 0]
    for way, ref in enumerate((whole, whole, whole.at[:, :, upper], whole.at[:, :, lower])):
        all_left(ref, sq_s.at[way])
    all_left(tok.at[:, 0], pd_s.at[0])
    all_left(give, tk_s.at[0])
    for way, ref in enumerate((from_x, from_y, to_y, to_x)):
        all_left(ref, hop_s.at[way])
    all_left(zsend, hz_s.at[0])


def moe(n, normed, notes, capacity, w_gate, w_up, w_down, cuts=4):
    share, depth = normed.shape
    units = w_gate.shape[2]
    chips = n // 2
    kind = normed.dtype
    width = depth // cuts
    half = width // 2
    steps = chips * cuts
    group, slots = 4 * share, 4 * capacity
    dma = pltpu.SemaphoreType.DMA

    def room(*extent):
        return pltpu.VMEM(extent, kind)

    def exact(*extent):
        return pltpu.VMEM(extent, jnp.float32)

    return pl.pallas_call(
        functools.partial(moe_kernel, n, cuts),
        out_shape=jax.ShapeDtypeStruct((share, depth), jnp.float32),
        in_specs=in_vmem(2) + [pl.BlockSpec(memory_space=pl.ANY)] * 3,
        out_specs=in_vmem(1)[0],
        scratch_shapes=[
            room(chips, 2, 2, 4, share, depth // 2),
            room(depth, units),
            room(depth, units),
            room(cuts, units, width),
            room(2 * slots, depth),
            room(chips, 2 * slots, units),
            room(chips, 2, group, 2 * slots),
            room(2, 2 * slots, width),
            exact(3, group, width),
            room(steps, group, width),
            room(steps, group, width),
            room(steps, 2, 2, share, half),
            room(steps, 2, 2, share, half),
            room(steps, 2, share, half),
            room(steps, 2, share, half),
            room(steps, share, half),
            room(steps, share, half),
            room(steps, share, half),
            room(steps, share, half),
            exact(cuts, share, width),
            room(steps - cuts, share, width),
            room(chips, cuts, share, width),
            room(cuts, share, width),
            dma((2 + cuts,)),
            dma((chips, 2, 2)),
            dma((chips, 2)),
            dma((4,)),
            dma((chips, 2, 4)),
            dma((1,)),
            dma((chips, 2, 4)),
            dma((1,)),
            dma((steps,)),
            dma((4,)),
            dma((steps, 4)),
            dma((1,)),
            dma((chips, cuts)),
            dma((cuts,)),
        ],
        compiler_params=params(2),
        name="moe",
    )(normed, notes, w_gate, w_up, w_down)


def start_state(batch, rows, width):
    return (
        jnp.full((batch, rows), NEG_START, jnp.float32),
        jnp.zeros((batch, rows), jnp.float32),
        jnp.zeros((batch, rows, width), jnp.float32),
    )


def local(
    queries,
    keys,
    values,
    query_gain,
    key_gain,
    out_proj,
    expert_norm_scale,
    residual,
    routes,
    route_weights,
    w_gate,
    w_up,
    w_down,
):
    head_size = query_gain.shape[0]
    tok_sp = queries.shape[0]
    tp_count = lax.axis_size("tp")
    sp_count = lax.axis_size("sp")
    heads_dev = queries.shape[1] // head_size
    all_heads = heads_dev * tp_count
    kv_heads = keys.shape[1] // head_size
    group = all_heads // kv_heads
    scale = head_size ** (-0.5)
    tp_index = lax.axis_index("tp")
    sp_index = lax.axis_index("sp")
    tok_dev = residual.shape[0]
    top = routes.shape[1]
    capacity = max(2, 2 * tok_dev * top // sp_count)
    direct = (
        tp_count == 4
        and sp_count // 2 == 4
        and sp_count % 2 == 0
        and capacity % 16 == 0
        and 2 * tok_dev % 128 == 0
        and tok_sp % (2 * GRID_W) == 0
        and heads_dev % 2 == 0
        and 2 * heads_dev <= group
        and tok_sp == tp_count * tok_dev
    )
    if direct:
        mixed, normed, notes = attend(
            sp_count,
            queries,
            keys,
            values,
            query_gain,
            key_gain,
            residual,
            expert_norm_scale,
            routes,
            route_weights,
            out_proj,
        )
        summed = moe(sp_count, normed, notes, capacity, w_gate, w_up, w_down)
        return (mixed.astype(jnp.float32) + summed).astype(jnp.bfloat16)
    position = sp_index * tok_sp + jnp.arange(tok_sp, dtype=jnp.int32)
    q_rot = prepare(queries, query_gain, position)
    shared_value_head = tp_index * heads_dev // group
    own_keys = prepare(
        lax.dynamic_slice_in_dim(keys, shared_value_head * head_size, head_size, 1),
        key_gain,
        position,
    )
    own_values = lax.dynamic_slice_in_dim(values, shared_value_head * head_size, head_size, 1)
    query_matrix = (
        q_rot.reshape(tok_sp, heads_dev, head_size)
        .transpose(1, 0, 2)
        .reshape(1, heads_dev * tok_sp, head_size)
    )
    key_piece = lax.all_gather(own_keys, "sp", axis=0, tiled=True)
    value_piece = lax.all_gather(own_values, "sp", axis=0, tiled=True)
    run_max, run_sum, run_acc = absorb(
        start_state(1, heads_dev * tok_sp, head_size),
        query_matrix,
        key_piece[:, None, :],
        value_piece[:, None, :],
        scale,
    )
    attn = (run_acc / run_sum[..., None]).astype(jnp.bfloat16)
    attn = (
        attn.reshape(heads_dev, tok_sp, head_size)
        .transpose(1, 0, 2)
        .reshape(tok_sp, heads_dev * head_size)
    )
    columns = jnp.dot(
        lax.all_gather(attn, "tp", axis=1, tiled=True),
        out_proj,
        preferred_element_type=jnp.float32,
    )
    projected = lax.all_to_all(
        columns.astype(jnp.bfloat16), "tp", split_axis=0, concat_axis=1, tiled=True
    )
    mixed_float_output = residual.astype(jnp.float32) + projected.astype(jnp.float32)
    mixed = mixed_float_output.astype(jnp.bfloat16)
    mixed_float_output = mixed.astype(jnp.float32)
    normed = (
        mixed_float_output
        * lax.rsqrt(jnp.mean(mixed_float_output * mixed_float_output, axis=-1, keepdims=True) + EPS)
        * expert_norm_scale
    ).astype(jnp.bfloat16)
    flat_routes = routes.reshape(-1)
    one_hot = (flat_routes[:, None] == jnp.arange(sp_count, dtype=jnp.int32)[None, :]).astype(
        jnp.int32
    )
    earlier = jnp.cumsum(one_hot, axis=0) - one_hot
    slot_index = jnp.sum(earlier * one_hot, axis=1)
    target = flat_routes * capacity + slot_index
    selector = (
        jnp.arange(sp_count * capacity, dtype=jnp.int32)[:, None] == target[None, :]
    ).astype(jnp.bfloat16)
    selector = jnp.sum(selector.reshape(sp_count * capacity, tok_dev, top), axis=2)
    send_rows = jnp.dot(selector, normed, preferred_element_type=jnp.float32).astype(jnp.bfloat16)
    arrived = lax.all_to_all(send_rows, "sp", split_axis=0, concat_axis=0, tiled=True)
    piece = lax.all_gather(arrived, "tp", axis=0, tiled=True)
    gate = jnp.dot(piece, w_gate[0], preferred_element_type=jnp.float32)
    upper = jnp.dot(piece, w_up[0], preferred_element_type=jnp.float32)
    hidden = (jax.nn.silu(gate) * upper).astype(jnp.bfloat16)
    partial = jnp.dot(hidden, w_down[0], preferred_element_type=jnp.float32).astype(jnp.bfloat16)
    expert_out = lax.psum_scatter(partial, "tp", scatter_dimension=0, tiled=True)
    returned = lax.all_to_all(expert_out, "sp", split_axis=0, concat_axis=0, tiled=True)
    picked = (
        jnp.take(returned, target, axis=0)
        .astype(jnp.float32)
        .reshape(tok_dev, top, returned.shape[1])
    )
    moe_sum = jnp.sum(picked * route_weights[:, :, None], axis=1)
    return (mixed_float_output + moe_sum).astype(jnp.bfloat16)


def solution(mesh):
    placed = (
        P("sp", "tp"),
        P("sp", None),
        P("sp", None),
        P(),
        P(),
        P(None, "tp"),
        P(),
        P(("sp", "tp"), None),
        P(("sp", "tp"), None),
        P(("sp", "tp"), None),
        P("sp", None, "tp"),
        P("sp", None, "tp"),
        P("sp", "tp", None),
    )
    return jax.shard_map(
        local, mesh=mesh, in_specs=placed, out_specs=P(("sp", "tp"), None), check_vma=False
    )
```

```python
import functools

import jax
import jax.numpy as jnp
import numpy as np
from jax import lax
from jax.experimental import pallas as pl
from jax.experimental.pallas import tpu as pltpu
from jax.sharding import PartitionSpec as P

GRID_W = 64


EPS = 1e-06
ROPE_BASE = 10000.0
NEG_START = -1e30


def rotate(field, position):
    half = field.shape[-1] // 2
    quarter = half // 2
    freqs = ROPE_BASE ** (-jnp.arange(quarter, dtype=jnp.float32) / quarter)
    grid_row = (position // GRID_W).astype(jnp.float32)
    grid_col = (position % GRID_W).astype(jnp.float32)

    def turn_half(part, coord):
        angle = coord[:, None] * freqs[None, :]
        cosine = jnp.cos(angle)[:, None, :]
        sine = jnp.sin(angle)[:, None, :]
        first, second = (part[..., :quarter], part[..., quarter:])
        return jnp.concatenate(
            [first * cosine - second * sine, second * cosine + first * sine], axis=-1
        )

    return jnp.concatenate(
        [turn_half(field[..., :half], grid_row), turn_half(field[..., half:], grid_col)], axis=-1
    )


def prepare(field, gain, position):
    count = field.shape[0]
    width = gain.shape[0]
    heads_here = field.shape[1] // width
    values_f = field.reshape(count, heads_here, width).astype(jnp.float32)
    scaled = (
        values_f * lax.rsqrt(jnp.mean(values_f * values_f, axis=-1, keepdims=True) + EPS) * gain
    )
    return rotate(scaled, position).reshape(count, heads_here * width).astype(jnp.bfloat16)


def absorb(carry, query_matrix, key_rows, value_rows, scale):
    count = key_rows.shape[0]
    width = 2048 if count > 2048 and count % 2048 == 0 else count
    key_blocks = key_rows.reshape(count // width, width, key_rows.shape[1], key_rows.shape[2])
    value_blocks = value_rows.reshape(
        count // width, width, value_rows.shape[1], value_rows.shape[2]
    )

    def step(state, block):
        run_max, run_sum, run_acc = state
        key_tile_rows, value_tile_rows = block
        scores = (
            jnp.einsum(
                "hxt,ght->hxg", query_matrix, key_tile_rows, preferred_element_type=jnp.float32
            )
            * scale
        )
        new_max = jnp.maximum(run_max, jnp.max(scores, axis=-1))
        weight_tensors = jnp.exp(scores - new_max[..., None]).astype(jnp.bfloat16)
        factor = jnp.exp(run_max - new_max)
        run_sum = run_sum * factor + jnp.sum(weight_tensors.astype(jnp.float32), axis=-1)
        run_acc = run_acc * factor[..., None] + jnp.einsum(
            "zij,jzu->ziu", weight_tensors, value_tile_rows, preferred_element_type=jnp.float32
        )
        return ((new_max, run_sum, run_acc), None)

    result, unused = lax.scan(step, carry, (key_blocks, value_blocks))
    return result


MESH = pl.DeviceIdType.MESH
VMEM_LIMIT = 60 * 1024 * 1024


def greet(partners, count):
    barrier = pltpu.get_barrier_semaphore()
    for where in partners:
        pl.semaphore_signal(barrier, inc=1, device_id=where, device_id_type=MESH)
    pl.semaphore_wait(barrier, count)


def remote(src, dst, send, recv, where):
    return pltpu.make_async_remote_copy(
        src_ref=src, dst_ref=dst, send_sem=send, recv_sem=recv, device_id=where, device_id_type=MESH
    )


def square():
    mine = lax.axis_index("tp")
    return mine, mine + 1 - 2 * lax.rem(mine, 2), lax.rem(mine + 2, 4), 3 - mine


def in_vmem(count):
    return [pl.BlockSpec(memory_space=pltpu.VMEM)] * count


def params(number):
    return pltpu.CompilerParams(
        collective_id=number, has_side_effects=True, vmem_limit_bytes=VMEM_LIMIT
    )


def turn_tables(width, rows):
    quarter = width // 4
    freqs = ROPE_BASE ** (-np.arange(quarter, dtype=np.float32) / np.float32(quarter))
    zero = np.zeros((max(rows, GRID_W), quarter), np.float32)

    def table(count, blocks):
        angle = np.arange(count, dtype=np.float32)[:, None] * freqs.astype(np.float32)[None, :]
        kinds = {"c": np.cos(angle), "s": np.sin(angle), "m": -np.sin(angle), "0": zero[:count]}
        return np.stack([np.concatenate([kinds[k] for k in b], axis=1) for b in blocks])

    by_col = table(GRID_W, ("00cc", "00m0", "000s"))
    by_row = table(rows, ("cc00", "m000", "0s00"))
    return by_col.astype(np.float32), by_row.astype(np.float32)


def attend_part(
    n, q_ref, k_ref, v_ref, qg_ref, kg_ref, col_ref, row_ref, res_ref, gain_ref, name_ref, share_ref, w_ref,
    mixed_ref, normed_ref, notes_ref, loads,
    w, kv, qs, top, acc, held, total, stage, proj, sheet,
    load, zs, zr, xs, xr, ds, dr, ns, nr, fs, fr, give, take, tell, told, names, shares,
):
    me = lax.axis_index("sp")
    chips = n // 2
    chip, core = me // 2, lax.rem(me, 2)
    other = 1 - core
    partner = {"sp": 2 * chip + other}
    mine, across, along, corner = square()
    x = lax.rem(mine, 2)
    rows, width = q_ref.shape
    size = qg_ref.shape[1]
    heads = width // size
    pairs = heads // 2
    share = rows // 4
    keys_half = rows // 2
    fetch = pltpu.make_async_copy(w_ref, w, load.at[0])
    fetch.start()
    for c in loads:
        c.start()

    barrier = pltpu.get_barrier_semaphore()
    peers = [lax.rem(me + d, n) for d in range(1, n)]
    for p in peers:
        pl.semaphore_signal(barrier, inc=1, device_id={"sp": p}, device_id_type=MESH)
    for p in (across, along, corner):
        pl.semaphore_signal(barrier, inc=1, device_id={"tp": p}, device_id_type=MESH)

    def turned(part, gain_row, g):
        values = part.astype(jnp.float32)
        mean = jnp.mean(values * values, axis=-1, keepdims=True)
        scaled = values * lax.rsqrt(mean + EPS) * gain_row
        grid_row = pl.ds(me * (rows // GRID_W) + g, 1)
        turn = [col_ref[i] + row_ref[i, grid_row] for i in range(3)]
        return (
            scaled * turn[0]
            + pltpu.roll(scaled, size - size // 4, 1) * turn[1]
            + pltpu.roll(scaled, size // 4, 1) * turn[2]
        ).astype(jnp.bfloat16)

    kv_heads = k_ref.shape[1] // size
    kv_head = mine * kv_heads // 4
    at = pl.ds(pl.multiple_of(kv_head * size, size), size)
    for g in range(rows // GRID_W):
        span = pl.ds(g * GRID_W, GRID_W)
        side, low = (g * GRID_W) // keys_half, (g * GRID_W) % keys_half
        place = pl.ds(low, GRID_W)
        kv[chip, core, side, 0, place] = turned(k_ref[span, at], kg_ref[...], g)
        kv[chip, core, side, 1, place] = v_ref[span, at]
    lanes = lax.broadcasted_iota(jnp.int32, (n, 2 * share), 1)
    expert = lax.broadcasted_iota(jnp.int32, (n, 2 * share), 0)
    def as_rows(ref, into):
        into[:, :share] = jnp.broadcast_to(ref[0:1].astype(jnp.float32), (n, share))
        into[:, share:] = jnp.broadcast_to(ref[1:2].astype(jnp.float32), (n, share))
        both = into[...]
        swapped = pltpu.roll(both, share, 1)
        return jnp.where(lanes < share, both, swapped), jnp.where(lanes < share, swapped, both)

    first_one, second_one = [r.astype(jnp.int32) == expert for r in as_rows(name_ref, names)]
    first_part, second_part = as_rows(share_ref, shares)
    taken = jnp.where((first_one | second_one) & (lanes < share), 1.0, 0.0)
    before = lax.broadcasted_iota(jnp.int32, (2 * share, 2 * share), 0)
    after = lax.broadcasted_iota(jnp.int32, (2 * share, 2 * share), 1)
    ladder = jnp.where(before < after, 1.0, 0.0).astype(jnp.bfloat16)
    slot = jnp.dot(taken.astype(jnp.bfloat16), ladder, preferred_element_type=jnp.float32)
    weight = jnp.where(first_one, first_part, 0.0) + jnp.where(second_one, second_part, 0.0)
    sheet[me] = jnp.where(lanes < share, jnp.where(taken > 0, slot, -1.0), weight)

    pl.semaphore_wait(barrier, n + 2)

    def to_plane(p):
        block = kv.at[chip, core, x]
        return remote(block, block, zs.at[p], zr.at[chip], {"sp": 2 * p + core})

    def from_plane(p):
        block = kv.at[p, core, x]
        remote(block, block, zs.at[p], zr.at[p], partner).wait_recv()

    def sideways(p):
        block = kv.at[p, core, x]
        return remote(block, block, xs.at[p], xr.at[p], {"tp": across})

    def from_side(p):
        block = kv.at[p, core, 1 - x]
        remote(block, block, xs.at[p], xr.at[p], partner).wait_recv()

    def hand(p, side):
        block = kv.at[p, core, side]
        return remote(block, block, ds.at[p, side], dr.at[p, side], partner)

    def handed(p, side):
        block = kv.at[p, other, side]
        remote(block, block, ds.at[p, side], dr.at[p, side], partner).wait_recv()

    for j in range(1, chips):

        @pl.when(chip + j < chips)
        def _():
            to_plane(chip + j).start()

        @pl.when(chip - j >= 0)
        def _():
            to_plane(chip - j).start()

    for side in range(2):
        hand(chip, side).start()
    inform = [
        remote(sheet.at[me], sheet.at[me], ns.at[d], nr.at[d], {"sp": p})
        for d, p in enumerate(peers)
    ]
    for c in inform:
        c.start()

    @pl.loop(0, heads)
    def _(h):
        @pl.loop(0, rows // GRID_W)
        def _(g):
            span = pl.ds(pl.multiple_of(g * GRID_W, GRID_W), GRID_W)
            block = q_ref[span, pl.ds(pl.multiple_of(h * size, size), size)]
            qs[h, span] = turned(block, qg_ref[...], g)

        top[h] = jnp.full(top.shape[1:], NEG_START, jnp.float32)
        acc[h] = jnp.zeros(acc.shape[1:], jnp.float32)

    grade = size ** (-0.5) * 1.4426950408889634

    def first(j, way):
        block = held.at[mine, j]
        where = (across, along)[way]
        return remote(block, block, fs.at[j, way], fr.at[j, way], {"tp": where})

    upper, lower = pl.ds(0, rows // 2), pl.ds(rows // 2, rows // 2)

    def second(j, way):
        block = (held.at[across, j, upper], held.at[along, j, lower])[way]
        where = (along, across)[way]
        return remote(block, block, fs.at[j, 2 + way], fr.at[j, 2 + way], {"tp": where})

    def arrive(j, way):
        block = (
            held.at[across, j],
            held.at[along, j],
            held.at[corner, j, upper],
            held.at[corner, j, lower],
        )[way]
        remote(block, block, fs.at[j, way], fr.at[j, way], partner).wait_recv()

    def bring(p):
        from_plane(p)
        sideways(p).start()
        hand(p, x).start()

    def bring_side(p):
        from_side(p)
        hand(p, 1 - x).start()

    @pl.loop(0, chips)
    def _(s):
        p = visit(chip, chips, s)
        for side in range(2):
            handed(p, side)

        @pl.loop(0, pairs)
        def _(j):
            for i in range(2):
                h = 2 * j + i
                keys = kv[p, :, :, 0].reshape(2 * rows, size)
                values = kv[p, :, :, 1].reshape(2 * rows, size)
                scores = lax.dot_general(
                    qs[h], keys, (((1,), (1,)), ((), ())), preferred_element_type=jnp.float32
                )
                old = top[h]
                new = jnp.maximum(old, jnp.max(scores, axis=1, keepdims=True))
                top[h] = new
                weights = jnp.exp2((scores - new[:, :1]) * grade).astype(jnp.bfloat16)
                full = jnp.concatenate([values, jnp.ones_like(values)], axis=1)
                grown = jnp.dot(weights, full, preferred_element_type=jnp.float32)
                factor = jnp.exp2((old - new) * grade)
                acc[h] = acc[h] * jnp.concatenate([factor, factor], axis=1) + grown

            @pl.when(s == chips - 1)
            def _():
                for i in range(2):
                    done = acc[2 * j + i]
                    ratio = done[:, :size] / done[:, size:]
                    held[mine, j, :, i * size : (i + 1) * size] = ratio.astype(held.dtype)
                first(j, 0).start()
                first(j, 1).start()

        @pl.when(s == 0)
        def _():
            bring(visit(chip, chips, 1))

        @pl.when(s + 2 < chips)
        def _():
            bring(visit(chip, chips, s + 2))

        @pl.when(s + 1 < chips)
        def _():
            bring_side(visit(chip, chips, s + 1))

        @pl.when(s == chips - 2)
        def _():
            for c in inform:
                c.wait_recv()
            notes_ref[mine] = sheet[...]
            for i, p in enumerate((corner, across, along)):
                remote(sheet, notes_ref.at[mine], tell.at[i], told.at[i], {"tp": p}).start()

    fetch.wait()

    def term(owner, j):
        start = pl.multiple_of(owner * width + j * 2 * size, 2 * size)
        part = w[pl.ds(start, 2 * size), :]
        total[...] += jnp.dot(held[owner, j], part, preferred_element_type=jnp.float32)

    total[...] = jnp.zeros_like(total)

    @pl.loop(0, pairs)
    def _(j):
        term(mine, j)

    @pl.loop(0, pairs)
    def _(j):
        arrive(j, 0)
        second(j, 0).start()
        arrive(j, 1)
        second(j, 1).start()
        term(across, j)
        term(along, j)

    @pl.loop(0, pairs)
    def _(j):
        arrive(j, 2)
        arrive(j, 3)
        term(corner, j)

    stage[...] = total[...].astype(stage.dtype)
    columns = pl.ds(pl.multiple_of(mine * width, width), width)

    def piece(owner):
        return pl.ds(pl.multiple_of(owner * share, share), share)

    back = [
        remote(stage.at[piece(p)], proj.at[:, columns], give.at[i], take.at[i], {"tp": p})
        for i, p in enumerate((corner, across, along))
    ]
    for c in back:
        c.start()
    proj[:, columns] = stage[piece(mine), :]
    for c in back:
        c.wait()
    mixed = (res_ref[...].astype(jnp.float32) + proj[...].astype(jnp.float32)).astype(mixed_ref.dtype)
    mixed_ref[...] = mixed
    mixed = mixed.astype(jnp.float32)
    mean = jnp.mean(mixed * mixed, axis=-1, keepdims=True)
    normed_ref[...] = (mixed * lax.rsqrt(mean + EPS) * gain_ref[...]).astype(normed_ref.dtype)

    for i, p in enumerate((corner, across, along)):
        remote(sheet, notes_ref.at[mine], tell.at[i], told.at[i], {"tp": p}).wait()

    def settle_sends():
        for c in inform:
            c.wait_send()
        for d in range(1, chips):
            p = lax.rem(chip + d, chips)
            to_plane(p).wait_send()
            sideways(p).wait_send()
        for p in range(chips):
            for side in range(2):
                hand(p, side).wait_send()
        for j in range(pairs):
            for way in range(2):
                first(j, way).wait_send()
                second(j, way).wait_send()

    return settle_sends


def visit(chip, chips, step):
    near = jnp.minimum(chip, chips - 1 - chip)
    up = chip < chips - 1 - chip
    swing = (step + 1) // 2 * (2 * lax.rem(step, 2) - 1)
    swing = jnp.where(up, chip + swing, chip - swing)
    tail = jnp.where(up, chip + (step - near), chip - (step - near))
    return jnp.where(step <= 2 * near, swing, tail)


def wide(value):
    return value.astype(jnp.float32)


def moe_part(
    n, cuts, x_ref, note_ref, mixed_ref, loads, out_ref,
    tok, wg, wu, wd, picked, hid, wsel, held, own, give, take,
    low, high, from_x, from_y, to_y, to_x, last_y, last_x, acc, zsend, zrecv, zmid,
    zs, zr, sq_s, sq_r, pd_s, pd_r, tk_s, tk_r, hop_s, hop_r, hz_s, hz_r, mid_r,
):
    me = lax.axis_index("sp")
    chips = n // 2
    chip, core = me // 2, lax.rem(me, 2)
    other = 1 - core
    partner = {"sp": 2 * chip + other}
    mine, across, along, corner = square()
    x, y = lax.rem(mine, 2), mine // 2
    share, depth = x_ref.shape
    units = wg.shape[1]
    group = 4 * share
    slots = wsel.shape[3] // 2
    width = depth // cuts
    half = width // 2
    steps = chips * cuts

    def column(k):
        return pl.ds(pl.multiple_of(k * width, width), width)

    has_right, has_left = chip < chips - 1, chip > 0

    def cols(h):
        return pl.ds(pl.multiple_of(h * (depth // 2), depth // 2), depth // 2)

    def own_half(h):
        return x_ref.at[:, cols(h)]

    def along_z(p, h, way, first=False):
        block = tok.at[p, core, h, mine]
        to = 2 * (chip + 1 - 2 * way) + core
        return remote(
            own_half(h) if first else block, block, zs.at[p, h, way], zr.at[p, h], {"sp": to}
        )

    upper, lower = pl.ds(0, share // 2), pl.ds(share // 2, share // 2)

    def pass_on(p, h, way, first=False):
        block = tok.at[p, core, h]
        start = own_half(h) if first else block.at[mine]
        src, dst, where = (
            (start, block.at[mine], across),
            (start, block.at[mine], along),
            (block.at[across, upper], block.at[across, upper], along),
            (block.at[along, lower], block.at[along, lower], across),
        )[way]
        return remote(src, dst, sq_s.at[way], sq_r.at[p, h, way], {"tp": where})

    def arrive(p, h, way):
        block = tok.at[p, core, h]
        dst = (
            block.at[across],
            block.at[along],
            block.at[corner, upper],
            block.at[corner, lower],
        )[way]
        remote(dst, dst, sq_s.at[way], sq_r.at[p, h, way], {"tp": across}).wait_recv()

    def hand(p, h, t, first=False):
        block = tok.at[p, core, h, t]
        src = own_half(h) if first else block
        return remote(src, block, pd_s.at[0], pd_r.at[p, h, t], partner)

    def handed(p, h, t):
        block = tok.at[p, other, h, t]
        remote(block, block, pd_s.at[0], pd_r.at[p, h, t], partner).wait_recv()

    for h in range(2):
        pass_on(chip, h, 0, True).start()
        pass_on(chip, h, 1, True).start()

        @pl.when(has_right)
        def _():
            along_z(chip, h, 0, True).start()

        @pl.when(has_left)
        def _():
            along_z(chip, h, 1, True).start()

        hand(chip, h, mine, True).start()
        tok[chip, core, h, mine] = x_ref[:, cols(h)]

    def part(u):
        return visit(chip, chips, u // 2), lax.rem(u, 2)

    def finish(u):
        p, h = part(u)
        arrive(p, h, 2)
        arrive(p, h, 3)
        hand(p, h, corner).start()

    def wait_rows(p):
        for h in range(2):
            for t in range(4):
                handed(p, h, t)

    def pick_rows(p, side):
        tiles = [note_ref[t, 2 * p + side] for t in range(4)]
        lane = lax.broadcasted_iota(jnp.int32, (n, 2 * share), 1)
        chosen = lax.broadcasted_iota(jnp.int32, (n, 2 * share), 0) == me

        def across_two(even, odd, swap_even):
            moved = pltpu.roll(even if swap_even else odd, share, 1)
            return jnp.where(lane < share, moved, odd) if swap_even else jnp.where(
                lane < share, even, moved
            )

        def row_of(swap_even):
            parts_two = [across_two(tiles[t], tiles[t + 1], swap_even) for t in (0, 2)]
            picks = [
                jnp.sum(jnp.where(chosen, v, 0.0), axis=0, keepdims=True) for v in parts_two
            ]
            return jnp.concatenate(picks, axis=1)

        spot = row_of(False)
        base = lax.broadcasted_iota(jnp.int32, (1, group), 1) // share * (slots // 4)
        spot = jnp.where(spot >= 0, spot.astype(jnp.int32) + base, -1)
        weight = row_of(True)
        coarse = weight.astype(jnp.bfloat16).astype(jnp.float32)
        parts = (coarse, weight - coarse)
        hit = lax.broadcasted_iota(jnp.int32, (slots, group), 0) == spot
        pick = jnp.where(hit, 1.0, 0.0).astype(tok.dtype)
        for i in range(2):
            turned = jnp.transpose(jnp.where(hit, parts[i], 0.0))
            wsel[p, side, :, i * slots : (i + 1) * slots] = turned.astype(wsel.dtype)
        for h in range(2):
            block = tok[p, side, h].reshape(group, depth // 2)
            rows = jnp.dot(pick, block, preferred_element_type=jnp.float32)
            picked[side * slots : (side + 1) * slots, cols(h)] = rows.astype(picked.dtype)

    def activate(p, u):
        some = pl.ds(pl.multiple_of(u * 512, 512), 512)
        gate = jnp.dot(picked[...], wg[:, some], preferred_element_type=jnp.float32)
        rise = jnp.dot(picked[...], wu[:, some], preferred_element_type=jnp.float32)
        hid[p, :, some] = (jax.nn.silu(gate) * rise).astype(hid.dtype)

    def expert(p):
        wait_rows(p)
        pick_rows(p, 0)
        pick_rows(p, 1)

        @pl.loop(0, units // 512)
        def _(u):
            activate(p, u)

    def forward(u):
        p, h = part(u)
        arrive(p, h, 0)
        pass_on(p, h, 2).start()
        hand(p, h, across).start()
        arrive(p, h, 1)
        pass_on(p, h, 3).start()
        hand(p, h, along).start()

    last = 2 * chips - 1

    def passes(p):
        return ((p < chip) & has_right) | ((p > chip) & has_left)

    def relay(u):
        p, h = part(u)

        @pl.when(passes(p))
        def _():
            along_z(p, h, 0).wait_recv()

        @pl.when((p < chip) & has_right)
        def _():
            along_z(p, h, 0).start()

        @pl.when((p > chip) & has_left)
        def _():
            along_z(p, h, 1).start()

    def open_up(u):
        p, h = part(u)

        @pl.when(jnp.logical_not(passes(p)))
        def _():
            along_z(p, h, 0).wait_recv()

        pass_on(p, h, 0).start()
        pass_on(p, h, 1).start()
        hand(p, h, mine).start()

    relay(2)
    open_up(2)

    @pl.loop(0, last)
    def _(u):
        forward(u)

        @pl.when(u + 4 <= last)
        def _():
            relay(u + 4)

        @pl.when(u == 0)
        def _():
            relay(3)

        @pl.when(u + 3 <= last)
        def _():
            open_up(u + 3)

        @pl.when(u == 0)
        def _():
            for c in loads:
                c.wait()

        @pl.when((u == 4) | ((u > 4) & (lax.rem(u, 2) == 1)))
        def _():
            expert(visit(chip, chips, (u - 3) // 2))

        @pl.when((u >= 2) & (lax.rem(u, 2) == 0))
        def _():
            finish(u - 2)

            @pl.when(u < last - 1)
            def _():
                finish(u - 1)

    def plane_of(k):
        return visit(chip, chips, lax.rem(k // cuts + 1, chips))

    def swap(k):
        return remote(give.at[k], take.at[k], tk_s.at[0], tk_r.at[k], partner)

    def hop(k, way):
        src, dst, where = (
            (low.at[k, 1 - x], from_x.at[k], across),
            (high.at[k, 1 - y], from_y.at[k], along),
            (to_y.at[k], last_y.at[k], along),
            (to_x.at[k], last_x.at[k], across),
        )[way]
        return remote(src, dst, hop_s.at[way], hop_r.at[k, way], {"tp": where})

    def home(k):
        p, q = plane_of(k), lax.rem(k, cuts)
        return remote(
            zsend.at[k], zrecv.at[chip, q], hz_s.at[0], hz_r.at[chip, q], {"sp": 2 * p + core}
        )

    is_end = (chip == 0) | (chip == chips - 1)

    def lend(k):
        to = chip + jnp.where(chip == 0, 1, -1)
        return remote(
            zsend.at[k], zmid.at[lax.rem(k, cuts)], hz_s.at[0], mid_r.at[lax.rem(k, cuts)],
            {"sp": 2 * to + core},
        )

    def homed(p, q):
        return remote(zsend.at[0], zrecv.at[p, q], hz_s.at[0], hz_r.at[p, q], partner)

    def settle(k):
        swap(k).wait_recv()
        total = own[lax.rem(k, 3)] + wide(take[k])
        cast = total.astype(low.dtype).reshape(4, share, width)
        for t in range(4):
            low[k, t % 2, t // 2] = cast[t, :, :half]
            high[k, t // 2, t % 2] = cast[t, :, half:]
        hop(k, 0).start()
        hop(k, 1).start()

    @pl.loop(0, steps + 6)
    def _(step):
        @pl.when((step >= 2) & (step < steps + 2))
        def _():
            settle(step - 2)

        @pl.when((step >= 4) & (step < steps + 4))
        def _(k=step - 4):
            hop(k, 0).wait_recv()
            to_y[k] = (wide(low[k, x, 1 - y]) + wide(from_x[k, 1 - y])).astype(to_y.dtype)
            hop(k, 2).start()
            hop(k, 1).wait_recv()
            to_x[k] = (wide(high[k, y, 1 - x]) + wide(from_y[k, 1 - x])).astype(to_x.dtype)
            hop(k, 3).start()

        @pl.when(step >= 6)
        def _(k=step - 6):
            hop(k, 2).wait_recv()
            left = wide(low[k, x, y]) + wide(from_x[k, y]) + wide(last_y[k])
            hop(k, 3).wait_recv()
            right = wide(high[k, y, x]) + wide(from_y[k, x]) + wide(last_x[k])

            far = (k >= steps - 2 * cuts) & (k < steps - cuts)

            @pl.when((k < steps - cuts) & jnp.logical_not(far & jnp.logical_not(is_end)))
            def _():
                zsend[k, :, :half] = left.astype(zsend.dtype)
                zsend[k, :, half:] = right.astype(zsend.dtype)

                @pl.when(far)
                def _():
                    lend(k).start()

                @pl.when(jnp.logical_not(far))
                def _():
                    home(k).start()

            @pl.when(far & jnp.logical_not(is_end))
            def _():
                lend(k).wait_recv()
                more = wide(zmid[lax.rem(k, cuts)])
                zsend[k, :, :half] = (left + more[:, :half]).astype(zsend.dtype)
                zsend[k, :, half:] = (right + more[:, half:]).astype(zsend.dtype)
                home(k).start()

            @pl.when(k >= steps - cuts)
            def _():
                acc[lax.rem(k, cuts), :, :half] = left
                acc[lax.rem(k, cuts), :, half:] = right

        @pl.when(step < steps)
        def _(k=step):
            third, fourth = visit(chip, chips, chips - 2), visit(chip, chips, chips - 1)

            @pl.when(k == cuts)
            def _():
                @pl.loop(0, units // 512)
                def _(u):
                    activate(third, u)

            p, q = plane_of(k), lax.rem(k, cuts)
            out = jnp.dot(hid[p], wd[q], preferred_element_type=jnp.float32).astype(held.dtype)
            for side in range(2):
                block = out[side * slots : (side + 1) * slots]
                held[side, :slots] = block
                held[side, slots:] = block

            def spread(side):
                return jnp.dot(wsel[p, side], held[side], preferred_element_type=jnp.float32)

            give[k] = spread(other).astype(give.dtype)
            swap(k).start()
            own[lax.rem(k, 3)] = spread(core)

            @pl.when(k == cuts // 2)
            def _():
                forward(last)
                finish(last - 2)

            @pl.when(k == cuts)
            def _():
                finish(last - 1)
                finish(last)

            @pl.when((k == cuts - 1) | (k == cuts + 1))
            def _():
                p = jnp.where(k < cuts, third, fourth)
                wait_rows(p)
                pick_rows(p, 0)
                pick_rows(p, 1)

            each = units // 1024

            @pl.when((k >= cuts + 2) & (k < cuts + 4))
            def _():
                @pl.loop(0, each)
                def _(u):
                    activate(fourth, (k - cuts - 2) * each + u)

    @pl.loop(0, cuts)
    def _(q):
        for d in range(1, chips):
            p = lax.rem(chip + d, chips)

            @pl.when(jnp.logical_not(is_end & (p == chips - 1 - chip)))
            def _():
                homed(p, q).wait_recv()
                acc[q] += wide(zrecv[p, q])

        out_ref[:, column(q)] = (acc[q] + wide(mixed_ref[:, column(q)])).astype(out_ref.dtype)

    @pl.loop(0, 2 * chips)
    def _(u):
        p, h = u // 2, lax.rem(u, 2)
        @pl.when((p <= chip) & has_right)
        def _():
            along_z(p, h, 0).wait_send()

        @pl.when((p >= chip) & has_left)
        def _():
            along_z(p, h, 1).wait_send()

    def all_left(ref, sem):
        remote(ref, ref, sem, sem, partner).wait_send()

    whole = tok.at[:, 0, :, 0]
    for way, ref in enumerate((whole, whole, whole.at[:, :, upper], whole.at[:, :, lower])):
        all_left(ref, sq_s.at[way])
    all_left(tok.at[:, 0], pd_s.at[0])
    all_left(give, tk_s.at[0])
    for way, ref in enumerate((from_x, from_y, to_y, to_x)):
        all_left(ref, hop_s.at[way])
    all_left(zsend, hz_s.at[0])


def layer_kernel(n, cuts, *refs):
    attend_in, (wg_ref, wu_ref, wd_ref, out_ref), refs = refs[:12], refs[12:16], refs[16:]
    (mixed, normed, notes, load), refs = refs[:4], refs[4:]
    attend_room, moe_room = refs[:27], refs[27:]
    tok, wg, wu, wd = moe_room[:4]
    width = wd.shape[2]
    loads = [
        pltpu.make_async_copy(wg_ref.at[0], wg, load.at[0]),
        pltpu.make_async_copy(wu_ref.at[0], wu, load.at[1]),
    ] + [
        pltpu.make_async_copy(wd_ref.at[0, :, pl.ds(q * width, width)], wd.at[q], load.at[2 + q])
        for q in range(cuts)
    ]
    settle_sends = attend_part(n, *attend_in, mixed, normed, notes, loads, *attend_room)
    moe_part(n, cuts, normed, notes, mixed, loads, out_ref, *moe_room)
    settle_sends()


def layer(
    n, queries, keys, values, query_gain, key_gain, residual, gain, names, shares, out_proj,
    w_gate, w_up, w_down, capacity, cuts=4,
):
    rows, width = queries.shape
    size = query_gain.shape[0]
    heads = width // size
    share, depth = residual.shape
    units = w_gate.shape[2]
    chips = n // 2
    kind = queries.dtype
    cut = depth // cuts
    half = cut // 2
    steps = chips * cuts
    group, slots = 4 * share, 4 * capacity
    by_col, by_row = turn_tables(size, n * rows // GRID_W)
    dma = pltpu.SemaphoreType.DMA

    def room(*extent):
        return pltpu.VMEM(extent, kind)

    def exact(*extent):
        return pltpu.VMEM(extent, jnp.float32)

    return pl.pallas_call(
        functools.partial(layer_kernel, n, cuts),
        out_shape=jax.ShapeDtypeStruct((share, depth), kind),
        in_specs=in_vmem(11) + [pl.BlockSpec(memory_space=pl.ANY)] * 4,
        out_specs=in_vmem(1)[0],
        scratch_shapes=[
            room(share, depth),
            room(share, depth),
            exact(4, n, n, 2 * share),
            dma((2 + cuts,)),
            room(*out_proj.shape),
            room(chips, 2, 2, 2, rows // 2, size),
            room(heads, rows, size),
            exact(heads, rows, size),
            exact(heads, rows, 2 * size),
            room(4, heads // 2, rows, 2 * size),
            exact(rows, width),
            room(rows, width),
            room(share, depth),
            exact(n, n, 2 * share),
            dma((1,)),
            dma((chips,)),
            dma((chips,)),
            dma((chips,)),
            dma((chips,)),
            dma((chips, 2)),
            dma((chips, 2)),
            dma((n - 1,)),
            dma((n - 1,)),
            dma((heads // 2, 4)),
            dma((heads // 2, 4)),
            dma((3,)),
            dma((3,)),
            dma((3,)),
            dma((3,)),
            exact(n, 2 * share),
            exact(n, 2 * share),
            room(chips, 2, 2, 4, share, depth // 2),
            room(depth, units),
            room(depth, units),
            room(cuts, units, cut),
            room(2 * slots, depth),
            room(chips, 2 * slots, units),
            room(chips, 2, group, 2 * slots),
            room(2, 2 * slots, cut),
            exact(3, group, cut),
            room(steps, group, cut),
            room(steps, group, cut),
            room(steps, 2, 2, share, half),
            room(steps, 2, 2, share, half),
            room(steps, 2, share, half),
            room(steps, 2, share, half),
            room(steps, share, half),
            room(steps, share, half),
            room(steps, share, half),
            room(steps, share, half),
            exact(cuts, share, cut),
            room(steps - cuts, share, cut),
            room(chips, cuts, share, cut),
            room(cuts, share, cut),
            dma((chips, 2, 2)),
            dma((chips, 2)),
            dma((4,)),
            dma((chips, 2, 4)),
            dma((1,)),
            dma((chips, 2, 4)),
            dma((1,)),
            dma((steps,)),
            dma((4,)),
            dma((steps, 4)),
            dma((1,)),
            dma((chips, cuts)),
            dma((cuts,)),
        ],
        compiler_params=params(0),
        name="layer",
    )(
        queries,
        keys,
        values,
        query_gain[None, :],
        key_gain[None, :],
        jnp.asarray(by_col),
        jnp.asarray(by_row),
        residual,
        gain[None, :],
        names,
        shares,
        out_proj,
        w_gate,
        w_up,
        w_down,
    )


def start_state(batch, rows, width):
    return (
        jnp.full((batch, rows), NEG_START, jnp.float32),
        jnp.zeros((batch, rows), jnp.float32),
        jnp.zeros((batch, rows, width), jnp.float32),
    )


def local(
    queries,
    keys,
    values,
    query_gain,
    key_gain,
    out_proj,
    expert_norm_scale,
    residual,
    routes,
    route_weights,
    w_gate,
    w_up,
    w_down,
):
    head_size = query_gain.shape[0]
    tok_sp = queries.shape[0]
    tp_count = lax.axis_size("tp")
    sp_count = lax.axis_size("sp")
    heads_dev = queries.shape[1] // head_size
    all_heads = heads_dev * tp_count
    kv_heads = keys.shape[1] // head_size
    group = all_heads // kv_heads
    scale = head_size ** (-0.5)
    tp_index = lax.axis_index("tp")
    sp_index = lax.axis_index("sp")
    tok_dev = residual.shape[0]
    top = routes.shape[1]
    capacity = max(2, 2 * tok_dev * top // sp_count)
    direct = (
        tp_count == 4
        and sp_count // 2 == 4
        and sp_count % 2 == 0
        and capacity % 16 == 0
        and 2 * tok_dev % 128 == 0
        and tok_sp % (2 * GRID_W) == 0
        and heads_dev % 2 == 0
        and 2 * heads_dev <= group
        and tok_sp == tp_count * tok_dev
    )
    if direct:
        return layer(
            sp_count,
            queries,
            keys,
            values,
            query_gain,
            key_gain,
            residual,
            expert_norm_scale,
            routes.T,
            route_weights.T,
            out_proj,
            w_gate,
            w_up,
            w_down,
            capacity,
        )
    position = sp_index * tok_sp + jnp.arange(tok_sp, dtype=jnp.int32)
    q_rot = prepare(queries, query_gain, position)
    shared_value_head = tp_index * heads_dev // group
    own_keys = prepare(
        lax.dynamic_slice_in_dim(keys, shared_value_head * head_size, head_size, 1),
        key_gain,
        position,
    )
    own_values = lax.dynamic_slice_in_dim(values, shared_value_head * head_size, head_size, 1)
    query_matrix = (
        q_rot.reshape(tok_sp, heads_dev, head_size)
        .transpose(1, 0, 2)
        .reshape(1, heads_dev * tok_sp, head_size)
    )
    key_piece = lax.all_gather(own_keys, "sp", axis=0, tiled=True)
    value_piece = lax.all_gather(own_values, "sp", axis=0, tiled=True)
    run_max, run_sum, run_acc = absorb(
        start_state(1, heads_dev * tok_sp, head_size),
        query_matrix,
        key_piece[:, None, :],
        value_piece[:, None, :],
        scale,
    )
    attn = (run_acc / run_sum[..., None]).astype(jnp.bfloat16)
    attn = (
        attn.reshape(heads_dev, tok_sp, head_size)
        .transpose(1, 0, 2)
        .reshape(tok_sp, heads_dev * head_size)
    )
    columns = jnp.dot(
        lax.all_gather(attn, "tp", axis=1, tiled=True),
        out_proj,
        preferred_element_type=jnp.float32,
    )
    projected = lax.all_to_all(
        columns.astype(jnp.bfloat16), "tp", split_axis=0, concat_axis=1, tiled=True
    )
    mixed_float_output = residual.astype(jnp.float32) + projected.astype(jnp.float32)
    mixed = mixed_float_output.astype(jnp.bfloat16)
    mixed_float_output = mixed.astype(jnp.float32)
    normed = (
        mixed_float_output
        * lax.rsqrt(jnp.mean(mixed_float_output * mixed_float_output, axis=-1, keepdims=True) + EPS)
        * expert_norm_scale
    ).astype(jnp.bfloat16)
    flat_routes = routes.reshape(-1)
    one_hot = (flat_routes[:, None] == jnp.arange(sp_count, dtype=jnp.int32)[None, :]).astype(
        jnp.int32
    )
    earlier = jnp.cumsum(one_hot, axis=0) - one_hot
    slot_index = jnp.sum(earlier * one_hot, axis=1)
    target = flat_routes * capacity + slot_index
    selector = (
        jnp.arange(sp_count * capacity, dtype=jnp.int32)[:, None] == target[None, :]
    ).astype(jnp.bfloat16)
    selector = jnp.sum(selector.reshape(sp_count * capacity, tok_dev, top), axis=2)
    send_rows = jnp.dot(selector, normed, preferred_element_type=jnp.float32).astype(jnp.bfloat16)
    arrived = lax.all_to_all(send_rows, "sp", split_axis=0, concat_axis=0, tiled=True)
    piece = lax.all_gather(arrived, "tp", axis=0, tiled=True)
    gate = jnp.dot(piece, w_gate[0], preferred_element_type=jnp.float32)
    upper = jnp.dot(piece, w_up[0], preferred_element_type=jnp.float32)
    hidden = (jax.nn.silu(gate) * upper).astype(jnp.bfloat16)
    partial = jnp.dot(hidden, w_down[0], preferred_element_type=jnp.float32).astype(jnp.bfloat16)
    expert_out = lax.psum_scatter(partial, "tp", scatter_dimension=0, tiled=True)
    returned = lax.all_to_all(expert_out, "sp", split_axis=0, concat_axis=0, tiled=True)
    picked = (
        jnp.take(returned, target, axis=0)
        .astype(jnp.float32)
        .reshape(tok_dev, top, returned.shape[1])
    )
    moe_sum = jnp.sum(picked * route_weights[:, :, None], axis=1)
    return (mixed_float_output + moe_sum).astype(jnp.bfloat16)


def solution(mesh):
    placed = (
        P("sp", "tp"),
        P("sp", None),
        P("sp", None),
        P(),
        P(),
        P(None, "tp"),
        P(),
        P(("sp", "tp"), None),
        P(("sp", "tp"), None),
        P(("sp", "tp"), None),
        P("sp", None, "tp"),
        P("sp", None, "tp"),
        P("sp", "tp", None),
    )
    return jax.shard_map(
        local, mesh=mesh, in_specs=placed, out_specs=P(("sp", "tp"), None), check_vma=False
    )
```

```python
import functools

import jax
import jax.numpy as jnp
import numpy as np
from jax import lax
from jax.experimental import pallas as pl
from jax.experimental.pallas import tpu as pltpu
from jax.sharding import PartitionSpec as P

GRID_W = 64


EPS = 1e-06
ROPE_BASE = 10000.0
NEG_START = -1e30


def rotate(field, position):
    half = field.shape[-1] // 2
    quarter = half // 2
    freqs = ROPE_BASE ** (-jnp.arange(quarter, dtype=jnp.float32) / quarter)
    grid_row = (position // GRID_W).astype(jnp.float32)
    grid_col = (position % GRID_W).astype(jnp.float32)

    def turn_half(part, coord):
        angle = coord[:, None] * freqs[None, :]
        cosine = jnp.cos(angle)[:, None, :]
        sine = jnp.sin(angle)[:, None, :]
        first, second = (part[..., :quarter], part[..., quarter:])
        return jnp.concatenate(
            [first * cosine - second * sine, second * cosine + first * sine], axis=-1
        )

    return jnp.concatenate(
        [turn_half(field[..., :half], grid_row), turn_half(field[..., half:], grid_col)], axis=-1
    )


def prepare(field, gain, position):
    count = field.shape[0]
    width = gain.shape[0]
    heads_here = field.shape[1] // width
    values_f = field.reshape(count, heads_here, width).astype(jnp.float32)
    scaled = (
        values_f * lax.rsqrt(jnp.mean(values_f * values_f, axis=-1, keepdims=True) + EPS) * gain
    )
    return rotate(scaled, position).reshape(count, heads_here * width).astype(jnp.bfloat16)


def absorb(carry, query_matrix, key_rows, value_rows, scale):
    count = key_rows.shape[0]
    width = 2048 if count > 2048 and count % 2048 == 0 else count
    key_blocks = key_rows.reshape(count // width, width, key_rows.shape[1], key_rows.shape[2])
    value_blocks = value_rows.reshape(
        count // width, width, value_rows.shape[1], value_rows.shape[2]
    )

    def step(state, block):
        run_max, run_sum, run_acc = state
        key_tile_rows, value_tile_rows = block
        scores = (
            jnp.einsum(
                "hxt,ght->hxg", query_matrix, key_tile_rows, preferred_element_type=jnp.float32
            )
            * scale
        )
        new_max = jnp.maximum(run_max, jnp.max(scores, axis=-1))
        weight_tensors = jnp.exp(scores - new_max[..., None]).astype(jnp.bfloat16)
        factor = jnp.exp(run_max - new_max)
        run_sum = run_sum * factor + jnp.sum(weight_tensors.astype(jnp.float32), axis=-1)
        run_acc = run_acc * factor[..., None] + jnp.einsum(
            "zij,jzu->ziu", weight_tensors, value_tile_rows, preferred_element_type=jnp.float32
        )
        return ((new_max, run_sum, run_acc), None)

    result, unused = lax.scan(step, carry, (key_blocks, value_blocks))
    return result


MESH = pl.DeviceIdType.MESH
VMEM_LIMIT = 60 * 1024 * 1024


def greet(partners, count):
    barrier = pltpu.get_barrier_semaphore()
    for where in partners:
        pl.semaphore_signal(barrier, inc=1, device_id=where, device_id_type=MESH)
    pl.semaphore_wait(barrier, count)


def remote(src, dst, send, recv, where):
    return pltpu.make_async_remote_copy(
        src_ref=src, dst_ref=dst, send_sem=send, recv_sem=recv, device_id=where, device_id_type=MESH
    )


def square():
    mine = lax.axis_index("tp")
    return mine, mine + 1 - 2 * lax.rem(mine, 2), lax.rem(mine + 2, 4), 3 - mine


def in_vmem(count):
    return [pl.BlockSpec(memory_space=pltpu.VMEM)] * count


def params(number):
    return pltpu.CompilerParams(
        collective_id=number, has_side_effects=True, vmem_limit_bytes=VMEM_LIMIT
    )


def turn_tables(width, rows):
    quarter = width // 4
    freqs = ROPE_BASE ** (-np.arange(quarter, dtype=np.float32) / np.float32(quarter))
    zero = np.zeros((max(rows, GRID_W), quarter), np.float32)

    def table(count, blocks):
        angle = np.arange(count, dtype=np.float32)[:, None] * freqs.astype(np.float32)[None, :]
        kinds = {"c": np.cos(angle), "s": np.sin(angle), "m": -np.sin(angle), "0": zero[:count]}
        return np.stack([np.concatenate([kinds[k] for k in b], axis=1) for b in blocks])

    by_col = table(GRID_W, ("00cc", "00m0", "000s"))
    by_row = table(rows, ("cc00", "m000", "0s00"))
    return by_col.astype(np.float32), by_row.astype(np.float32)


def attend_part(
    n, q_ref, k_ref, v_ref, qg_ref, kg_ref, col_ref, row_ref, res_ref, gain_ref, name_ref, share_ref, w_ref,
    mixed_ref, normed_ref, notes_ref, loads,
    w, kv, qs, top, acc, held, total, stage, proj, sheet,
    load, zs, zr, xs, xr, ds, dr, ns, nr, fs, fr, give, take, tell, told, names, shares,
):
    me = lax.axis_index("sp")
    chips = n // 2
    chip, core = me // 2, lax.rem(me, 2)
    other = 1 - core
    partner = {"sp": 2 * chip + other}
    mine, across, along, corner = square()
    x = lax.rem(mine, 2)
    rows, width = q_ref.shape
    size = qg_ref.shape[1]
    heads = width // size
    pairs = heads // 2
    share = rows // 4
    keys_half = rows // 2
    fetch = pltpu.make_async_copy(w_ref, w, load.at[0])
    fetch.start()
    for c in loads:
        c.start()

    barrier = pltpu.get_barrier_semaphore()
    peers = [lax.rem(me + d, n) for d in range(1, n)]
    for p in peers:
        pl.semaphore_signal(barrier, inc=1, device_id={"sp": p}, device_id_type=MESH)
    for p in (across, along, corner):
        pl.semaphore_signal(barrier, inc=1, device_id={"tp": p}, device_id_type=MESH)

    def turned(part, gain_row, g):
        values = part.astype(jnp.float32)
        mean = jnp.mean(values * values, axis=-1, keepdims=True)
        scaled = values * lax.rsqrt(mean + EPS) * gain_row
        grid_row = pl.ds(me * (rows // GRID_W) + g, 1)
        turn = [col_ref[i] + row_ref[i, grid_row] for i in range(3)]
        return (
            scaled * turn[0]
            + pltpu.roll(scaled, size - size // 4, 1) * turn[1]
            + pltpu.roll(scaled, size // 4, 1) * turn[2]
        ).astype(jnp.bfloat16)

    kv_heads = k_ref.shape[1] // size
    kv_head = mine * kv_heads // 4
    at = pl.ds(pl.multiple_of(kv_head * size, size), size)
    for g in range(rows // GRID_W):
        span = pl.ds(g * GRID_W, GRID_W)
        side, low = (g * GRID_W) // keys_half, (g * GRID_W) % keys_half
        place = pl.ds(low, GRID_W)
        kv[chip, core, side, 0, place] = turned(k_ref[span, at], kg_ref[...], g)
        kv[chip, core, side, 1, place] = v_ref[span, at]
    lanes = lax.broadcasted_iota(jnp.int32, (n, 2 * share), 1)
    expert = lax.broadcasted_iota(jnp.int32, (n, 2 * share), 0)
    def as_rows(ref, into):
        into[:, :share] = jnp.broadcast_to(ref[0:1].astype(jnp.float32), (n, share))
        into[:, share:] = jnp.broadcast_to(ref[1:2].astype(jnp.float32), (n, share))
        both = into[...]
        swapped = pltpu.roll(both, share, 1)
        return jnp.where(lanes < share, both, swapped), jnp.where(lanes < share, swapped, both)

    first_one, second_one = [r.astype(jnp.int32) == expert for r in as_rows(name_ref, names)]
    first_part, second_part = as_rows(share_ref, shares)
    taken = jnp.where((first_one | second_one) & (lanes < share), 1.0, 0.0)
    before = lax.broadcasted_iota(jnp.int32, (2 * share, 2 * share), 0)
    after = lax.broadcasted_iota(jnp.int32, (2 * share, 2 * share), 1)
    ladder = jnp.where(before < after, 1.0, 0.0).astype(jnp.bfloat16)
    slot = jnp.dot(taken.astype(jnp.bfloat16), ladder, preferred_element_type=jnp.float32)
    weight = jnp.where(first_one, first_part, 0.0) + jnp.where(second_one, second_part, 0.0)
    sheet[me] = jnp.where(lanes < share, jnp.where(taken > 0, slot, -1.0), weight)

    @pl.loop(0, heads // 2)
    def _(h):
        @pl.loop(0, rows // GRID_W)
        def _(g):
            span = pl.ds(pl.multiple_of(g * GRID_W, GRID_W), GRID_W)
            block = q_ref[span, pl.ds(pl.multiple_of(h * size, size), size)]
            qs[h, span] = turned(block, qg_ref[...], g)

        top[h] = jnp.full(top.shape[1:], NEG_START, jnp.float32)
        acc[h] = jnp.zeros(acc.shape[1:], jnp.float32)

    pl.semaphore_wait(barrier, n + 2)

    def to_plane(p):
        block = kv.at[chip, core, x]
        return remote(block, block, zs.at[p], zr.at[chip], {"sp": 2 * p + core})

    def from_plane(p):
        block = kv.at[p, core, x]
        remote(block, block, zs.at[p], zr.at[p], partner).wait_recv()

    def sideways(p):
        block = kv.at[p, core, x]
        return remote(block, block, xs.at[p], xr.at[p], {"tp": across})

    def from_side(p):
        block = kv.at[p, core, 1 - x]
        remote(block, block, xs.at[p], xr.at[p], partner).wait_recv()

    def hand(p, side):
        block = kv.at[p, core, side]
        return remote(block, block, ds.at[p, side], dr.at[p, side], partner)

    def handed(p, side):
        block = kv.at[p, other, side]
        remote(block, block, ds.at[p, side], dr.at[p, side], partner).wait_recv()

    for j in range(1, chips):

        @pl.when(chip + j < chips)
        def _():
            to_plane(chip + j).start()

        @pl.when(chip - j >= 0)
        def _():
            to_plane(chip - j).start()

    for side in range(2):
        hand(chip, side).start()
    inform = [
        remote(sheet.at[me], sheet.at[me], ns.at[d], nr.at[d], {"sp": p})
        for d, p in enumerate(peers)
    ]
    for c in inform:
        c.start()

    @pl.loop(heads // 2, heads)
    def _(h):
        @pl.loop(0, rows // GRID_W)
        def _(g):
            span = pl.ds(pl.multiple_of(g * GRID_W, GRID_W), GRID_W)
            block = q_ref[span, pl.ds(pl.multiple_of(h * size, size), size)]
            qs[h, span] = turned(block, qg_ref[...], g)

        top[h] = jnp.full(top.shape[1:], NEG_START, jnp.float32)
        acc[h] = jnp.zeros(acc.shape[1:], jnp.float32)

    grade = size ** (-0.5) * 1.4426950408889634

    def first(j, way):
        block = held.at[mine, j]
        where = (across, along)[way]
        return remote(block, block, fs.at[j, way], fr.at[j, way], {"tp": where})

    upper, lower = pl.ds(0, rows // 2), pl.ds(rows // 2, rows // 2)

    def second(j, way):
        block = (held.at[across, j, upper], held.at[along, j, lower])[way]
        where = (along, across)[way]
        return remote(block, block, fs.at[j, 2 + way], fr.at[j, 2 + way], {"tp": where})

    def arrive(j, way):
        block = (
            held.at[across, j],
            held.at[along, j],
            held.at[corner, j, upper],
            held.at[corner, j, lower],
        )[way]
        remote(block, block, fs.at[j, way], fr.at[j, way], partner).wait_recv()

    def bring(p):
        from_plane(p)
        sideways(p).start()
        hand(p, x).start()

    def bring_side(p):
        from_side(p)
        hand(p, 1 - x).start()

    @pl.loop(0, chips)
    def _(s):
        p = visit(chip, chips, s)
        for side in range(2):
            handed(p, side)

        @pl.loop(0, pairs)
        def _(j):
            for i in range(2):
                h = 2 * j + i
                keys = kv[p, :, :, 0].reshape(2 * rows, size)
                values = kv[p, :, :, 1].reshape(2 * rows, size)
                scores = lax.dot_general(
                    qs[h], keys, (((1,), (1,)), ((), ())), preferred_element_type=jnp.float32
                )
                old = top[h]
                new = jnp.maximum(old, jnp.max(scores, axis=1, keepdims=True))
                top[h] = new
                weights = jnp.exp2((scores - new[:, :1]) * grade).astype(jnp.bfloat16)
                full = jnp.concatenate([values, jnp.ones_like(values)], axis=1)
                grown = jnp.dot(weights, full, preferred_element_type=jnp.float32)
                factor = jnp.exp2((old - new) * grade)
                acc[h] = acc[h] * jnp.concatenate([factor, factor], axis=1) + grown

            @pl.when(s == chips - 1)
            def _():
                for i in range(2):
                    done = acc[2 * j + i]
                    ratio = done[:, :size] / done[:, size:]
                    held[mine, j, :, i * size : (i + 1) * size] = ratio.astype(held.dtype)
                first(j, 0).start()
                first(j, 1).start()

        @pl.when(s == 0)
        def _():
            bring(visit(chip, chips, 1))

        @pl.when(s + 2 < chips)
        def _():
            bring(visit(chip, chips, s + 2))

        @pl.when(s + 1 < chips)
        def _():
            bring_side(visit(chip, chips, s + 1))

        @pl.when(s == chips - 2)
        def _():
            for c in inform:
                c.wait_recv()
            notes_ref[mine] = sheet[...]
            for i, p in enumerate((corner, across, along)):
                remote(sheet, notes_ref.at[mine], tell.at[i], told.at[i], {"tp": p}).start()

    fetch.wait()

    def term(owner, j):
        start = pl.multiple_of(owner * width + j * 2 * size, 2 * size)
        part = w[pl.ds(start, 2 * size), :]
        total[...] += jnp.dot(held[owner, j], part, preferred_element_type=jnp.float32)

    total[...] = jnp.zeros_like(total)

    @pl.loop(0, pairs)
    def _(j):
        term(mine, j)

    @pl.loop(0, pairs)
    def _(j):
        arrive(j, 0)
        second(j, 0).start()
        arrive(j, 1)
        second(j, 1).start()
        term(across, j)
        term(along, j)

    @pl.loop(0, pairs)
    def _(j):
        arrive(j, 2)
        arrive(j, 3)
        term(corner, j)

    stage[...] = total[...].astype(stage.dtype)
    columns = pl.ds(pl.multiple_of(mine * width, width), width)

    def piece(owner):
        return pl.ds(pl.multiple_of(owner * share, share), share)

    back = [
        remote(stage.at[piece(p)], proj.at[:, columns], give.at[i], take.at[i], {"tp": p})
        for i, p in enumerate((corner, across, along))
    ]
    for c in back:
        c.start()
    proj[:, columns] = stage[piece(mine), :]
    for c in back:
        c.wait()
    mixed = (res_ref[...].astype(jnp.float32) + proj[...].astype(jnp.float32)).astype(mixed_ref.dtype)
    mixed_ref[...] = mixed
    mixed = mixed.astype(jnp.float32)
    mean = jnp.mean(mixed * mixed, axis=-1, keepdims=True)
    normed_ref[...] = (mixed * lax.rsqrt(mean + EPS) * gain_ref[...]).astype(normed_ref.dtype)

    for i, p in enumerate((corner, across, along)):
        remote(sheet, notes_ref.at[mine], tell.at[i], told.at[i], {"tp": p}).wait()

    def settle_sends():
        for c in inform:
            c.wait_send()
        for d in range(1, chips):
            p = lax.rem(chip + d, chips)
            to_plane(p).wait_send()
            sideways(p).wait_send()
        for p in range(chips):
            for side in range(2):
                hand(p, side).wait_send()
        for j in range(pairs):
            for way in range(2):
                first(j, way).wait_send()
                second(j, way).wait_send()

    return settle_sends


def visit(chip, chips, step):
    near = jnp.minimum(chip, chips - 1 - chip)
    up = chip < chips - 1 - chip
    swing = (step + 1) // 2 * (2 * lax.rem(step, 2) - 1)
    swing = jnp.where(up, chip + swing, chip - swing)
    tail = jnp.where(up, chip + (step - near), chip - (step - near))
    return jnp.where(step <= 2 * near, swing, tail)


def wide(value):
    return value.astype(jnp.float32)


def moe_part(
    n, cuts, x_ref, note_ref, mixed_ref, loads, out_ref,
    tok, wg, wu, wd, picked, hid, wsel, held, own, give, take,
    low, high, from_x, from_y, to_y, to_x, last_y, last_x, acc, zsend, zrecv, zmid,
    zs, zr, sq_s, sq_r, pd_s, pd_r, tk_s, tk_r, hop_s, hop_r, hz_s, hz_r, mid_r,
    outbox, inbox, out_s, in_r, kept,
):
    me = lax.axis_index("sp")
    chips = n // 2
    chip, core = me // 2, lax.rem(me, 2)
    other = 1 - core
    partner = {"sp": 2 * chip + other}
    mine, across, along, corner = square()
    x, y = lax.rem(mine, 2), mine // 2
    share, depth = x_ref.shape
    units = wg.shape[1]
    group = 4 * share
    slots = wsel.shape[3] // 2
    width = depth // cuts
    half = width // 2
    steps = chips * cuts

    def column(k):
        return pl.ds(pl.multiple_of(k * width, width), width)

    has_right, has_left = chip < chips - 1, chip > 0

    def cols(h):
        return pl.ds(pl.multiple_of(h * (depth // 2), depth // 2), depth // 2)

    def own_half(h):
        return x_ref.at[:, cols(h)]

    def along_z(p, h, way, first=False):
        block = tok.at[p, core, h, mine]
        to = 2 * (chip + 1 - 2 * way) + core
        return remote(
            own_half(h) if first else block, block, zs.at[p, h, way], zr.at[p, h], {"sp": to}
        )

    upper, lower = pl.ds(0, share // 2), pl.ds(share // 2, share // 2)

    def pass_on(p, h, way, first=False):
        block = tok.at[p, core, h]
        start = own_half(h) if first else block.at[mine]
        src, dst, where = (
            (start, block.at[mine], across),
            (start, block.at[mine], along),
            (block.at[across, upper], block.at[across, upper], along),
            (block.at[along, lower], block.at[along, lower], across),
        )[way]
        return remote(src, dst, sq_s.at[way], sq_r.at[p, h, way], {"tp": where})

    def arrive(p, h, way):
        block = tok.at[p, core, h]
        dst = (
            block.at[across],
            block.at[along],
            block.at[corner, upper],
            block.at[corner, lower],
        )[way]
        remote(dst, dst, sq_s.at[way], sq_r.at[p, h, way], {"tp": across}).wait_recv()

    def hand(p, h, t, first=False):
        block = tok.at[p, core, h, t]
        src = own_half(h) if first else block
        return remote(src, block, pd_s.at[0], pd_r.at[p, h, t], partner)

    def handed(p, h, t):
        block = tok.at[p, other, h, t]
        remote(block, block, pd_s.at[0], pd_r.at[p, h, t], partner).wait_recv()

    for h in range(2):
        pass_on(chip, h, 0, True).start()
        pass_on(chip, h, 1, True).start()

        @pl.when(has_right)
        def _():
            along_z(chip, h, 0, True).start()

        @pl.when(has_left)
        def _():
            along_z(chip, h, 1, True).start()

        hand(chip, h, mine, True).start()
        tok[chip, core, h, mine] = x_ref[:, cols(h)]

    def part(u):
        return visit(chip, chips, u // 2), lax.rem(u, 2)

    def finish(u):
        p, h = part(u)
        arrive(p, h, 2)
        arrive(p, h, 3)
        hand(p, h, corner).start()

    def wait_rows(p):
        for h in range(2):
            for t in range(4):
                handed(p, h, t)

    def pick_rows(p, side):
        tiles = [note_ref[t, 2 * p + side] for t in range(4)]
        lane = lax.broadcasted_iota(jnp.int32, (n, 2 * share), 1)
        chosen = lax.broadcasted_iota(jnp.int32, (n, 2 * share), 0) == me

        def across_two(even, odd, swap_even):
            moved = pltpu.roll(even if swap_even else odd, share, 1)
            return jnp.where(lane < share, moved, odd) if swap_even else jnp.where(
                lane < share, even, moved
            )

        def row_of(swap_even):
            parts_two = [across_two(tiles[t], tiles[t + 1], swap_even) for t in (0, 2)]
            picks = [
                jnp.sum(jnp.where(chosen, v, 0.0), axis=0, keepdims=True) for v in parts_two
            ]
            return jnp.concatenate(picks, axis=1)

        spot = row_of(False)
        base = lax.broadcasted_iota(jnp.int32, (1, group), 1) // share * (slots // 4)
        spot = jnp.where(spot >= 0, spot.astype(jnp.int32) + base, -1)
        weight = row_of(True)
        coarse = weight.astype(jnp.bfloat16).astype(jnp.float32)
        parts = (coarse, weight - coarse)
        hit = lax.broadcasted_iota(jnp.int32, (slots, group), 0) == spot
        pick = jnp.where(hit, 1.0, 0.0).astype(tok.dtype)
        for i in range(2):
            turned = jnp.transpose(jnp.where(hit, parts[i], 0.0))
            wsel[p, side, :, i * slots : (i + 1) * slots] = turned.astype(wsel.dtype)
        for h in range(2):
            block = tok[p, side, h].reshape(group, depth // 2)
            rows = jnp.dot(pick, block, preferred_element_type=jnp.float32)
            picked[side * slots : (side + 1) * slots, cols(h)] = rows.astype(picked.dtype)

    def activate(p, u):
        some = pl.ds(pl.multiple_of(u * 512, 512), 512)
        gate = jnp.dot(picked[...], wg[:, some], preferred_element_type=jnp.float32)
        rise = jnp.dot(picked[...], wu[:, some], preferred_element_type=jnp.float32)
        hid[p, :, some] = (jax.nn.silu(gate) * rise).astype(hid.dtype)

    def expert(p):
        wait_rows(p)
        pick_rows(p, 0)
        pick_rows(p, 1)

        @pl.loop(0, units // 512)
        def _(u):
            activate(p, u)

    def forward(u):
        p, h = part(u)
        arrive(p, h, 0)
        pass_on(p, h, 2).start()
        hand(p, h, across).start()
        arrive(p, h, 1)
        pass_on(p, h, 3).start()
        hand(p, h, along).start()

    last = 2 * chips - 1

    def passes(p):
        return ((p < chip) & has_right) | ((p > chip) & has_left)

    def relay(u):
        p, h = part(u)

        @pl.when(passes(p))
        def _():
            along_z(p, h, 0).wait_recv()

        @pl.when((p < chip) & has_right)
        def _():
            along_z(p, h, 0).start()

        @pl.when((p > chip) & has_left)
        def _():
            along_z(p, h, 1).start()

    def open_up(u):
        p, h = part(u)

        @pl.when(jnp.logical_not(passes(p)))
        def _():
            along_z(p, h, 0).wait_recv()

        pass_on(p, h, 0).start()
        pass_on(p, h, 1).start()
        hand(p, h, mine).start()

    @pl.loop(0, last)
    def _(u):
        forward(u)

        @pl.when(u == 0)
        def _():
            relay(2)
            open_up(2)

        @pl.when(u + 4 <= last)
        def _():
            relay(u + 4)

        @pl.when(u == 0)
        def _():
            relay(3)

        @pl.when(u + 3 <= last)
        def _():
            open_up(u + 3)

        @pl.when(u == 0)
        def _():
            for c in loads:
                c.wait()

        @pl.when((u == 4) | ((u > 4) & (lax.rem(u, 2) == 1)))
        def _():
            expert(visit(chip, chips, (u - 3) // 2))

        @pl.when((u >= 2) & (lax.rem(u, 2) == 0))
        def _():
            finish(u - 2)

            @pl.when(u < last - 1)
            def _():
                finish(u - 1)

    fold = cuts - 1

    def is_whole(k):
        return k == 0

    def rank_of(k):
        return lax.rem(k // cuts + 1, chips)

    def cut_of(k):
        return lax.rem(jnp.where(k < cuts, k + fold, k), cuts)

    def plane_of(k):
        return visit(chip, chips, rank_of(k))

    def swap(k):
        return remote(give.at[k], take.at[k], tk_s.at[0], tk_r.at[k], partner)

    def hop(k, way):
        src, dst, where = (
            (low.at[k, 1 - x], from_x.at[k], across),
            (high.at[k, 1 - y], from_y.at[k], along),
            (to_y.at[k], last_y.at[k], along),
            (to_x.at[k], last_x.at[k], across),
        )[way]
        return remote(src, dst, hop_s.at[way], hop_r.at[k, way], {"tp": where})

    def home(k):
        p, q = plane_of(k), cut_of(k)
        return remote(
            zsend.at[k], zrecv.at[chip, q], hz_s.at[0], hz_r.at[chip, q], {"sp": 2 * p + core}
        )

    is_end = (chip == 0) | (chip == chips - 1)

    def lend(k):
        to = chip + jnp.where(chip == 0, 1, -1)
        return remote(
            zsend.at[k], zmid.at[cut_of(k)], hz_s.at[0], mid_r.at[cut_of(k)],
            {"sp": 2 * to + core},
        )

    def homed(p, q):
        return remote(zsend.at[0], zrecv.at[p, q], hz_s.at[0], hz_r.at[p, q], partner)

    def whole_to(k):
        p, i = plane_of(k), cut_of(k) - fold
        spot = jnp.where(chip < p, 0, 1)
        return remote(
            outbox.at[i], inbox.at[spot, i], out_s.at[i], in_r.at[spot, i], {"sp": 2 * p + core}
        )

    def settle(k):
        swap(k).wait_recv()
        total = own[lax.rem(k, 3)] + wide(take[k])

        @pl.when(is_whole(k))
        def _():
            outbox[cut_of(k) - fold] = total.astype(outbox.dtype)
            whole_to(k).start()

        @pl.when(jnp.logical_not(is_whole(k)))
        def _():
            own[lax.rem(k, 3)] = total

            @pl.when((k == steps - 1) & jnp.logical_not(is_end))
            def _():
                i = 0
                for spot in range(2):
                    remote(
                        outbox.at[i], inbox.at[spot, i], out_s.at[i], in_r.at[spot, i], partner
                    ).wait_recv()
                    own[lax.rem(k, 3)] += wide(inbox[spot, i])

            cast = own[lax.rem(k, 3)].astype(low.dtype).reshape(4, share, width)
            for t in range(4):
                low[k, t % 2, t // 2] = cast[t, :, :half]
                high[k, t // 2, t % 2] = cast[t, :, half:]
            hop(k, 0).start()
            hop(k, 1).start()

    @pl.loop(0, steps + 6)
    def _(step):
        @pl.when((step >= 2) & (step < steps + 2))
        def _():
            settle(step - 2)

        @pl.when((step >= 4) & (step < steps + 4) & jnp.logical_not(is_whole(step - 4)))
        def _(k=step - 4):
            hop(k, 0).wait_recv()
            to_y[k] = (wide(low[k, x, 1 - y]) + wide(from_x[k, 1 - y])).astype(to_y.dtype)
            hop(k, 2).start()
            hop(k, 1).wait_recv()
            to_x[k] = (wide(high[k, y, 1 - x]) + wide(from_y[k, 1 - x])).astype(to_x.dtype)
            hop(k, 3).start()

        @pl.when((step >= 6) & jnp.logical_not(is_whole(step - 6)))
        def _(k=step - 6):
            hop(k, 2).wait_recv()
            left = wide(low[k, x, y]) + wide(from_x[k, y]) + wide(last_y[k])
            hop(k, 3).wait_recv()
            right = wide(high[k, y, x]) + wide(from_y[k, x]) + wide(last_x[k])

            far, own_plane = rank_of(k) == chips - 1, rank_of(k) == 0

            @pl.when(jnp.logical_not(own_plane | (far & jnp.logical_not(is_end))))
            def _():
                zsend[k, :, :half] = left.astype(zsend.dtype)
                zsend[k, :, half:] = right.astype(zsend.dtype)

                @pl.when(far)
                def _():
                    lend(k).start()

                @pl.when(jnp.logical_not(far))
                def _():
                    home(k).start()

            @pl.when(far & jnp.logical_not(is_end))
            def _():
                kept[cut_of(k), :, :half] = left
                kept[cut_of(k), :, half:] = right

            @pl.when(own_plane)
            def _():
                acc[cut_of(k), :, :half] = left
                acc[cut_of(k), :, half:] = right

        due = step - 8

        @pl.when((due >= 2 * cuts) & (due < 3 * cuts) & jnp.logical_not(is_end))
        def _():
            lend(due).wait_recv()
            q = cut_of(due)
            zsend[due] = (kept[q] + wide(zmid[q])).astype(zsend.dtype)
            home(due).start()

        @pl.when(step < steps)
        def _(k=step):
            third, fourth = visit(chip, chips, chips - 2), visit(chip, chips, chips - 1)

            @pl.when(k == cuts)
            def _():
                @pl.loop(0, units // 512)
                def _(u):
                    activate(third, u)

            p, q = plane_of(k), cut_of(k)
            out = jnp.dot(hid[p], wd[q], preferred_element_type=jnp.float32).astype(held.dtype)
            for side in range(2):
                block = out[side * slots : (side + 1) * slots]
                held[side, :slots] = block
                held[side, slots:] = block

            def spread(side):
                return jnp.dot(wsel[p, side], held[side], preferred_element_type=jnp.float32)

            give[k] = spread(other).astype(give.dtype)
            swap(k).start()
            own[lax.rem(k, 3)] = spread(core)

            @pl.when(k == cuts // 2)
            def _():
                forward(last)
                finish(last - 2)

            @pl.when(k == cuts)
            def _():
                finish(last - 1)
                finish(last)

            @pl.when((k == cuts - 1) | (k == cuts + 1))
            def _():
                p = jnp.where(k < cuts, third, fourth)
                wait_rows(p)
                pick_rows(p, 0)
                pick_rows(p, 1)

            each = units // 1024

            @pl.when((k >= cuts + 2) & (k < cuts + 4))
            def _():
                @pl.loop(0, each)
                def _(u):
                    activate(fourth, (k - cuts - 2) * each + u)

    @pl.loop(0, cuts)
    def _(q):
        for d in range(1, chips):
            p = lax.rem(chip + d, chips)

            folded = jnp.logical_not(is_end) & (jnp.abs(p - chip) == 1) & (q >= fold)

            @pl.when(jnp.logical_not((is_end & (p == chips - 1 - chip)) | folded))
            def _():
                homed(p, q).wait_recv()
                acc[q] += wide(zrecv[p, q])

        out_ref[:, column(q)] = (acc[q] + wide(mixed_ref[:, column(q)])).astype(out_ref.dtype)

    @pl.loop(0, 2 * chips)
    def _(u):
        p, h = u // 2, lax.rem(u, 2)
        @pl.when((p <= chip) & has_right)
        def _():
            along_z(p, h, 0).wait_send()

        @pl.when((p >= chip) & has_left)
        def _():
            along_z(p, h, 1).wait_send()

    def all_left(ref, sem):
        remote(ref, ref, sem, sem, partner).wait_send()

    blocks = tok.at[:, 0, :, 0]
    halves = (blocks.at[:, :, upper], blocks.at[:, :, lower])
    for way, ref in enumerate((blocks, blocks) + halves):
        all_left(ref, sq_s.at[way])
    all_left(tok.at[:, 0], pd_s.at[0])
    all_left(give, tk_s.at[0])
    for way, ref in enumerate((from_x, from_y, to_y, to_x)):
        all_left(ref.at[pl.ds(0, steps - 1)], hop_s.at[way])
    all_left(zsend.at[pl.ds(0, steps - cuts - 1)], hz_s.at[0])
    whole_to(0).wait_send()


def layer_kernel(n, cuts, *refs):
    attend_in, (wg_ref, wu_ref, wd_ref, out_ref), refs = refs[:12], refs[12:16], refs[16:]
    (mixed, normed, notes, load), refs = refs[:4], refs[4:]
    attend_room, moe_room = refs[:27], refs[27:]
    tok, wg, wu, wd = moe_room[:4]
    width = wd.shape[2]
    loads = [
        pltpu.make_async_copy(wg_ref.at[0], wg, load.at[0]),
        pltpu.make_async_copy(wu_ref.at[0], wu, load.at[1]),
    ] + [
        pltpu.make_async_copy(wd_ref.at[0, :, pl.ds(q * width, width)], wd.at[q], load.at[2 + q])
        for q in range(cuts)
    ]
    settle_sends = attend_part(n, *attend_in, mixed, normed, notes, loads, *attend_room)
    moe_part(n, cuts, normed, notes, mixed, loads, out_ref, *moe_room)
    settle_sends()


def layer(
    n, queries, keys, values, query_gain, key_gain, residual, gain, names, shares, out_proj,
    w_gate, w_up, w_down, capacity, cuts=4,
):
    rows, width = queries.shape
    size = query_gain.shape[0]
    heads = width // size
    share, depth = residual.shape
    units = w_gate.shape[2]
    chips = n // 2
    kind = queries.dtype
    cut = depth // cuts
    half = cut // 2
    steps = chips * cuts
    group, slots = 4 * share, 4 * capacity
    by_col, by_row = turn_tables(size, n * rows // GRID_W)
    dma = pltpu.SemaphoreType.DMA

    def room(*extent):
        return pltpu.VMEM(extent, kind)

    def exact(*extent):
        return pltpu.VMEM(extent, jnp.float32)

    return pl.pallas_call(
        functools.partial(layer_kernel, n, cuts),
        out_shape=jax.ShapeDtypeStruct((share, depth), kind),
        in_specs=in_vmem(11) + [pl.BlockSpec(memory_space=pl.ANY)] * 4,
        out_specs=in_vmem(1)[0],
        scratch_shapes=[
            room(share, depth),
            room(share, depth),
            exact(4, n, n, 2 * share),
            dma((2 + cuts,)),
            room(*out_proj.shape),
            room(chips, 2, 2, 2, rows // 2, size),
            room(heads, rows, size),
            exact(heads, rows, size),
            exact(heads, rows, 2 * size),
            room(4, heads // 2, rows, 2 * size),
            exact(rows, width),
            room(rows, width),
            room(share, depth),
            exact(n, n, 2 * share),
            dma((1,)),
            dma((chips,)),
            dma((chips,)),
            dma((chips,)),
            dma((chips,)),
            dma((chips, 2)),
            dma((chips, 2)),
            dma((n - 1,)),
            dma((n - 1,)),
            dma((heads // 2, 4)),
            dma((heads // 2, 4)),
            dma((3,)),
            dma((3,)),
            dma((3,)),
            dma((3,)),
            exact(n, 2 * share),
            exact(n, 2 * share),
            room(chips, 2, 2, 4, share, depth // 2),
            room(depth, units),
            room(depth, units),
            room(cuts, units, cut),
            room(2 * slots, depth),
            room(chips, 2 * slots, units),
            room(chips, 2, group, 2 * slots),
            room(2, 2 * slots, cut),
            exact(3, group, cut),
            room(steps, group, cut),
            room(steps, group, cut),
            room(steps, 2, 2, share, half),
            room(steps, 2, 2, share, half),
            room(steps, 2, share, half),
            room(steps, 2, share, half),
            room(steps, share, half),
            room(steps, share, half),
            room(steps, share, half),
            room(steps, share, half),
            exact(cuts, share, cut),
            room(steps, share, cut),
            room(chips, cuts, share, cut),
            room(cuts, share, cut),
            dma((chips, 2, 2)),
            dma((chips, 2)),
            dma((4,)),
            dma((chips, 2, 4)),
            dma((1,)),
            dma((chips, 2, 4)),
            dma((1,)),
            dma((steps,)),
            dma((4,)),
            dma((steps, 4)),
            dma((1,)),
            dma((chips, cuts)),
            dma((cuts,)),
            room(1, group, cut),
            room(2, 1, group, cut),
            dma((1,)),
            dma((2, 1)),
            exact(cuts, share, cut),
        ],
        compiler_params=params(0),
        name="layer",
    )(
        queries,
        keys,
        values,
        query_gain[None, :],
        key_gain[None, :],
        jnp.asarray(by_col),
        jnp.asarray(by_row),
        residual,
        gain[None, :],
        names,
        shares,
        out_proj,
        w_gate,
        w_up,
        w_down,
    )


def start_state(batch, rows, width):
    return (
        jnp.full((batch, rows), NEG_START, jnp.float32),
        jnp.zeros((batch, rows), jnp.float32),
        jnp.zeros((batch, rows, width), jnp.float32),
    )


def local(
    queries,
    keys,
    values,
    query_gain,
    key_gain,
    out_proj,
    expert_norm_scale,
    residual,
    routes,
    route_weights,
    w_gate,
    w_up,
    w_down,
):
    head_size = query_gain.shape[0]
    tok_sp = queries.shape[0]
    tp_count = lax.axis_size("tp")
    sp_count = lax.axis_size("sp")
    heads_dev = queries.shape[1] // head_size
    all_heads = heads_dev * tp_count
    kv_heads = keys.shape[1] // head_size
    group = all_heads // kv_heads
    scale = head_size ** (-0.5)
    tp_index = lax.axis_index("tp")
    sp_index = lax.axis_index("sp")
    tok_dev = residual.shape[0]
    top = routes.shape[1]
    capacity = max(2, 2 * tok_dev * top // sp_count)
    direct = (
        tp_count == 4
        and sp_count // 2 == 4
        and sp_count % 2 == 0
        and capacity % 16 == 0
        and 2 * tok_dev % 128 == 0
        and tok_sp % (2 * GRID_W) == 0
        and heads_dev % 2 == 0
        and 2 * heads_dev <= group
        and tok_sp == tp_count * tok_dev
    )
    if direct:
        return layer(
            sp_count,
            queries,
            keys,
            values,
            query_gain,
            key_gain,
            residual,
            expert_norm_scale,
            routes.T,
            route_weights.T,
            out_proj,
            w_gate,
            w_up,
            w_down,
            capacity,
        )
    position = sp_index * tok_sp + jnp.arange(tok_sp, dtype=jnp.int32)
    q_rot = prepare(queries, query_gain, position)
    shared_value_head = tp_index * heads_dev // group
    own_keys = prepare(
        lax.dynamic_slice_in_dim(keys, shared_value_head * head_size, head_size, 1),
        key_gain,
        position,
    )
    own_values = lax.dynamic_slice_in_dim(values, shared_value_head * head_size, head_size, 1)
    query_matrix = (
        q_rot.reshape(tok_sp, heads_dev, head_size)
        .transpose(1, 0, 2)
        .reshape(1, heads_dev * tok_sp, head_size)
    )
    key_piece = lax.all_gather(own_keys, "sp", axis=0, tiled=True)
    value_piece = lax.all_gather(own_values, "sp", axis=0, tiled=True)
    run_max, run_sum, run_acc = absorb(
        start_state(1, heads_dev * tok_sp, head_size),
        query_matrix,
        key_piece[:, None, :],
        value_piece[:, None, :],
        scale,
    )
    attn = (run_acc / run_sum[..., None]).astype(jnp.bfloat16)
    attn = (
        attn.reshape(heads_dev, tok_sp, head_size)
        .transpose(1, 0, 2)
        .reshape(tok_sp, heads_dev * head_size)
    )
    columns = jnp.dot(
        lax.all_gather(attn, "tp", axis=1, tiled=True),
        out_proj,
        preferred_element_type=jnp.float32,
    )
    projected = lax.all_to_all(
        columns.astype(jnp.bfloat16), "tp", split_axis=0, concat_axis=1, tiled=True
    )
    mixed_float_output = residual.astype(jnp.float32) + projected.astype(jnp.float32)
    mixed = mixed_float_output.astype(jnp.bfloat16)
    mixed_float_output = mixed.astype(jnp.float32)
    normed = (
        mixed_float_output
        * lax.rsqrt(jnp.mean(mixed_float_output * mixed_float_output, axis=-1, keepdims=True) + EPS)
        * expert_norm_scale
    ).astype(jnp.bfloat16)
    flat_routes = routes.reshape(-1)
    one_hot = (flat_routes[:, None] == jnp.arange(sp_count, dtype=jnp.int32)[None, :]).astype(
        jnp.int32
    )
    earlier = jnp.cumsum(one_hot, axis=0) - one_hot
    slot_index = jnp.sum(earlier * one_hot, axis=1)
    target = flat_routes * capacity + slot_index
    selector = (
        jnp.arange(sp_count * capacity, dtype=jnp.int32)[:, None] == target[None, :]
    ).astype(jnp.bfloat16)
    selector = jnp.sum(selector.reshape(sp_count * capacity, tok_dev, top), axis=2)
    send_rows = jnp.dot(selector, normed, preferred_element_type=jnp.float32).astype(jnp.bfloat16)
    arrived = lax.all_to_all(send_rows, "sp", split_axis=0, concat_axis=0, tiled=True)
    piece = lax.all_gather(arrived, "tp", axis=0, tiled=True)
    gate = jnp.dot(piece, w_gate[0], preferred_element_type=jnp.float32)
    upper = jnp.dot(piece, w_up[0], preferred_element_type=jnp.float32)
    hidden = (jax.nn.silu(gate) * upper).astype(jnp.bfloat16)
    partial = jnp.dot(hidden, w_down[0], preferred_element_type=jnp.float32).astype(jnp.bfloat16)
    expert_out = lax.psum_scatter(partial, "tp", scatter_dimension=0, tiled=True)
    returned = lax.all_to_all(expert_out, "sp", split_axis=0, concat_axis=0, tiled=True)
    picked = (
        jnp.take(returned, target, axis=0)
        .astype(jnp.float32)
        .reshape(tok_dev, top, returned.shape[1])
    )
    moe_sum = jnp.sum(picked * route_weights[:, :, None], axis=1)
    return (mixed_float_output + moe_sum).astype(jnp.bfloat16)


def solution(mesh):
    placed = (
        P("sp", "tp"),
        P("sp", None),
        P("sp", None),
        P(),
        P(),
        P(None, "tp"),
        P(),
        P(("sp", "tp"), None),
        P(("sp", "tp"), None),
        P(("sp", "tp"), None),
        P("sp", None, "tp"),
        P("sp", None, "tp"),
        P("sp", "tp", None),
    )
    return jax.shard_map(
        local, mesh=mesh, in_specs=placed, out_specs=P(("sp", "tp"), None), check_vma=False
    )
```
